512 devices in a mesh: sp: 128 (over z, y, core), tp: 4 (over x).
Axes of the slice: x: 4, y: 8, z: 8, core: 2. Of those that a mesh axis runs over, the one named last changes fastest.
Arguments:
- activations: bfloat16 [65536, 2048], P('sp', 'tp'), may hold values from -250 to 250
- norm_gain: bfloat16 [2048], P('tp'), may hold values from 0.099609375 to 1.8984375
- pool_weight: bfloat16 [2048, 1024], P('sp', 'tp'), may hold values from -0.125 to 0.125
- gate_weight: bfloat16 [2048, 1024], P('sp', 'tp'), may hold values from -0.125 to 0.125
- value_weight: bfloat16 [2048, 1024], P('sp', 'tp'), may hold values from -0.125 to 0.125
- key_weight: bfloat16 [2048, 256], P('sp', 'tp'), may hold values from -0.125 to 0.125
- read_weight: bfloat16 [2048, 256], P('sp', 'tp'), may hold values from -0.125 to 0.125
- step_weight: bfloat16 [2048, 16], P('sp', 'tp'), may hold values from -0.125 to 0.125
- pool_mix: bfloat16 [4, 256, 256], P('tp'), may hold values from -0.375 to 0.375
- pool_scale: float32 [1024], P('tp'), may hold values from 0.1 to 1.9
- taps_value: float32 [4, 1024], P(None, 'tp'), may hold values from -3 to 3
- taps_key: float32 [4, 256], P(None, 'tp'), may hold values from -3 to 3
- taps_read: float32 [4, 256], P(None, 'tp'), may hold values from -3 to 3
- step_bias: float32 [16], P('tp'), may hold values from -1 to 1
- decay_log: float32 [16], P('tp')
- decay_extra: float32 [65536, 16], P('sp', 'tp'), may hold values from -1 to 0
- skip_scale: float32 [16], P('tp'), may hold values from 0.5 to 2
- state_gain: float32 [1024], P('tp'), may hold values from 0.1 to 1.9
- out_pool_weight: bfloat16 [1024, 2048], P('tp', 'sp'), may hold values from -0.125 to 0.125
- out_state_weight: bfloat16 [1024, 2048], P('tp', 'sp'), may hold values from -0.125 to 0.125
Outputs:
- mixed: bfloat16 [65536, 2048], P('sp', 'tp')
The draws below stay inside these ranges and needn't reach their ends.
All inputs are finite; a program needn't handle non-finite values.
Results may differ from the reference program's by a relative error of at most 0.007.
Values may be sent and summed in bfloat16 or wider, within the bound.
No kernel may reach another device: no remote copies, remote signals or barrier semaphores. Data moves between devices by JAX's collectives and lax.ppermute only.
A program may use at most 64 MiB of HBM per device.

```python
import math
import jax
import jax.numpy as jnp
from jax import lax

D = 2048
SCAN_HEAD_NUMBER = 16
SSM_HEAD_DIM = 64
SSM_GROUPS = 4
SSM_STATE = 64
POOL_GROUPS = 4
MIXER_CONV_TAPS = 4
SCAN_BLOCK = 128
TOK_DEV = 512
MIX_W = 1024
GW = 256
TOKENS = 65536


def draw_activations(key, part):
    first, second = jax.random.split(key, 2)
    spot = jnp.arange(D).astype(jnp.float32) / D
    rough = jnp.exp(jax.random.uniform(second, (1, D), jnp.float32, -0.35, 0.35))
    basic = jnp.clip(jax.random.normal(first, (TOKENS, D), jnp.float32), -4.0, 4.0)
    rising = jnp.exp(spot * 1.1)[None, :]
    return (basic * rising * rough).astype(jnp.bfloat16)


def draw_decay_log(key, part):
    first, second, third = jax.random.split(key, 3)
    fast_rate = jnp.log(jax.random.uniform(first, (SCAN_HEAD_NUMBER,), jnp.float32, 0.03, 0.1))
    slow_rate = jax.random.uniform(second, (SCAN_HEAD_NUMBER,), jnp.float32, jnp.log(0.1), jnp.log(0.5)) - jnp.log(TOKENS * 1.0)
    chance = 0.5
    quick = jax.random.uniform(third, (SCAN_HEAD_NUMBER,), jnp.float32) < chance
    return jnp.where(quick, fast_rate, slow_rate)


def draw_decay_extra(key, part):
    first, second, third, quarter_slice = jax.random.split(key, 4)
    steady_rate = jnp.exp(jax.random.uniform(first, (1, 1, SCAN_HEAD_NUMBER), jnp.float32, jnp.log(0.2), jnp.log(0.6))) / TOKENS
    factor = jnp.exp(jax.random.uniform(second, (TOKENS // TOK_DEV, 1, 1), jnp.float32, jnp.log(0.25), jnp.log(2.0)))
    constant_baseline = -(factor * steady_rate * jnp.ones((1, TOK_DEV, 1), jnp.float32)).reshape(TOKENS, SCAN_HEAD_NUMBER)
    places = jax.random.randint(third, (3,), 0, TOKENS)
    masked_elements = jnp.any(jnp.arange(TOKENS)[:, None] == places[None, :], axis=1)
    sudden_impulse = jnp.log(jax.random.uniform(quarter_slice, (1, SCAN_HEAD_NUMBER), jnp.float32, 0.5, 0.8))
    return constant_baseline + jnp.where(masked_elements[:, None], sudden_impulse, 0.0)


def shard_levels(key, dims, pieces, least, top_value):
    def one(axis_at, blocks):
        steps = jax.random.uniform(jax.random.fold_in(jax.random.fold_in(key, 6), axis_at), (blocks,), jnp.float32, least / len(pieces), top_value / len(pieces))
        return jnp.repeat(jnp.exp(steps), dims[axis_at] // blocks).reshape((-1,) + (1,) * (len(dims) - axis_at - 1))

    gain = one(*pieces[0])
    for cut in pieces[1:]:
        gain = gain * one(*cut)
    return gain


def normal_values(rng, dims, scale, bound, shards=(), held_as=jnp.bfloat16):
    values = scale * jax.random.normal(rng, dims, jnp.float32)
    if shards:
        values = values * shard_levels(rng, dims, shards, -0.22, 0.18)
    return jnp.clip(values, -bound, bound).astype(held_as)


def setup_inputs(seed: int = 0) -> dict:
    streams_of = jax.random.split(jax.random.key(seed), 21)
    activations = draw_activations(jax.random.fold_in(streams_of[20], 71), 0)
    norm_gain = jnp.clip(1.0 + 0.18 * jax.random.normal(streams_of[1], (D,), jnp.float32), 0.099609375, 1.8984375).astype(jnp.bfloat16)
    pool_weight = normal_values(streams_of[2], (D, MIX_W), D ** -0.5, 0.125, ((0, 128), (1, 4)))
    gate_weight = normal_values(streams_of[3], (D, MIX_W), D ** -0.5, 0.125, ((0, 128), (1, 4)))
    value_weight = normal_values(streams_of[4], (D, MIX_W), D ** -0.5, 0.125, ((0, 128), (1, 4)))
    key_weight = normal_values(streams_of[5], (D, SSM_GROUPS * SSM_STATE), D ** -0.5, 0.125, ((0, 128), (1, 4)))
    read_weight = normal_values(streams_of[6], (D, SSM_GROUPS * SSM_STATE), D ** -0.5, 0.125, ((0, 128), (1, 4)))
    step_weight = normal_values(streams_of[7], (D, SCAN_HEAD_NUMBER), D ** -0.5, 0.125, ((0, 128), (1, 4)))
    pool_mix = normal_values(streams_of[8], (POOL_GROUPS, GW, GW), GW ** -0.5, 0.375, ((0, 4),))
    pool_scale = jnp.clip(1.0 + 0.18 * jax.random.normal(streams_of[9], (MIX_W,), jnp.float32), 0.1, 1.9)
    taps_value = normal_values(streams_of[10], (MIXER_CONV_TAPS, MIX_W), MIXER_CONV_TAPS ** -0.5, 3.0, ((1, 4),), jnp.float32)
    taps_key = normal_values(streams_of[11], (MIXER_CONV_TAPS, SSM_GROUPS * SSM_STATE), MIXER_CONV_TAPS ** -0.5, 3.0, ((1, 4),), jnp.float32)
    taps_read = normal_values(streams_of[12], (MIXER_CONV_TAPS, SSM_GROUPS * SSM_STATE), MIXER_CONV_TAPS ** -0.5, 3.0, ((1, 4),), jnp.float32)
    step_bias = jnp.clip(jax.random.uniform(streams_of[13], (SCAN_HEAD_NUMBER,), jnp.float32, -1.0, 1.0) * shard_levels(streams_of[13], (SCAN_HEAD_NUMBER,), ((0, 4),), -0.4, 0.0), -1.0, 1.0)
    decay_log = draw_decay_log(jax.random.fold_in(streams_of[20], 71), 0)
    decay_extra = draw_decay_extra(jax.random.fold_in(streams_of[20], 71), 0)
    skip_scale = jnp.clip(jnp.exp(math.log(2.0) - 1.3862944 * jax.random.uniform(streams_of[16], (SCAN_HEAD_NUMBER,), jnp.float32) ** shard_levels(streams_of[16], (SCAN_HEAD_NUMBER,), ((0, 4),), -0.2, 0.2)), 0.5, 2.0)
    state_gain = jnp.clip(1.0 + 0.18 * jax.random.normal(streams_of[17], (MIX_W,), jnp.float32), 0.1, 1.9)
    out_pool_weight = normal_values(streams_of[18], (MIX_W, D), (2 * MIX_W) ** -0.5, 0.125, ((0, 4), (1, 128)))
    out_state_weight = normal_values(streams_of[19], (MIX_W, D), (2 * MIX_W) ** -0.5, 0.125, ((0, 4), (1, 128)))
    return {"activations": activations, "norm_gain": norm_gain, "pool_weight": pool_weight, "gate_weight": gate_weight, "value_weight": value_weight, "key_weight": key_weight, "read_weight": read_weight, "step_weight": step_weight, "pool_mix": pool_mix, "pool_scale": pool_scale, "taps_value": taps_value, "taps_key": taps_key, "taps_read": taps_read, "step_bias": step_bias, "decay_log": decay_log, "decay_extra": decay_extra, "skip_scale": skip_scale, "state_gain": state_gain, "out_pool_weight": out_pool_weight, "out_state_weight": out_state_weight}


EPSILON = 1e-06
HIGH = lax.Precision.HIGHEST

def backward_kernel(raw, taps):
    width = taps.shape[0]
    length = raw.shape[0]
    padded = jnp.pad(raw.astype(jnp.float32), ((width - 1, 0), (0, 0)))
    total = jnp.zeros(raw.shape, jnp.float32)
    for offset in range(width):
        total = total + taps[offset][None, :] * padded[offset:offset + length]
    return jax.nn.silu(total).astype(jnp.bfloat16)

def scan_block(state, inputs):
    head_value, step_size, log_decay, key_heads, read_heads = inputs
    length = head_value.shape[0]
    running = jnp.cumsum(log_decay, axis=0)
    lower = jnp.arange(length)[:, None] >= jnp.arange(length)[None, :]
    gaps = jnp.where(lower[:, :, None], running[:, None, :] - running[None, :, :], -jnp.inf)
    weights = jnp.einsum('lhn,shn->lsh', read_heads, key_heads, precision=HIGH) * jnp.exp(gaps)
    scaled_value = head_value * step_size[:, :, None]
    inner = jnp.einsum('lsh,shp->lhp', weights, scaled_value, precision=HIGH)
    carried = jnp.einsum('lhn,hpn->lhp', read_heads, state, precision=HIGH) * jnp.exp(running)[:, :, None]
    trailing = jnp.exp(running[-1][None, :] - running)
    fresh = jnp.einsum('shn,sh,shp->hpn', key_heads, trailing, scaled_value, precision=HIGH)
    new_state = state * jnp.exp(running[-1])[:, None, None] + fresh
    return (new_state, inner + carried)

def reference(activations, norm_gain, pool_weight, gate_weight, value_weight, key_weight, read_weight, step_weight, pool_mix, pool_scale, taps_value, taps_key, taps_read, step_bias, decay_log, decay_extra, skip_scale, state_gain, out_pool_weight, out_state_weight):
    values = activations.astype(jnp.float32)
    normed = (values * lax.rsqrt(lax.optimization_barrier(jnp.mean(values * values, axis=-1, keepdims=True)) + EPSILON) * norm_gain.astype(jnp.float32)).astype(jnp.bfloat16)
    pool_in = jnp.dot(normed, pool_weight, preferred_element_type=jnp.float32).astype(jnp.bfloat16)
    gate_in = jnp.dot(normed, gate_weight, preferred_element_type=jnp.float32).astype(jnp.bfloat16)
    raw_value = jnp.dot(normed, value_weight, preferred_element_type=jnp.float32).astype(jnp.bfloat16)
    raw_key = jnp.dot(normed, key_weight, preferred_element_type=jnp.float32).astype(jnp.bfloat16)
    raw_read = jnp.dot(normed, read_weight, preferred_element_type=jnp.float32).astype(jnp.bfloat16)
    step_raw = jnp.dot(normed, step_weight, preferred_element_type=jnp.float32)
    reach = 2 ** POOL_GROUPS - 1
    pool_values = pool_in.astype(jnp.float32)
    padded = jnp.pad(pool_values, ((reach, 0), (0, 0)))
    position = jnp.arange(TOKENS).astype(jnp.float32)
    outputs = []
    for group in range(POOL_GROUPS):
        window = 2 ** (group + 1)
        column_count = padded[:, group * GW:(group + 1) * GW]
        window_sum = jnp.zeros((TOKENS, GW), jnp.float32)
        for back in range(window):
            window_sum = window_sum + column_count[reach - back:reach - back + TOKENS]
        counts = jnp.minimum(position + 1.0, float(window))
        pooled = (window_sum / counts[:, None] - pool_values[:, group * GW:(group + 1) * GW]).astype(jnp.bfloat16)
        outputs.append(jnp.dot(pooled, pool_mix[group], preferred_element_type=jnp.float32))
    pool_out = (jnp.concatenate(outputs, axis=1) * pool_scale).astype(jnp.bfloat16)
    head_value = backward_kernel(raw_value, taps_value)
    key_vectors = backward_kernel(raw_key, taps_key)
    read_vectors = backward_kernel(raw_read, taps_read)
    step_size = jax.nn.softplus(step_raw + step_bias)
    log_decay = -jnp.exp(decay_log) * step_size + decay_extra
    repeat = SCAN_HEAD_NUMBER // SSM_GROUPS
    blocks = TOKENS // SCAN_BLOCK
    value_heads = head_value.astype(jnp.float32).reshape(TOKENS, SCAN_HEAD_NUMBER, SSM_HEAD_DIM)
    key_heads = jnp.repeat(key_vectors.astype(jnp.float32).reshape(TOKENS, SSM_GROUPS, SSM_STATE), repeat, axis=1)
    read_heads = jnp.repeat(read_vectors.astype(jnp.float32).reshape(TOKENS, SSM_GROUPS, SSM_STATE), repeat, axis=1)
    start = jnp.zeros((SCAN_HEAD_NUMBER, SSM_HEAD_DIM, SSM_STATE), jnp.float32)
    _, scanned = lax.scan(scan_block, start, (value_heads.reshape(blocks, SCAN_BLOCK, SCAN_HEAD_NUMBER, SSM_HEAD_DIM), step_size.reshape(blocks, SCAN_BLOCK, SCAN_HEAD_NUMBER), log_decay.reshape(blocks, SCAN_BLOCK, SCAN_HEAD_NUMBER), key_heads.reshape(blocks, SCAN_BLOCK, SCAN_HEAD_NUMBER, SSM_STATE), read_heads.reshape(blocks, SCAN_BLOCK, SCAN_HEAD_NUMBER, SSM_STATE)))
    scan_out = scanned.reshape(TOKENS, SCAN_HEAD_NUMBER, SSM_HEAD_DIM) + skip_scale[None, :, None] * value_heads
    gated = scan_out.reshape(TOKENS, MIX_W) * jax.nn.silu(gate_in.astype(jnp.float32))
    state_out = (gated * lax.rsqrt(lax.optimization_barrier(jnp.mean(gated * gated, axis=-1, keepdims=True)) + EPSILON) * state_gain).astype(jnp.bfloat16)
    result = jnp.dot(pool_out, out_pool_weight, preferred_element_type=jnp.float32) + jnp.dot(state_out, out_state_weight, preferred_element_type=jnp.float32)
    return result.astype(jnp.bfloat16)
```

```python
import jax
import jax.numpy as jnp
from jax import lax
from jax.sharding import Mesh
from jax.sharding import PartitionSpec as P

D = 2048
SSM_STATE = 64
POOL_GROUPS = 4
SCAN_BLOCK = 128
MIX_W = 1024
SP = ("sp_0", "sp_1", "sp_2")


EPSILON = 1e-06
HIGH = lax.Precision.HIGHEST


def sent_to_all(array, axis):
    copies = jnp.broadcast_to(array, (lax.axis_size(axis), *array.shape))
    return lax.all_to_all(copies, axis, split_axis=0, concat_axis=0, tiled=True)


def over_copies(array, axis):
    everything = sent_to_all(array, axis)
    return jnp.sum(everything, axis=0)


def shifted(value, axis, steps):
    count = lax.axis_size(axis)
    leading, last = (max(0, -steps), min(count, count - steps))
    return lax.ppermute(value, axis, [(source, source + steps) for source in range(leading, last)])


def parts_of(value):
    high = value.astype(jnp.bfloat16)
    rest = value - high.astype(jnp.float32)
    middle = rest.astype(jnp.bfloat16)
    low = (rest - middle.astype(jnp.float32)).astype(jnp.bfloat16)
    return jnp.concatenate([high, middle, low])


def packed(state, log_total):
    lanes = 128
    numbers = parts_of(log_total)
    tail = jnp.pad(numbers, (0, 16 * lanes - numbers.shape[0])).reshape(16, lanes)
    return jnp.concatenate([state.astype(jnp.bfloat16).reshape(-1, lanes), tail])


def unpacked(pieces, heads, shape):
    rows = pieces.shape[1] - 16
    numbers = pieces[:, rows, : 3 * heads].astype(jnp.float32).reshape(-1, 3, heads)
    return pieces[:, :rows].reshape(-1, *shape), jnp.sum(numbers, axis=1)


def weighted(states, logs, begin, end):
    count = states.shape[0]
    source = jnp.arange(count)
    between = (source[None, :] > source[:, None]) & (source[None, :] < end)
    total = jnp.sum(jnp.where(between[:, :, None], logs[None, :, :], 0.0), axis=1)
    factors = jnp.where((source < end)[:, None], jnp.exp(total + begin), 0.0)
    return jnp.sum(states.astype(jnp.float32) * factors[:, :, None, None], axis=0)


def split_up(array, dim, count):
    before, after = (array.shape[:dim], array.shape[dim + 1 :])
    return jnp.moveaxis(array.reshape(*before, count, -1, *after), dim, 0)


def summed_on_arrival(array, axis, dim):
    pieces = split_up(array, dim, lax.axis_size(axis))
    arrived = lax.all_to_all(pieces, axis, split_axis=0, concat_axis=0, tiled=True)
    return arrived.astype(jnp.float32).sum(axis=0)


def backward_kernel(extended, taps):
    width = taps.shape[0]
    length = extended.shape[0] - (width - 1)
    widened_rows = extended.astype(jnp.float32)
    total = jnp.zeros((length, extended.shape[1]), jnp.float32)
    for offset in range(width):
        total = total + taps[offset][None, :] * widened_rows[offset : offset + length]
    return jax.nn.silu(total).astype(jnp.bfloat16)


def local(
    activations,
    norm_gain,
    pool_weight,
    gate_weight,
    value_weight,
    key_weight,
    read_weight,
    step_weight,
    pool_mix,
    pool_scale,
    taps_value,
    taps_key,
    taps_read,
    step_bias,
    decay_log,
    decay_extra,
    skip_scale,
    state_gain,
    out_pool_weight,
    out_state_weight,
):
    length = activations.shape[0]
    cluster_span = pool_weight.shape[1]
    local_mix = gate_weight.shape[1]
    local_state = key_weight.shape[1]
    local_heads = step_weight.shape[1]
    plane = ("sp_0", "sp_1")
    place = lax.axis_index("tp")
    core = lax.axis_index("sp_2")
    sent = jnp.concatenate(
        [activations, jnp.broadcast_to(norm_gain[None, :], (8, norm_gain.shape[0]))], axis=0
    )
    everything = sent_to_all(sent, "tp")
    first_weights = jnp.concatenate([value_weight, key_weight, step_weight], axis=1)
    mine = sent_to_all(first_weights, plane)
    other = lax.ppermute(mine, "sp_2", [(0, 1), (1, 0)])
    joined = jnp.concatenate(
        [
            pool_weight,
            gate_weight,
            read_weight,
            jnp.transpose(out_pool_weight),
            jnp.transpose(out_state_weight),
        ],
        axis=1,
    )
    later_weights = lax.all_gather(joined, SP, axis=0, tiled=True)
    reach = 2**POOL_GROUPS
    received = everything[:, :length]
    before = shifted(received[:, length - reach :], SP, 1)
    rows = jnp.concatenate([before, received], axis=1).astype(jnp.float32)
    squares = jnp.sum(rows * rows, axis=(0, 2))
    gains = everything[:, length].astype(jnp.float32)
    normed = (
        rows * lax.rsqrt(squares / D + EPSILON)[None, :, None] * gains[:, None, :]
    ).astype(jnp.bfloat16)
    in_weight = jnp.stack(
        [jnp.where(core == 0, mine, other), jnp.where(core == 0, other, mine)], axis=1
    ).reshape(lax.axis_size("tp"), -1, first_weights.shape[1])
    first = jnp.einsum("ktd,kdn->tn", normed, in_weight, preferred_element_type=jnp.float32)
    raw_value = first[:, :local_mix].astype(jnp.bfloat16)
    raw_key = first[:, local_mix : local_mix + local_state].astype(jnp.bfloat16)
    step_raw = first[reach:, local_mix + local_state :]
    second_weights = later_weights[:, : cluster_span + local_mix + local_state]
    second = jnp.einsum(
        "ktd,kdn->tn",
        normed,
        second_weights.reshape(lax.axis_size("tp"), -1, second_weights.shape[1]),
        preferred_element_type=jnp.float32,
    ).astype(jnp.bfloat16)
    pool_all = second[:, :cluster_span]
    pool_in = pool_all[reach:]
    gate_in = second[reach:, cluster_span : cluster_span + local_mix]
    raw_read = second[:, cluster_span + local_mix :]
    width = taps_value.shape[0]
    group = place
    running = pool_all[1:].astype(jnp.float32)
    levels = []
    for level in range(POOL_GROUPS):
        stride = 2**level
        running = running[stride:] + running[:-stride]
        levels.append(running[running.shape[0] - length :])
    window_sum = lax.dynamic_index_in_dim(jnp.stack(levels), group, 0, keepdims=False)
    window = jnp.exp2((group + 1).astype(jnp.float32))
    position = (lax.axis_index(SP) * length + jnp.arange(length, dtype=jnp.int32)).astype(
        jnp.float32
    )
    counts = jnp.minimum(position + 1.0, window)
    pooled = (window_sum / counts[:, None] - pool_in.astype(jnp.float32)).astype(jnp.bfloat16)
    pool_out = (
        jnp.dot(pooled, pool_mix[0], preferred_element_type=jnp.float32) * pool_scale
    ).astype(jnp.bfloat16)
    start = reach - width + 1
    head_value = backward_kernel(raw_value[start:], taps_value)
    key_vectors = backward_kernel(raw_key[start:], taps_key)
    read_vectors = backward_kernel(raw_read[start:], taps_read)
    head_dim = local_mix // local_heads
    groups_here = local_state // SSM_STATE
    repeat = local_heads // groups_here
    blocks = length // SCAN_BLOCK
    step_size = jax.nn.softplus(step_raw + step_bias)
    log_decay = -jnp.exp(decay_log) * step_size + decay_extra
    value_heads = head_value.astype(jnp.float32).reshape(length, local_heads, head_dim)
    value_blocks = value_heads.reshape(blocks, SCAN_BLOCK, local_heads, head_dim)
    key_blocks = jnp.repeat(
        key_vectors.astype(jnp.float32).reshape(length, groups_here, SSM_STATE), repeat, axis=1
    ).reshape(blocks, SCAN_BLOCK, local_heads, SSM_STATE)
    read_blocks = jnp.repeat(
        read_vectors.astype(jnp.float32).reshape(length, groups_here, SSM_STATE), repeat, axis=1
    ).reshape(blocks, SCAN_BLOCK, local_heads, SSM_STATE)
    step_blocks = step_size.reshape(blocks, SCAN_BLOCK, local_heads)
    running_decay = jnp.cumsum(log_decay.reshape(blocks, SCAN_BLOCK, local_heads), axis=1)
    lower = jnp.arange(SCAN_BLOCK)[:, None] >= jnp.arange(SCAN_BLOCK)[None, :]
    gaps = jnp.where(
        lower[None, :, :, None],
        running_decay[:, :, None, :] - running_decay[:, None, :, :],
        -jnp.inf,
    )
    weights = jnp.einsum("blhn,bshn->blsh", read_blocks, key_blocks, precision=HIGH) * jnp.exp(gaps)
    scaled_value = value_blocks * step_blocks[..., None]
    inner = jnp.einsum("blsh,bshp->blhp", weights, scaled_value, precision=HIGH)
    block_ends = running_decay[:, -1, :]
    trailing = jnp.exp(block_ends[:, None, :] - running_decay)
    fresh = jnp.einsum("bshn,bsh,bshp->bhpn", key_blocks, trailing, scaled_value, precision=HIGH)

    def advance(carry, inputs):
        block_decay, block_state = inputs
        return (carry * block_decay[:, None, None] + block_state, carry)

    local_total, prefix = lax.scan(
        advance,
        jnp.zeros((local_heads, head_dim, SSM_STATE), jnp.float32),
        (jnp.exp(block_ends), fresh),
    )
    offsets = jnp.cumsum(block_ends, axis=0) - block_ends
    device_log = offsets[-1] + block_ends[-1]
    state_shape = local_total.shape
    row = lax.axis_index(("sp_1", "sp_2"))
    row_count = lax.axis_size(("sp_1", "sp_2"))
    row_states, row_logs = unpacked(
        lax.all_gather(packed(local_total, device_log), ("sp_1", "sp_2")), local_heads, state_shape
    )
    row_total = weighted(row_states, row_logs, 0.0, row_count)
    plane_states, plane_logs = unpacked(
        sent_to_all(packed(row_total, jnp.sum(row_logs, axis=0)), "sp_0"), local_heads, state_shape
    )
    row_before = jnp.sum(jnp.where((jnp.arange(row_count) < row)[:, None], row_logs, 0.0), axis=0)
    incoming = weighted(row_states, row_logs, 0.0, row) + weighted(
        plane_states, plane_logs, row_before, lax.axis_index("sp_0")
    )
    from_device = running_decay + offsets[:, None, :]
    local_off = (
        jnp.einsum("blhn,bhpn->blhp", read_blocks, prefix, precision=HIGH)
        * jnp.exp(running_decay)[..., None]
    )
    far_off = (
        jnp.einsum("blhn,hpn->blhp", read_blocks, incoming, precision=HIGH)
        * jnp.exp(from_device)[..., None]
    )
    scan_out = (inner + local_off + far_off).reshape(length, local_heads, head_dim) + skip_scale[
        None, :, None
    ] * value_heads
    gated = scan_out.reshape(length, local_mix) * jax.nn.silu(gate_in.astype(jnp.float32))
    gate_squares = over_copies(jnp.sum(gated * gated, axis=-1), "tp")
    state_rows = (gated * state_gain).astype(jnp.bfloat16)
    out_weights = later_weights[:, second_weights.shape[1] :]
    pool_terms = jnp.einsum(
        "tc,dc->td", pool_out, out_weights[:, :cluster_span], preferred_element_type=jnp.float32
    )
    state_terms = jnp.einsum(
        "tc,dc->td", state_rows, out_weights[:, cluster_span:], preferred_element_type=jnp.float32
    )
    terms = pool_terms + state_terms * lax.rsqrt(gate_squares / MIX_W + EPSILON)[:, None]
    result = summed_on_arrival(terms.astype(jnp.bfloat16), "tp", 1)
    return result.astype(jnp.bfloat16)


def solution(mesh):
    torus = Mesh(mesh.devices.reshape(8, 8, 2, mesh.shape["tp"]), ("sp_0", "sp_1", "sp_2", "tp"))
    placed = (
        P(SP, "tp"),
        P("tp"),
        P(SP, "tp"),
        P(SP, "tp"),
        P(SP, "tp"),
        P(SP, "tp"),
        P(SP, "tp"),
        P(SP, "tp"),
        P("tp", None, None),
        P("tp"),
        P(None, "tp"),
        P(None, "tp"),
        P(None, "tp"),
        P("tp"),
        P("tp"),
        P(SP, "tp"),
        P("tp"),
        P("tp"),
        P("tp", SP),
        P("tp", SP),
    )
    return jax.shard_map(local, mesh=torus, in_specs=placed, out_specs=P(SP, "tp"), check_vma=False)
```

```python
import jax
import jax.numpy as jnp
from jax import lax
from jax.experimental import pallas as pl
from jax.experimental.pallas import tpu as pltpu
from jax.sharding import Mesh
from jax.sharding import PartitionSpec as P

D = 2048
POOL_GROUPS = 4
HEAD = 64
MIX_W = 1024
HALO = 16
PAY = 16
BLOCK = 128
SP = ("sp_0", "sp_1", "sp_2")
EPSILON = 1e-06
HIGH = lax.Precision.HIGHEST
F32 = jnp.float32
BF16 = jnp.bfloat16


def sent_to_all(array, axis):
    copies = jnp.broadcast_to(array, (lax.axis_size(axis), *array.shape))
    return lax.all_to_all(copies, axis, split_axis=0, concat_axis=0, tiled=True)


def dot(a, b, left=1, right=0, precision=None):
    return lax.dot_general(
        a, b, (((left,), (right,)), ((), ())), precision=precision, preferred_element_type=F32
    )


def silu(x):
    return x * jax.nn.sigmoid(x)


def heads_of_lanes(lanes):
    head = lax.broadcasted_iota(jnp.int32, (8, lanes), 0)
    lane = lax.broadcasted_iota(jnp.int32, (8, lanes), 1)
    return (head == lane // HEAD).astype(F32)


def convolved(raw, taps, length):
    width = taps.shape[0]
    total = jnp.zeros((length, raw.shape[1]), F32)
    for k in range(width):
        at = HALO - width + 1 + k
        total = total + taps[k : k + 1] * raw[at : at + length]
    return silu(total).astype(BF16)


def write_payload(ref, state, log_row):
    rows = state.shape[0]
    high = log_row.astype(BF16).astype(F32)
    middle = (log_row - high).astype(BF16).astype(F32)
    low = log_row - high - middle
    at = lax.broadcasted_iota(jnp.int32, (PAY, log_row.shape[1]), 0)
    tail = jnp.where(at == 0, high, jnp.where(at == 1, middle, jnp.where(at == 2, low, 0.0)))
    ref[:rows] = state.astype(BF16)
    ref[rows:] = tail.astype(BF16)


def read_payload(ref, k):
    rows = ref.shape[1] - PAY
    tail = ref[k, rows:].astype(F32)
    return ref[k, :rows].astype(F32), jnp.sum(tail, axis=0, keepdims=True)


def scan_payloads(ref, place):
    rows, lanes = ref.shape[1] - PAY, ref.shape[2]
    total = before = jnp.zeros((rows, lanes), F32)
    logs = logs_before = jnp.zeros((1, lanes), F32)
    for k in range(ref.shape[0]):
        state, log_row = read_payload(ref, k)
        total = total * jnp.exp(log_row) + state
        logs = logs + log_row
        before = jnp.where(k < place, total, before)
        logs_before = jnp.where(k < place, logs, logs_before)
    return total, logs, before, logs_before


def first_kernel(
    at, x0, x1, x2, x3, mine, other, taps, bias, rate, extra,
    normed, value_out, key_out, cum_out, step_out, payload, weight,
):
    core = at[1]
    weight[:, pl.ds(core, 1)] = mine[...][:, None]
    weight[:, pl.ds(1 - core, 1)] = other[...][:, None]
    pieces = (x0, x1, x2, x3)
    total_rows = x0.shape[0] - PAY
    length = total_rows - HALO
    squares = jnp.zeros((total_rows, 1), F32)
    for piece in pieces:
        values = piece[:total_rows].astype(F32)
        squares = squares + jnp.sum(values * values, axis=1, keepdims=True)
    scale = lax.rsqrt(squares / D + EPSILON)
    chips, columns = weight.shape[0] // 4, weight.shape[3]
    acc = jnp.zeros((total_rows, columns), F32)
    for k, piece in enumerate(pieces):
        gain = piece[total_rows : total_rows + 1].astype(F32)
        part = (piece[:total_rows].astype(F32) * scale * gain).astype(BF16)
        normed[k] = part
        block = weight[pl.ds(((at[0] - k) & 3) * chips, chips)]
        acc = acc + dot(part, block.reshape(-1, columns))
    mix = value_out.shape[1]
    done = convolved(acc.astype(BF16).astype(F32), taps[...], length)
    value_out[...] = done[:, :mix]
    key_out[...] = done[:, mix:]
    raw = jnp.transpose(acc[HALO:, mix:])[HEAD : HEAD + 8] + bias[...]
    step = jnp.maximum(raw, 0.0) + jnp.log1p(jnp.exp(-jnp.abs(raw)))
    decay = rate[...] * step + extra[...]
    rows = lax.broadcasted_iota(jnp.int32, (BLOCK, BLOCK), 0)
    upper = (rows <= lax.broadcasted_iota(jnp.int32, (BLOCK, BLOCK), 1)).astype(F32)
    carry, cums = jnp.zeros((8, 1), F32), []
    for b in range(length // BLOCK):
        cums.append(dot(decay[:, b * BLOCK : (b + 1) * BLOCK], upper, precision=HIGH) + carry)
        carry = cums[-1][:, BLOCK - 1 :]
    cum = jnp.concatenate(cums, axis=1)
    cum_out[...] = cum
    step_out[...] = step
    lanes = heads_of_lanes(mix)
    spread = dot(jnp.exp(carry - cum) * step, lanes, 0, 0, HIGH)
    state = dot(done[:, mix:].astype(F32), done[:, :mix].astype(F32) * spread, 0, 0, HIGH)
    write_payload(payload, state[:HEAD], jnp.sum(carry * lanes, axis=0, keepdims=True))


def row_kernel(at, rows, before_out, logs_out, payload):
    total, logs, before, logs_before = scan_payloads(rows, at[2])
    before_out[...] = before
    logs_out[...] = jnp.broadcast_to(logs_before, logs_out.shape)
    write_payload(payload, total, logs)


def second_kernel(
    at, normed, weight, weight_read, value, key, cum, step, taps, mix_weight, pool_scale, skip,
    pool_out, gate_out, read_out, local_out,
):
    length, span = pool_out.shape
    total_rows = normed.shape[1]
    acc = jnp.zeros((total_rows, weight.shape[1]), F32)
    acc_read = jnp.zeros((total_rows, weight_read.shape[1]), F32)
    width = normed.shape[2]
    for k in range(normed.shape[0]):
        start = pl.multiple_of(((at[0] - k) & 3) * width, width)
        acc = acc + dot(normed[k], weight[pl.ds(start, width)])
        acc_read = acc_read + dot(normed[k], weight_read[pl.ds(start, width)])
    gate_out[...] = acc[HALO:, span:].astype(BF16)
    running = acc[:, :span].astype(BF16).astype(F32)
    own = running[HALO:]
    chosen = own
    for level in range(POOL_GROUPS):
        stride = 2**level
        running = running[stride:] + running[:-stride]
        chosen = jnp.where(at[0] == level, running[running.shape[0] - length :], chosen)
    position = at[4] * length + lax.broadcasted_iota(jnp.int32, (length, 1), 0) + 1
    counts = jnp.minimum(position, 2 << at[0]).astype(F32)
    pooled = (chosen / counts - own).astype(BF16)
    pool_out[...] = (dot(pooled, mix_weight[...]) * pool_scale[...]).astype(BF16)
    reads = convolved(acc_read.astype(BF16).astype(F32), taps[...], length)
    read_out[...] = reads
    lanes = heads_of_lanes(span)
    values = value[...].astype(F32)
    scaled = (values * dot(step[...], lanes, 0, 0, HIGH)).astype(BF16)
    columns = jnp.transpose(cum[...])
    lower = lax.broadcasted_iota(jnp.int32, (BLOCK, BLOCK), 0) >= lax.broadcasted_iota(
        jnp.int32, (BLOCK, BLOCK), 1
    )
    for i in range(length // BLOCK):
        here = slice(i * BLOCK, (i + 1) * BLOCK)
        products = [
            dot(reads[here], key[j * BLOCK : (j + 1) * BLOCK], 1, 1) for j in range(i + 1)
        ]
        results = []
        for h in range(span // HEAD):
            parts = []
            for j in range(i + 1):
                gap = columns[here, h : h + 1] - cum[h : h + 1, j * BLOCK : (j + 1) * BLOCK]
                if i == j:
                    gap = jnp.where(lower, gap, -jnp.inf)
                parts.append((products[j] * jnp.exp(gap)).astype(BF16))
            left = jnp.concatenate(parts, axis=1)
            right = scaled[: (i + 1) * BLOCK, h * HEAD : (h + 1) * HEAD]
            results.append(dot(left, right))
        local_out[here] = jnp.concatenate(results, axis=1) + skip[...] * values[here]


def third_kernel(
    at, planes, before, logs_before, reads, local_in, gate, cum, gain, rows_out, squares_out
):
    _, _, earlier, _ = scan_payloads(planes, at[3])
    incoming = earlier * jnp.exp(logs_before[:1]) + before[...]
    lanes = heads_of_lanes(local_in.shape[1])
    decay = dot(jnp.exp(cum[...]), lanes, 0, 0, HIGH)
    far = dot(reads[:, :HEAD].astype(F32), incoming, precision=HIGH) * decay
    gated = (local_in[...] + far) * silu(gate[...].astype(F32))
    ones = jnp.ones((8, gated.shape[1]), F32)
    squares_out[...] = dot(ones, gated * gated, 1, 1, HIGH)
    rows_out[...] = (gated * gain[...]).astype(BF16)


def out_kernel(pool, rows, squares, weight, out):
    span = pool.shape[1]
    mean = jnp.sum(squares[...], axis=0) / MIX_W
    scale = jnp.transpose(lax.rsqrt(mean + EPSILON))[:, :1]
    for d in range(out.shape[0]):
        width = out.shape[2]
        block = weight[d * width : (d + 1) * width]
        terms = dot(pool[...], block[:, :span], 1, 1)
        terms = terms + dot(rows[...], block[:, span:], 1, 1) * scale
        out[d] = terms.astype(BF16)


def whole(shape):
    return pl.BlockSpec(shape, lambda *_: (0,) * len(shape))


SMEM = pl.BlockSpec(memory_space=pltpu.SMEM)


def call(kernel, args, outs, flops, scratch=(), specs=None):
    specs = specs or {}
    moved = sum(a.size * a.dtype.itemsize for a in args)
    return pl.pallas_call(
        kernel,
        grid=(1,),
        in_specs=[specs.get(k, whole(a.shape)) for k, a in enumerate(args)],
        out_specs=[whole(o.shape) for o in outs],
        out_shape=outs,
        scratch_shapes=list(scratch),
        compiler_params=pltpu.CompilerParams(vmem_limit_bytes=48 * 1024 * 1024),
        cost_estimate=pl.CostEstimate(flops=flops, transcendentals=0, bytes_accessed=moved),
    )(*args)


def shape_of(shape, dtype):
    return jax.ShapeDtypeStruct(shape, dtype)


def columns_of(array):
    return jnp.pad(array[:, None], ((0, 8 - array.shape[0]), (0, 0)))


def local(
    activations,
    norm_gain,
    pool_weight,
    gate_weight,
    value_weight,
    key_weight,
    read_weight,
    step_weight,
    pool_mix,
    pool_scale,
    taps_value,
    taps_key,
    taps_read,
    step_bias,
    decay_log,
    decay_extra,
    skip_scale,
    state_gain,
    out_pool_weight,
    out_state_weight,
):
    length, width = activations.shape
    mix = value_weight.shape[1]
    state = key_weight.shape[1]
    heads = step_weight.shape[1]
    count = lax.axis_size("tp")
    at = jnp.stack(
        [
            lax.axis_index("tp"),
            lax.axis_index("sp_2"),
            lax.axis_index(("sp_1", "sp_2")),
            lax.axis_index("sp_0"),
            lax.axis_index(SP),
        ]
    ).astype(jnp.int32)
    fill = jnp.zeros((read_weight.shape[0], BLOCK - state), BF16)
    joined = jnp.concatenate(
        [
            pool_weight,
            gate_weight,
            jnp.transpose(out_pool_weight),
            jnp.transpose(out_state_weight),
            read_weight,
            fill,
        ],
        axis=1,
    )
    later_weights = lax.all_gather(joined, SP, axis=0, tiled=True)
    fill = jnp.zeros((key_weight.shape[0], BLOCK - state - heads), BF16)
    first_weights = jnp.concatenate([value_weight, key_weight, step_weight, fill], axis=1)
    mine = sent_to_all(first_weights, ("sp_0", "sp_1"))
    other = lax.ppermute(mine, "sp_2", [(0, 1), (1, 0)])
    size = lax.axis_size(SP)
    before = lax.ppermute(activations[length - HALO :], SP, [(k, k + 1) for k in range(size - 1)])
    gains = jnp.broadcast_to(norm_gain[None, :], (PAY, width))
    sent = jnp.concatenate([before, activations, gains], axis=0)
    pieces = [sent] + [
        lax.ppermute(sent, "tp", [(k, (k + shift) % count) for k in range(count)])
        for shift in range(1, count)
    ]
    taps = jnp.pad(
        jnp.concatenate([taps_value, taps_key], axis=1), ((0, 0), (0, BLOCK - state))
    )
    extra = jnp.pad(jnp.transpose(decay_extra), ((0, 8 - heads), (0, 0)))
    rows = HALO + length
    columns = mix + BLOCK
    pay = shape_of((HEAD + PAY, mix), BF16)
    normed, value, key, cum, step, payload = call(
        first_kernel,
        (at, *pieces, mine, other, taps, columns_of(step_bias), columns_of(-jnp.exp(decay_log)), extra),
        (
            shape_of((count, rows, width), BF16),
            shape_of((length, mix), BF16),
            shape_of((length, BLOCK), BF16),
            shape_of((8, length), F32),
            shape_of((8, length), F32),
            pay,
        ),
        2 * rows * D * columns,
        [pltpu.VMEM((mine.shape[0], 2, mine.shape[1], columns), BF16)],
        {0: SMEM},
    )
    row_pieces = lax.all_gather(payload, ("sp_1", "sp_2"))
    before_row, logs_row, payload = call(
        row_kernel,
        (at, row_pieces),
        (shape_of((HEAD, mix), F32), shape_of((8, mix), F32), pay),
        10**6,
        specs={0: SMEM},
    )
    plane_pieces = sent_to_all(payload, "sp_0")
    taps_r = jnp.pad(taps_read, ((0, 0), (0, BLOCK - state)))
    pool_out, gate, reads, inside = call(
        second_kernel,
        (
            at, normed, later_weights, later_weights, value, key, cum, step, taps_r,
            pool_mix[0], pool_scale[None, :], jnp.repeat(skip_scale, HEAD)[None, :],
        ),
        (
            shape_of((length, mix), BF16),
            shape_of((length, mix), BF16),
            shape_of((length, BLOCK), BF16),
            shape_of((length, mix), F32),
        ),
        2 * rows * D * (2 * mix + BLOCK),
        specs={
            0: SMEM,
            2: pl.BlockSpec((D, 2 * mix), lambda *_: (0, 0)),
            3: pl.BlockSpec((D, BLOCK), lambda *_: (0, 4 * mix // BLOCK)),
        },
    )
    gated, squares = call(
        third_kernel,
        (at, plane_pieces, before_row, logs_row, reads, inside, gate, cum, state_gain[None, :]),
        (shape_of((length, mix), BF16), shape_of((8, length), F32)),
        10**7,
        specs={0: SMEM},
    )
    all_squares = sent_to_all(squares, "tp")
    terms = call(
        out_kernel,
        (pool_out, gated, all_squares, later_weights),
        (shape_of((count, length, width), BF16),),
        2 * length * 2 * mix * D,
        specs={3: pl.BlockSpec((D, 2 * mix), lambda *_: (0, 1))},
    )[0]
    arrived = lax.all_to_all(terms, "tp", split_axis=0, concat_axis=0, tiled=True)
    return arrived.astype(F32).sum(axis=0).astype(BF16)


def solution(mesh):
    torus = Mesh(mesh.devices.reshape(8, 8, 2, mesh.shape["tp"]), ("sp_0", "sp_1", "sp_2", "tp"))
    placed = (
        P(SP, "tp"),
        P("tp"),
        P(SP, "tp"),
        P(SP, "tp"),
        P(SP, "tp"),
        P(SP, "tp"),
        P(SP, "tp"),
        P(SP, "tp"),
        P("tp", None, None),
        P("tp"),
        P(None, "tp"),
        P(None, "tp"),
        P(None, "tp"),
        P("tp"),
        P("tp"),
        P(SP, "tp"),
        P("tp"),
        P("tp"),
        P("tp", SP),
        P("tp", SP),
    )
    return jax.shard_map(local, mesh=torus, in_specs=placed, out_specs=P(SP, "tp"), check_vma=False)
```

```python
import jax
import jax.numpy as jnp
from jax import lax
from jax.experimental import pallas as pl
from jax.experimental.pallas import tpu as pltpu
from jax.sharding import Mesh
from jax.sharding import PartitionSpec as P


D = 2048
POOL_GROUPS = 4
HEAD = 64
MIX_W = 1024
HALO = 16
PAY = 16
BLOCK = 128
SP = ("sp_0", "sp_1", "sp_2")
EPSILON = 1e-06
HIGH = lax.Precision.HIGHEST
F32 = jnp.float32
BF16 = jnp.bfloat16


def sent_to_all(array, axis):
    copies = jnp.broadcast_to(array, (lax.axis_size(axis), *array.shape))
    return lax.all_to_all(copies, axis, split_axis=0, concat_axis=0, tiled=True)


def dot(a, b, left=1, right=0, precision=None):
    return lax.dot_general(
        a, b, (((left,), (right,)), ((), ())), precision=precision, preferred_element_type=F32
    )


def silu(x):
    return x * jax.nn.sigmoid(x)


def heads_of_lanes(lanes):
    head = lax.broadcasted_iota(jnp.int32, (8, lanes), 0)
    lane = lax.broadcasted_iota(jnp.int32, (8, lanes), 1)
    return (head == lane // HEAD).astype(F32)


def convolved(raw, taps, length):
    width = taps.shape[0]
    total = jnp.zeros((length, raw.shape[1]), F32)
    for k in range(width):
        at = HALO - width + 1 + k
        total = total + taps[k : k + 1] * raw[at : at + length]
    return silu(total).astype(BF16)


def write_payload(ref, state, log_row):
    rows = state.shape[0]
    high = log_row.astype(BF16).astype(F32)
    middle = (log_row - high).astype(BF16).astype(F32)
    low = log_row - high - middle
    at = lax.broadcasted_iota(jnp.int32, (PAY, log_row.shape[1]), 0)
    tail = jnp.where(at == 0, high, jnp.where(at == 1, middle, jnp.where(at == 2, low, 0.0)))
    ref[:rows] = state.astype(BF16)
    ref[rows:] = tail.astype(BF16)


def read_payload(ref, k):
    rows = ref.shape[1] - PAY
    tail = ref[k, rows:].astype(F32)
    return ref[k, :rows].astype(F32), jnp.sum(tail, axis=0, keepdims=True)


def scan_payloads(ref, place):
    rows, lanes = ref.shape[1] - PAY, ref.shape[2]
    total = before = jnp.zeros((rows, lanes), F32)
    logs = logs_before = jnp.zeros((1, lanes), F32)
    for k in range(ref.shape[0]):
        state, log_row = read_payload(ref, k)
        total = total * jnp.exp(log_row) + state
        logs = logs + log_row
        before = jnp.where(k < place, total, before)
        logs_before = jnp.where(k < place, logs, logs_before)
    return total, logs, before, logs_before


def squares_of(pieces, total_rows):
    squares = jnp.zeros((total_rows, 1), F32)
    for piece in pieces:
        values = piece[:total_rows].astype(F32)
        squares = squares + jnp.sum(values * values, axis=1, keepdims=True)
    return squares


def early_kernel(x0, x3, out):
    out[...] = squares_of((x0, x3), out.shape[0])


def norm_kernel(early, x0, x1, x2, x3, normed):
    total_rows = normed.shape[1]
    scale = lax.rsqrt((early[...] + squares_of((x1, x2), total_rows)) / D + EPSILON)
    for k, piece in enumerate((x0, x1, x2, x3)):
        gain = piece[total_rows : total_rows + 1].astype(F32)
        normed[k] = (piece[:total_rows].astype(F32) * scale * gain).astype(BF16)


def first_kernel(
    at, normed, mine, other, taps, bias, rate, extra,
    value_out, key_out, cum_out, step_out, payload, weight,
):
    core = at[1]
    weight[:, pl.ds(core, 1)] = mine[...][:, None]
    weight[:, pl.ds(1 - core, 1)] = other[...][:, None]
    total_rows = normed.shape[1]
    length = total_rows - HALO
    chips, columns = weight.shape[0] // 4, weight.shape[3]
    acc = jnp.zeros((total_rows, columns), F32)
    for k in range(normed.shape[0]):
        block = weight[pl.ds(((at[0] - k) & 3) * chips, chips)]
        acc = acc + dot(normed[k], block.reshape(-1, columns))
    mix = value_out.shape[1]
    done = convolved(acc.astype(BF16).astype(F32), taps[...], length)
    value_out[...] = done[:, :mix]
    key_out[...] = done[:, mix:]
    raw = jnp.transpose(acc[HALO:, mix:])[HEAD : HEAD + 8] + bias[...]
    step = jnp.maximum(raw, 0.0) + jnp.log1p(jnp.exp(-jnp.abs(raw)))
    decay = rate[...] * step + extra[...]
    rows = lax.broadcasted_iota(jnp.int32, (BLOCK, BLOCK), 0)
    upper = (rows <= lax.broadcasted_iota(jnp.int32, (BLOCK, BLOCK), 1)).astype(F32)
    carry, cums = jnp.zeros((8, 1), F32), []
    for b in range(length // BLOCK):
        cums.append(dot(decay[:, b * BLOCK : (b + 1) * BLOCK], upper, precision=HIGH) + carry)
        carry = cums[-1][:, BLOCK - 1 :]
    cum = jnp.concatenate(cums, axis=1)
    cum_out[...] = cum
    step_out[...] = step
    lanes = heads_of_lanes(mix)
    spread = dot(jnp.exp(carry - cum) * step, lanes, 0, 0, HIGH)
    state = dot(done[:, mix:].astype(F32), done[:, :mix].astype(F32) * spread, 0, 0, HIGH)
    write_payload(payload, state[:HEAD], jnp.sum(carry * lanes, axis=0, keepdims=True))


def row_kernel(at, rows, before_out, logs_out, payload):
    total, logs, before, logs_before = scan_payloads(rows, at[2])
    before_out[...] = before
    logs_out[...] = jnp.broadcast_to(logs_before, logs_out.shape)
    write_payload(payload, total, logs)


def second_kernel(
    at, normed, weight, weight_read, value, key, cum, step, taps, mix_weight, pool_scale, skip,
    pool_out, gate_out, read_out, local_out,
):
    length, span = pool_out.shape
    total_rows = normed.shape[1]
    acc = jnp.zeros((total_rows, weight.shape[1]), F32)
    acc_read = jnp.zeros((total_rows, weight_read.shape[1]), F32)
    width = normed.shape[2]
    for k in range(normed.shape[0]):
        start = pl.multiple_of(((at[0] - k) & 3) * width, width)
        acc = acc + dot(normed[k], weight[pl.ds(start, width)])
        acc_read = acc_read + dot(normed[k], weight_read[pl.ds(start, width)])
    gate_out[...] = acc[HALO:, span:].astype(BF16)
    running = acc[:, :span].astype(BF16).astype(F32)
    own = running[HALO:]
    chosen = own
    for level in range(POOL_GROUPS):
        stride = 2**level
        running = running[stride:] + running[:-stride]
        chosen = jnp.where(at[0] == level, running[running.shape[0] - length :], chosen)
    position = at[4] * length + lax.broadcasted_iota(jnp.int32, (length, 1), 0) + 1
    counts = jnp.minimum(position, 2 << at[0]).astype(F32)
    pooled = (chosen / counts - own).astype(BF16)
    pool_out[...] = (dot(pooled, mix_weight[...]) * pool_scale[...]).astype(BF16)
    reads = convolved(acc_read.astype(BF16).astype(F32), taps[...], length)
    read_out[...] = reads
    lanes = heads_of_lanes(span)
    values = value[...].astype(F32)
    scaled = (values * dot(step[...], lanes, 0, 0, HIGH)).astype(BF16)
    columns = jnp.transpose(cum[...])
    lower = lax.broadcasted_iota(jnp.int32, (BLOCK, BLOCK), 0) >= lax.broadcasted_iota(
        jnp.int32, (BLOCK, BLOCK), 1
    )
    for i in range(length // BLOCK):
        here = slice(i * BLOCK, (i + 1) * BLOCK)
        products = [
            dot(reads[here], key[j * BLOCK : (j + 1) * BLOCK], 1, 1) for j in range(i + 1)
        ]
        results = []
        for h in range(span // HEAD):
            parts = []
            for j in range(i + 1):
                gap = columns[here, h : h + 1] - cum[h : h + 1, j * BLOCK : (j + 1) * BLOCK]
                if i == j:
                    gap = jnp.where(lower, gap, -jnp.inf)
                parts.append((products[j] * jnp.exp(gap)).astype(BF16))
            left = jnp.concatenate(parts, axis=1)
            right = scaled[: (i + 1) * BLOCK, h * HEAD : (h + 1) * HEAD]
            results.append(dot(left, right))
        local_out[here] = jnp.concatenate(results, axis=1) + skip[...] * values[here]


def third_kernel(
    at, planes, before, logs_before, reads, local_in, gate, cum, gain, rows_out, squares_out
):
    _, _, earlier, _ = scan_payloads(planes, at[3])
    incoming = earlier * jnp.exp(logs_before[:1]) + before[...]
    lanes = heads_of_lanes(local_in.shape[1])
    decay = dot(jnp.exp(cum[...]), lanes, 0, 0, HIGH)
    far = dot(reads[:, :HEAD].astype(F32), incoming, precision=HIGH) * decay
    gated = (local_in[...] + far) * silu(gate[...].astype(F32))
    ones = jnp.ones((8, gated.shape[1]), F32)
    squares_out[...] = dot(ones, gated * gated, 1, 1, HIGH)
    rows_out[...] = (gated * gain[...]).astype(BF16)


def out_kernel(pool, rows, squares, weight, out):
    span = pool.shape[1]
    mean = jnp.sum(squares[...], axis=0) / MIX_W
    scale = jnp.transpose(lax.rsqrt(mean + EPSILON))[:, :1]
    for d in range(out.shape[0]):
        width = out.shape[2]
        block = weight[d * width : (d + 1) * width]
        terms = dot(pool[...], block[:, :span], 1, 1)
        terms = terms + dot(rows[...], block[:, span:], 1, 1) * scale
        out[d] = terms.astype(BF16)


def whole(shape):
    return pl.BlockSpec(shape, lambda *_: (0,) * len(shape))


SMEM = pl.BlockSpec(memory_space=pltpu.SMEM)


def call(kernel, args, outs, flops, scratch=(), specs=None):
    specs = specs or {}
    moved = sum(a.size * a.dtype.itemsize for a in args)
    return pl.pallas_call(
        kernel,
        grid=(1,),
        in_specs=[specs.get(k, whole(a.shape)) for k, a in enumerate(args)],
        out_specs=[whole(o.shape) for o in outs],
        out_shape=outs,
        scratch_shapes=list(scratch),
        compiler_params=pltpu.CompilerParams(vmem_limit_bytes=48 * 1024 * 1024),
        cost_estimate=pl.CostEstimate(flops=flops, transcendentals=0, bytes_accessed=moved),
    )(*args)


def shape_of(shape, dtype):
    return jax.ShapeDtypeStruct(shape, dtype)


def columns_of(array):
    return jnp.pad(array[:, None], ((0, 8 - array.shape[0]), (0, 0)))


def local(
    activations,
    norm_gain,
    pool_weight,
    gate_weight,
    value_weight,
    key_weight,
    read_weight,
    step_weight,
    pool_mix,
    pool_scale,
    taps_value,
    taps_key,
    taps_read,
    step_bias,
    decay_log,
    decay_extra,
    skip_scale,
    state_gain,
    out_pool_weight,
    out_state_weight,
):
    length, width = activations.shape
    mix = value_weight.shape[1]
    state = key_weight.shape[1]
    heads = step_weight.shape[1]
    count = lax.axis_size("tp")
    at = jnp.stack(
        [
            lax.axis_index("tp"),
            lax.axis_index("sp_2"),
            lax.axis_index(("sp_1", "sp_2")),
            lax.axis_index("sp_0"),
            lax.axis_index(SP),
        ]
    ).astype(jnp.int32)
    fill = jnp.zeros((read_weight.shape[0], BLOCK - state), BF16)
    joined = jnp.concatenate(
        [
            pool_weight,
            gate_weight,
            jnp.transpose(out_pool_weight),
            jnp.transpose(out_state_weight),
            read_weight,
            fill,
        ],
        axis=1,
    )
    later_weights = lax.all_gather(joined, SP, axis=0, tiled=True)
    fill = jnp.zeros((key_weight.shape[0], BLOCK - state - heads), BF16)
    first_weights = jnp.concatenate([value_weight, key_weight, step_weight, fill], axis=1)
    mine = sent_to_all(first_weights, ("sp_0", "sp_1"))
    other = lax.ppermute(mine, "sp_2", [(0, 1), (1, 0)])
    size = lax.axis_size(SP)
    before = lax.ppermute(activations[length - HALO :], SP, [(k, k + 1) for k in range(size - 1)])
    gains = jnp.broadcast_to(norm_gain[None, :], (PAY, width))
    sent = jnp.concatenate([before, activations, gains], axis=0)
    pieces = [sent]
    for shift in range(1, count):
        pairs = [(k, (k + shift) % count) for k in range(count)]
        pieces.append(lax.ppermute(sent, "tp", pairs))
    rows = HALO + length
    early = call(early_kernel, (pieces[0], pieces[-1]), (shape_of((rows, 1), F32),), 10**6)[0]
    normed = call(norm_kernel, (early, *pieces), (shape_of((count, rows, width), BF16),), 10**6)[0]
    taps = jnp.pad(
        jnp.concatenate([taps_value, taps_key], axis=1), ((0, 0), (0, BLOCK - state))
    )
    extra = jnp.pad(jnp.transpose(decay_extra), ((0, 8 - heads), (0, 0)))
    columns = mix + BLOCK
    pay = shape_of((HEAD + PAY, mix), BF16)
    value, key, cum, step, payload = call(
        first_kernel,
        (at, normed, mine, other, taps, columns_of(step_bias), columns_of(-jnp.exp(decay_log)), extra),
        (
            shape_of((length, mix), BF16),
            shape_of((length, BLOCK), BF16),
            shape_of((8, length), F32),
            shape_of((8, length), F32),
            pay,
        ),
        2 * rows * D * columns,
        [pltpu.VMEM((mine.shape[0], 2, mine.shape[1], columns), BF16)],
        {0: SMEM},
    )
    row_pieces = lax.all_gather(payload, ("sp_1", "sp_2"))
    before_row, logs_row, payload = call(
        row_kernel,
        (at, row_pieces),
        (shape_of((HEAD, mix), F32), shape_of((8, mix), F32), pay),
        10**6,
        specs={0: SMEM},
    )
    plane_pieces = sent_to_all(payload, "sp_0")
    taps_r = jnp.pad(taps_read, ((0, 0), (0, BLOCK - state)))
    pool_out, gate, reads, inside = call(
        second_kernel,
        (
            at, normed, later_weights, later_weights, value, key, cum, step, taps_r,
            pool_mix[0], pool_scale[None, :], jnp.repeat(skip_scale, HEAD)[None, :],
        ),
        (
            shape_of((length, mix), BF16),
            shape_of((length, mix), BF16),
            shape_of((length, BLOCK), BF16),
            shape_of((length, mix), F32),
        ),
        2 * rows * D * (2 * mix + BLOCK),
        specs={
            0: SMEM,
            2: pl.BlockSpec((D, 2 * mix), lambda *_: (0, 0)),
            3: pl.BlockSpec((D, BLOCK), lambda *_: (0, 4 * mix // BLOCK)),
        },
    )
    gated, squares = call(
        third_kernel,
        (at, plane_pieces, before_row, logs_row, reads, inside, gate, cum, state_gain[None, :]),
        (shape_of((length, mix), BF16), shape_of((8, length), F32)),
        10**7,
        specs={0: SMEM},
    )
    all_squares = sent_to_all(squares, "tp")
    terms = call(
        out_kernel,
        (pool_out, gated, all_squares, later_weights),
        (shape_of((count, length, width), BF16),),
        2 * length * 2 * mix * D,
        specs={3: pl.BlockSpec((D, 2 * mix), lambda *_: (0, 1))},
    )[0]
    arrived = lax.all_to_all(terms, "tp", split_axis=0, concat_axis=0, tiled=True)
    return arrived.astype(F32).sum(axis=0).astype(BF16)


def solution(mesh):
    torus = Mesh(mesh.devices.reshape(8, 8, 2, mesh.shape["tp"]), ("sp_0", "sp_1", "sp_2", "tp"))
    placed = (
        P(SP, "tp"),
        P("tp"),
        P(SP, "tp"),
        P(SP, "tp"),
        P(SP, "tp"),
        P(SP, "tp"),
        P(SP, "tp"),
        P(SP, "tp"),
        P("tp", None, None),
        P("tp"),
        P(None, "tp"),
        P(None, "tp"),
        P(None, "tp"),
        P("tp"),
        P("tp"),
        P(SP, "tp"),
        P("tp"),
        P("tp"),
        P("tp", SP),
        P("tp", SP),
    )
    return jax.shard_map(local, mesh=torus, in_specs=placed, out_specs=P(SP, "tp"), check_vma=False)
```

```python
import jax
import jax.numpy as jnp
from jax import lax
from jax.experimental import pallas as pl
from jax.experimental.pallas import tpu as pltpu
from jax.sharding import Mesh
from jax.sharding import PartitionSpec as P


D = 2048
POOL_GROUPS = 4
HEAD = 64
MIX_W = 1024
HALO = 16
PAY = 16
BLOCK = 128
SP = ("sp_0", "sp_1", "sp_2")
EPSILON = 1e-06
HIGH = lax.Precision.HIGHEST
F32 = jnp.float32
BF16 = jnp.bfloat16


def sent_to_all(array, axis):
    copies = jnp.broadcast_to(array, (lax.axis_size(axis), *array.shape))
    return lax.all_to_all(copies, axis, split_axis=0, concat_axis=0, tiled=True)


def dot(a, b, left=1, right=0, precision=None):
    return lax.dot_general(
        a, b, (((left,), (right,)), ((), ())), precision=precision, preferred_element_type=F32
    )


def silu(x):
    return x * jax.nn.sigmoid(x)


def heads_of_lanes(lanes):
    head = lax.broadcasted_iota(jnp.int32, (8, lanes), 0)
    lane = lax.broadcasted_iota(jnp.int32, (8, lanes), 1)
    return (head == lane // HEAD).astype(F32)


def convolved(raw, taps, length):
    width = taps.shape[0]
    total = jnp.zeros((length, raw.shape[1]), F32)
    for k in range(width):
        at = HALO - width + 1 + k
        total = total + taps[k : k + 1] * raw[at : at + length]
    return silu(total).astype(BF16)


def write_payload(ref, state, log_row):
    rows = state.shape[0]
    high = log_row.astype(BF16).astype(F32)
    middle = (log_row - high).astype(BF16).astype(F32)
    low = log_row - high - middle
    at = lax.broadcasted_iota(jnp.int32, (PAY, log_row.shape[1]), 0)
    tail = jnp.where(at == 0, high, jnp.where(at == 1, middle, jnp.where(at == 2, low, 0.0)))
    ref[:rows] = state.astype(BF16)
    ref[rows:] = tail.astype(BF16)


def read_payload(ref, k):
    rows = ref.shape[1] - PAY
    tail = ref[k, rows:].astype(F32)
    return ref[k, :rows].astype(F32), jnp.sum(tail, axis=0, keepdims=True)


def scan_payloads(ref, place):
    rows, lanes = ref.shape[1] - PAY, ref.shape[2]
    total = before = jnp.zeros((rows, lanes), F32)
    logs = logs_before = jnp.zeros((1, lanes), F32)
    for k in range(ref.shape[0]):
        state, log_row = read_payload(ref, k)
        total = total * jnp.exp(log_row) + state
        logs = logs + log_row
        before = jnp.where(k < place, total, before)
        logs_before = jnp.where(k < place, logs, logs_before)
    return total, logs, before, logs_before


def squares_of(pieces, total_rows):
    squares = jnp.zeros((total_rows, 1), F32)
    for piece in pieces:
        values = piece[:total_rows].astype(F32)
        squares = squares + jnp.sum(values * values, axis=1, keepdims=True)
    return squares


def early_kernel(x0, x3, out):
    out[...] = squares_of((x0, x3), out.shape[0])


def norm_kernel(early, x0, x1, x2, x3, normed):
    total_rows = normed.shape[1]
    scale = lax.rsqrt((early[...] + squares_of((x1, x2), total_rows)) / D + EPSILON)
    for k, piece in enumerate((x0, x1, x2, x3)):
        gain = piece[total_rows : total_rows + 1].astype(F32)
        normed[k] = (piece[:total_rows].astype(F32) * scale * gain).astype(BF16)


def first_kernel(
    normed, mine, other, params, extra,
    value_out, key_out, cum_out, step_out, payload, weight,
):
    core = lax.axis_index("sp_2")
    place = lax.axis_index("tp")
    weight[:, pl.ds(core, 1)] = mine[...][:, None]
    weight[:, pl.ds(1 - core, 1)] = other[...][:, None]
    total_rows = normed.shape[1]
    length = total_rows - HALO
    chips, columns = weight.shape[0] // 4, weight.shape[3]
    acc = jnp.zeros((total_rows, columns), F32)
    for k in range(normed.shape[0]):
        block = weight[pl.ds(((place - k) & 3) * chips, chips)]
        acc = acc + dot(normed[k], block.reshape(-1, columns))
    mix = value_out.shape[1]
    done = convolved(acc.astype(BF16).astype(F32), params[:4], length)
    value_out[...] = done[:, :mix]
    key_out[...] = done[:, mix:]
    raw = jnp.transpose(acc[HALO:, mix:])[HEAD : HEAD + 8] + params[8:16, :1]
    step = jnp.maximum(raw, 0.0) + jnp.log1p(jnp.exp(-jnp.abs(raw)))
    decay = params[16:24, :1] * step + extra[...]
    rows = lax.broadcasted_iota(jnp.int32, (BLOCK, BLOCK), 0)
    upper = (rows <= lax.broadcasted_iota(jnp.int32, (BLOCK, BLOCK), 1)).astype(F32)
    carry, cums = jnp.zeros((8, 1), F32), []
    for b in range(length // BLOCK):
        cums.append(dot(decay[:, b * BLOCK : (b + 1) * BLOCK], upper, precision=HIGH) + carry)
        carry = cums[-1][:, BLOCK - 1 :]
    cum = jnp.concatenate(cums, axis=1)
    cum_out[...] = cum
    step_out[...] = step
    lanes = heads_of_lanes(mix)
    spread = dot(jnp.exp(carry - cum) * step, lanes, 0, 0, HIGH)
    state = dot(done[:, mix:].astype(F32), done[:, :mix].astype(F32) * spread, 0, 0, HIGH)
    write_payload(payload, state[:HEAD], jnp.sum(carry * lanes, axis=0, keepdims=True))


def row_kernel(rows, before_out, logs_out, payload):
    total, logs, before, logs_before = scan_payloads(rows, lax.axis_index(("sp_1", "sp_2")))
    before_out[...] = before
    logs_out[...] = jnp.broadcast_to(logs_before, logs_out.shape)
    write_payload(payload, total, logs)


def second_kernel(
    normed, weight, weight_read, value, key, cum, step, params, mix_weight,
    pool_out, gate_out, read_out, local_out,
):
    length, span = pool_out.shape
    place = lax.axis_index("tp")
    total_rows = normed.shape[1]
    acc = jnp.zeros((total_rows, weight.shape[1]), F32)
    acc_read = jnp.zeros((total_rows, weight_read.shape[1]), F32)
    width = normed.shape[2]
    for k in range(normed.shape[0]):
        start = pl.multiple_of(((place - k) & 3) * width, width)
        acc = acc + dot(normed[k], weight[pl.ds(start, width)])
        acc_read = acc_read + dot(normed[k], weight_read[pl.ds(start, width)])
    gate_out[...] = acc[HALO:, span:].astype(BF16)
    running = acc[:, :span].astype(BF16).astype(F32)
    own = running[HALO:]
    chosen = own
    for level in range(POOL_GROUPS):
        stride = 2**level
        running = running[stride:] + running[:-stride]
        chosen = jnp.where(place == level, running[running.shape[0] - length :], chosen)
    position = lax.axis_index(SP) * length + lax.broadcasted_iota(jnp.int32, (length, 1), 0) + 1
    counts = jnp.minimum(position, 2 << place).astype(F32)
    pooled = (chosen / counts - own).astype(BF16)
    pool_out[...] = (dot(pooled, mix_weight[...]) * params[25:26, :span]).astype(BF16)
    reads = convolved(acc_read.astype(BF16).astype(F32), params[4:8, :BLOCK], length)
    read_out[...] = reads
    lanes = heads_of_lanes(span)
    values = value[...].astype(F32)
    scaled = (values * dot(step[...], lanes, 0, 0, HIGH)).astype(BF16)
    columns = jnp.transpose(cum[...])
    lower = lax.broadcasted_iota(jnp.int32, (BLOCK, BLOCK), 0) >= lax.broadcasted_iota(
        jnp.int32, (BLOCK, BLOCK), 1
    )
    for i in range(length // BLOCK):
        here = slice(i * BLOCK, (i + 1) * BLOCK)
        products = [
            dot(reads[here], key[j * BLOCK : (j + 1) * BLOCK], 1, 1) for j in range(i + 1)
        ]
        results = []
        for h in range(span // HEAD):
            parts = []
            for j in range(i + 1):
                gap = columns[here, h : h + 1] - cum[h : h + 1, j * BLOCK : (j + 1) * BLOCK]
                if i == j:
                    gap = jnp.where(lower, gap, -jnp.inf)
                parts.append((products[j] * jnp.exp(gap)).astype(BF16))
            left = jnp.concatenate(parts, axis=1)
            right = scaled[: (i + 1) * BLOCK, h * HEAD : (h + 1) * HEAD]
            results.append(dot(left, right))
        local_out[here] = jnp.concatenate(results, axis=1) + params[24:25, :span] * values[here]


def third_kernel(
    planes, before, logs_before, reads, local_in, gate, cum, params, rows_out, squares_out
):
    _, _, earlier, _ = scan_payloads(planes, lax.axis_index("sp_0"))
    incoming = earlier * jnp.exp(logs_before[:1]) + before[...]
    lanes = heads_of_lanes(local_in.shape[1])
    decay = dot(jnp.exp(cum[...]), lanes, 0, 0, HIGH)
    far = dot(reads[:, :HEAD].astype(F32), incoming, precision=HIGH) * decay
    gated = (local_in[...] + far) * silu(gate[...].astype(F32))
    ones = jnp.ones((8, gated.shape[1]), F32)
    squares_out[...] = dot(ones, gated * gated, 1, 1, HIGH)
    rows_out[...] = (gated * params[26:27, : gated.shape[1]]).astype(BF16)


def out_kernel(pool, rows, squares, weight, out):
    span = pool.shape[1]
    mean = jnp.sum(squares[...], axis=0) / MIX_W
    scale = jnp.transpose(lax.rsqrt(mean + EPSILON))[:, :1]
    for d in range(out.shape[0]):
        width = out.shape[2]
        block = weight[d * width : (d + 1) * width]
        terms = dot(pool[...], block[:, :span], 1, 1)
        terms = terms + dot(rows[...], block[:, span:], 1, 1) * scale
        out[d] = terms.astype(BF16)


def whole(shape):
    return pl.BlockSpec(shape, lambda *_: (0,) * len(shape))


LIMITS = {"early": 8, "norm": 16, "first": 16, "row": 6, "second": 24, "third": 10, "out": 16}


def call(kernel, name, args, outs, flops, scratch=(), specs=None, far=()):
    specs = specs or {}
    moved = sum(a.size * a.dtype.itemsize for a in args)
    args = [
        pltpu.with_memory_space_constraint(a, pltpu.HBM) if k in far else a
        for k, a in enumerate(args)
    ]
    return pl.pallas_call(
        kernel,
        grid=(1,),
        in_specs=[specs.get(k, whole(a.shape)) for k, a in enumerate(args)],
        out_specs=[whole(o.shape) for o in outs],
        out_shape=outs,
        scratch_shapes=list(scratch),
        compiler_params=pltpu.CompilerParams(vmem_limit_bytes=LIMITS[name] * 2**20),
        cost_estimate=pl.CostEstimate(flops=flops, transcendentals=0, bytes_accessed=moved),
    )(*args)


def far_of(shape, dtype):
    return pltpu.HBM(shape, dtype)


def shape_of(shape, dtype):
    return jax.ShapeDtypeStruct(shape, dtype)


def columns_of(array, lanes):
    return jnp.broadcast_to(jnp.pad(array, (0, 8 - array.shape[0]))[:, None], (8, lanes))


def padded(array, lanes):
    return jnp.pad(array, ((0, 0), (0, lanes - array.shape[1])))


def local(
    activations,
    norm_gain,
    pool_weight,
    gate_weight,
    value_weight,
    key_weight,
    read_weight,
    step_weight,
    pool_mix,
    pool_scale,
    taps_value,
    taps_key,
    taps_read,
    step_bias,
    decay_log,
    decay_extra,
    skip_scale,
    state_gain,
    out_pool_weight,
    out_state_weight,
):
    length, width = activations.shape
    mix = value_weight.shape[1]
    state = key_weight.shape[1]
    heads = step_weight.shape[1]
    count = lax.axis_size("tp")
    fill = jnp.zeros((read_weight.shape[0], BLOCK - state), BF16)
    joined = jnp.concatenate(
        [
            pool_weight,
            gate_weight,
            jnp.transpose(out_pool_weight),
            jnp.transpose(out_state_weight),
            read_weight,
            fill,
        ],
        axis=1,
    )
    later_weights = lax.all_gather(joined, SP, axis=0, tiled=True)
    fill = jnp.zeros((key_weight.shape[0], BLOCK - state - heads), BF16)
    first_weights = jnp.concatenate([value_weight, key_weight, step_weight, fill], axis=1)
    mine = sent_to_all(first_weights, ("sp_0", "sp_1"))
    other = lax.ppermute(mine, "sp_2", [(0, 1), (1, 0)])
    size = lax.axis_size(SP)
    before = lax.ppermute(activations[length - HALO :], SP, [(k, k + 1) for k in range(size - 1)])
    gains = jnp.broadcast_to(norm_gain[None, :], (PAY, width))
    sent = jnp.concatenate([before, activations, gains], axis=0)
    pieces = [sent]
    for shift in range(1, count):
        pairs = [(k, (k + shift) % count) for k in range(count)]
        pieces.append(lax.ppermute(sent, "tp", pairs))
    rows = HALO + length
    early = call(
        early_kernel, "early", (pieces[0], pieces[-1]), (far_of((rows, 1), F32),), 10**6
    )[0]
    normed = call(
        norm_kernel,
        "norm",
        (early, *pieces),
        (shape_of((count, rows, width), BF16),),
        10**6,
        far=range(5),
    )[0]
    lanes = mix + BLOCK
    params = jnp.concatenate(
        [
            padded(jnp.concatenate([taps_value, taps_key], axis=1), lanes),
            padded(taps_read, lanes),
            columns_of(step_bias, lanes),
            columns_of(-jnp.exp(decay_log), lanes),
            padded(jnp.repeat(skip_scale, HEAD)[None, :], lanes),
            padded(pool_scale[None, :], lanes),
            padded(state_gain[None, :], lanes),
            jnp.zeros((5, lanes), F32),
        ]
    )
    extra = jnp.pad(jnp.transpose(decay_extra), ((0, 8 - heads), (0, 0)))
    columns = mix + BLOCK
    pay = shape_of((HEAD + PAY, mix), BF16)
    value, key, cum, step, payload = call(
        first_kernel,
        "first",
        (normed, mine, other, params, extra),
        (
            far_of((length, mix), BF16),
            far_of((length, BLOCK), BF16),
            far_of((8, length), F32),
            far_of((8, length), F32),
            pay,
        ),
        2 * rows * D * columns,
        [pltpu.VMEM((mine.shape[0], 2, mine.shape[1], columns), BF16)],
        far=(3, 4),
    )
    row_pieces = lax.all_gather(payload, ("sp_1", "sp_2"))
    before_row, logs_row, payload = call(
        row_kernel,
        "row",
        (row_pieces,),
        (far_of((HEAD, mix), F32), far_of((8, mix), F32), pay),
        10**6,
    )
    plane_pieces = sent_to_all(payload, "sp_0")
    pool_out, gate, reads, inside = call(
        second_kernel,
        "second",
        (normed, later_weights, later_weights, value, key, cum, step, params, pool_mix[0]),
        (
            far_of((length, mix), BF16),
            far_of((length, mix), BF16),
            far_of((length, BLOCK), BF16),
            far_of((length, mix), F32),
        ),
        2 * rows * D * (2 * mix + BLOCK),
        specs={
            1: pl.BlockSpec((D, 2 * mix), lambda *_: (0, 0)),
            2: pl.BlockSpec((D, BLOCK), lambda *_: (0, 4 * mix // BLOCK)),
        },
        far=range(9),
    )
    gated, squares = call(
        third_kernel,
        "third",
        (plane_pieces, before_row, logs_row, reads, inside, gate, cum, params),
        (shape_of((length, mix), BF16), shape_of((8, length), F32)),
        10**7,
        far=range(1, 8),
    )
    all_squares = sent_to_all(squares, "tp")
    terms = call(
        out_kernel,
        "out",
        (pool_out, gated, all_squares, later_weights),
        (shape_of((count, length, width), BF16),),
        2 * length * 2 * mix * D,
        specs={3: pl.BlockSpec((D, 2 * mix), lambda *_: (0, 1))},
        far=(0, 3),
    )[0]
    arrived = lax.all_to_all(terms, "tp", split_axis=0, concat_axis=0, tiled=True)
    return arrived.astype(F32).sum(axis=0).astype(BF16)


def solution(mesh):
    torus = Mesh(mesh.devices.reshape(8, 8, 2, mesh.shape["tp"]), ("sp_0", "sp_1", "sp_2", "tp"))
    placed = (
        P(SP, "tp"),
        P("tp"),
        P(SP, "tp"),
        P(SP, "tp"),
        P(SP, "tp"),
        P(SP, "tp"),
        P(SP, "tp"),
        P(SP, "tp"),
        P("tp", None, None),
        P("tp"),
        P(None, "tp"),
        P(None, "tp"),
        P(None, "tp"),
        P("tp"),
        P("tp"),
        P(SP, "tp"),
        P("tp"),
        P("tp"),
        P("tp", SP),
        P("tp", SP),
    )
    return jax.shard_map(local, mesh=torus, in_specs=placed, out_specs=P(SP, "tp"), check_vma=False)
```

```python
import jax
import jax.numpy as jnp
from jax import lax
from jax.experimental import pallas as pl
from jax.experimental.pallas import tpu as pltpu
from jax.sharding import Mesh
from jax.sharding import PartitionSpec as P


D = 2048
POOL_GROUPS = 4
HEAD = 64
MIX_W = 1024
HALO = 16
PAY = 16
BLOCK = 128
SP = ("sp_0", "sp_1", "sp_2")
EPSILON = 1e-06
HIGH = lax.Precision.HIGHEST
F32 = jnp.float32
BF16 = jnp.bfloat16


def sent_to_all(array, axis):
    copies = jnp.broadcast_to(array, (lax.axis_size(axis), *array.shape))
    return lax.all_to_all(copies, axis, split_axis=0, concat_axis=0, tiled=True)


def dot(a, b, left=1, right=0, precision=None):
    return lax.dot_general(
        a, b, (((left,), (right,)), ((), ())), precision=precision, preferred_element_type=F32
    )


def silu(x):
    return x * jax.nn.sigmoid(x)


def heads_of_lanes(lanes):
    head = lax.broadcasted_iota(jnp.int32, (8, lanes), 0)
    lane = lax.broadcasted_iota(jnp.int32, (8, lanes), 1)
    return (head == lane // HEAD).astype(F32)


def convolved(raw, taps, length):
    width = taps.shape[0]
    total = jnp.zeros((length, raw.shape[1]), F32)
    for k in range(width):
        at = HALO - width + 1 + k
        total = total + taps[k : k + 1] * raw[at : at + length]
    return silu(total).astype(BF16)


def three_parts(row):
    high = row.astype(BF16).astype(F32)
    middle = (row - high).astype(BF16).astype(F32)
    low = row - high - middle
    at = lax.broadcasted_iota(jnp.int32, (PAY, row.shape[1]), 0)
    parts = jnp.where(at == 0, high, jnp.where(at == 1, middle, jnp.where(at == 2, low, 0.0)))
    return parts.astype(BF16)


def write_payload(ref, state, log_row):
    rows = state.shape[0]
    ref[:rows] = state.astype(BF16)
    ref[rows:] = three_parts(log_row)


def read_payload(ref, k):
    rows = ref.shape[1] - PAY
    tail = ref[k, rows:].astype(F32)
    return ref[k, :rows].astype(F32), jnp.sum(tail, axis=0, keepdims=True)


def scan_payloads(ref, place):
    rows, lanes = ref.shape[1] - PAY, ref.shape[2]
    total = before = jnp.zeros((rows, lanes), F32)
    logs = logs_before = jnp.zeros((1, lanes), F32)
    for k in range(ref.shape[0]):
        state, log_row = read_payload(ref, k)
        total = total * jnp.exp(log_row) + state
        logs = logs + log_row
        before = jnp.where(k < place, total, before)
        logs_before = jnp.where(k < place, logs, logs_before)
    return total, logs, before, logs_before


def squares_of(pieces, total_rows):
    squares = jnp.zeros((total_rows, 1), F32)
    for piece in pieces:
        values = piece[:total_rows].astype(F32)
        squares = squares + jnp.sum(values * values, axis=1, keepdims=True)
    return squares


def early_kernel(x0, x3, out):
    out[...] = squares_of((x0, x3), out.shape[0])


def norm_kernel(early, x0, x1, x2, x3, normed):
    total_rows = normed.shape[1]
    scale = lax.rsqrt((early[...] + squares_of((x1, x2), total_rows)) / D + EPSILON)
    for k, piece in enumerate((x0, x1, x2, x3)):
        gain = piece[total_rows : total_rows + 1].astype(F32)
        normed[k] = (piece[:total_rows].astype(F32) * scale * gain).astype(BF16)


def first_kernel(
    normed, mine, other, params, extra,
    value_out, key_out, cum_out, step_out, payload, weight,
):
    core = lax.axis_index("sp_2")
    place = lax.axis_index("tp")
    weight[:, pl.ds(core, 1)] = mine[...][:, None]
    weight[:, pl.ds(1 - core, 1)] = other[...][:, None]
    total_rows = normed.shape[1]
    length = total_rows - HALO
    chips, columns = weight.shape[0] // 4, weight.shape[3]
    acc = jnp.zeros((total_rows, columns), F32)
    for k in range(normed.shape[0]):
        block = weight[pl.ds(((place - k) & 3) * chips, chips)]
        acc = acc + dot(normed[k], block.reshape(-1, columns))
    mix = value_out.shape[1]
    done = convolved(acc.astype(BF16).astype(F32), params[:4], length)
    value_out[...] = done[:, :mix]
    key_out[...] = done[:, mix:]
    raw = jnp.transpose(acc[HALO:, mix:])[HEAD : HEAD + 8] + params[8:16, :1]
    step = jnp.maximum(raw, 0.0) + jnp.log1p(jnp.exp(-jnp.abs(raw)))
    decay = params[16:24, :1] * step + extra[...]
    rows = lax.broadcasted_iota(jnp.int32, (BLOCK, BLOCK), 0)
    upper = (rows <= lax.broadcasted_iota(jnp.int32, (BLOCK, BLOCK), 1)).astype(F32)
    carry, cums = jnp.zeros((8, 1), F32), []
    for b in range(length // BLOCK):
        cums.append(dot(decay[:, b * BLOCK : (b + 1) * BLOCK], upper, precision=HIGH) + carry)
        carry = cums[-1][:, BLOCK - 1 :]
    cum = jnp.concatenate(cums, axis=1)
    cum_out[...] = cum
    step_out[...] = step
    lanes = heads_of_lanes(mix)
    spread = dot(jnp.exp(carry - cum) * step, lanes, 0, 0, HIGH)
    state = dot(done[:, mix:].astype(F32), done[:, :mix].astype(F32) * spread, 0, 0, HIGH)
    write_payload(payload, state[:HEAD], jnp.sum(carry * lanes, axis=0, keepdims=True))


def row_kernel(rows, before_out, logs_out, payload):
    total, logs, before, logs_before = scan_payloads(rows, lax.axis_index(("sp_1", "sp_2")))
    before_out[...] = before
    logs_out[...] = jnp.broadcast_to(logs_before, logs_out.shape)
    write_payload(payload, total, logs)


def second_kernel(
    normed, weight, weight_read, value, key, cum, step, params, mix_weight,
    pool_out, gate_out, read_out, local_out,
):
    length, span = pool_out.shape
    place = lax.axis_index("tp")
    total_rows = normed.shape[1]
    acc = jnp.zeros((total_rows, weight.shape[1]), F32)
    acc_read = jnp.zeros((total_rows, weight_read.shape[1]), F32)
    width = normed.shape[2]
    for k in range(normed.shape[0]):
        start = pl.multiple_of(((place - k) & 3) * width, width)
        acc = acc + dot(normed[k], weight[pl.ds(start, width)])
        acc_read = acc_read + dot(normed[k], weight_read[pl.ds(start, width)])
    gate_out[...] = acc[HALO:, span:].astype(BF16)
    running = acc[:, :span].astype(BF16).astype(F32)
    own = running[HALO:]
    chosen = own
    for level in range(POOL_GROUPS):
        stride = 2**level
        running = running[stride:] + running[:-stride]
        chosen = jnp.where(place == level, running[running.shape[0] - length :], chosen)
    position = lax.axis_index(SP) * length + lax.broadcasted_iota(jnp.int32, (length, 1), 0) + 1
    counts = jnp.minimum(position, 2 << place).astype(F32)
    pooled = (chosen / counts - own).astype(BF16)
    pool_out[...] = (dot(pooled, mix_weight[...]) * params[25:26, :span]).astype(BF16)
    reads = convolved(acc_read.astype(BF16).astype(F32), params[4:8, :BLOCK], length)
    read_out[...] = reads
    lanes = heads_of_lanes(span)
    values = value[...].astype(F32)
    scaled = (values * dot(step[...], lanes, 0, 0, HIGH)).astype(BF16)
    columns = jnp.transpose(cum[...])
    lower = lax.broadcasted_iota(jnp.int32, (BLOCK, BLOCK), 0) >= lax.broadcasted_iota(
        jnp.int32, (BLOCK, BLOCK), 1
    )
    for i in range(length // BLOCK):
        here = slice(i * BLOCK, (i + 1) * BLOCK)
        products = [
            dot(reads[here], key[j * BLOCK : (j + 1) * BLOCK], 1, 1) for j in range(i + 1)
        ]
        results = []
        for h in range(span // HEAD):
            parts = []
            for j in range(i + 1):
                gap = columns[here, h : h + 1] - cum[h : h + 1, j * BLOCK : (j + 1) * BLOCK]
                if i == j:
                    gap = jnp.where(lower, gap, -jnp.inf)
                parts.append((products[j] * jnp.exp(gap)).astype(BF16))
            left = jnp.concatenate(parts, axis=1)
            right = scaled[: (i + 1) * BLOCK, h * HEAD : (h + 1) * HEAD]
            results.append(dot(left, right))
        local_out[here] = jnp.concatenate(results, axis=1) + params[24:25, :span] * values[here]


def third_kernel(planes, before, logs_before, reads, local_in, gate, cum, params, pool, out):
    _, _, earlier, _ = scan_payloads(planes, lax.axis_index("sp_0"))
    incoming = earlier * jnp.exp(logs_before[:1]) + before[...]
    length, span = local_in.shape
    lanes = heads_of_lanes(span)
    decay = dot(jnp.exp(cum[...]), lanes, 0, 0, HIGH)
    far = dot(reads[:, :HEAD].astype(F32), incoming, precision=HIGH) * decay
    gated = (local_in[...] + far) * silu(gate[...].astype(F32))
    ones = jnp.ones((8, span), F32)
    squares = dot(ones, gated * gated, 1, 1, HIGH)
    out[:length, :span] = pool[...]
    out[:length, span:] = (gated * params[26:27, :span]).astype(BF16)
    out[length:] = three_parts(squares[:1])


def out_kernel(rows, weight, out):
    length = out.shape[0]
    span = rows.shape[2] // 2
    count = rows.shape[0]
    halves = weight.shape[0] // (count * span)
    squares = jnp.zeros((1, length), F32)
    for j in range(count):
        parts = rows[j, length:].astype(F32)
        squares = squares + jnp.sum(parts, axis=0, keepdims=True)
    scale = lax.rsqrt(squares / MIX_W + EPSILON)
    scale = jnp.transpose(jnp.broadcast_to(scale, (8, length)))[:, :1]
    for half in range(halves):
        pooled = jnp.zeros((length, span), F32)
        states = jnp.zeros((length, span), F32)
        for j in range(count):
            first = (half * count + j) * span
            block = weight[first : first + span]
            pooled = pooled + dot(rows[j, :length, :span], block[:, :span], 1, 1)
            states = states + dot(rows[j, :length, span:], block[:, span:], 1, 1)
        out[:, half * span : (half + 1) * span] = (pooled + states * scale).astype(BF16)


def whole(shape):
    return pl.BlockSpec(shape, lambda *_: (0,) * len(shape))


LIMITS = {"early": 8, "norm": 16, "first": 16, "row": 6, "second": 24, "third": 10, "out": 16}


def call(kernel, name, args, outs, flops, scratch=(), specs=None, far=()):
    specs = specs or {}
    moved = sum(a.size * a.dtype.itemsize for a in args)
    args = [
        pltpu.with_memory_space_constraint(a, pltpu.HBM) if k in far else a
        for k, a in enumerate(args)
    ]
    return pl.pallas_call(
        kernel,
        grid=(1,),
        in_specs=[specs.get(k, whole(a.shape)) for k, a in enumerate(args)],
        out_specs=[whole(o.shape) for o in outs],
        out_shape=outs,
        scratch_shapes=list(scratch),
        compiler_params=pltpu.CompilerParams(vmem_limit_bytes=LIMITS[name] * 2**20),
        cost_estimate=pl.CostEstimate(flops=flops, transcendentals=0, bytes_accessed=moved),
    )(*args)


def far_of(shape, dtype):
    return pltpu.HBM(shape, dtype)


def shape_of(shape, dtype):
    return jax.ShapeDtypeStruct(shape, dtype)


def columns_of(array, lanes):
    return jnp.broadcast_to(jnp.pad(array, (0, 8 - array.shape[0]))[:, None], (8, lanes))


def padded(array, lanes):
    return jnp.pad(array, ((0, 0), (0, lanes - array.shape[1])))


def local(
    activations,
    norm_gain,
    pool_weight,
    gate_weight,
    value_weight,
    key_weight,
    read_weight,
    step_weight,
    pool_mix,
    pool_scale,
    taps_value,
    taps_key,
    taps_read,
    step_bias,
    decay_log,
    decay_extra,
    skip_scale,
    state_gain,
    out_pool_weight,
    out_state_weight,
):
    length, width = activations.shape
    mix = value_weight.shape[1]
    state = key_weight.shape[1]
    heads = step_weight.shape[1]
    count = lax.axis_size("tp")
    planes = lax.axis_size("sp_0")
    half = planes // count
    out_weights = lax.ppermute(
        jnp.transpose(jnp.concatenate([out_pool_weight, out_state_weight], axis=0)),
        ("sp_0", "tp"),
        [
            (z * count + x, (z % half * count + x) * count + z // half)
            for z in range(planes)
            for x in range(count)
        ],
    )
    fill = jnp.zeros((read_weight.shape[0], BLOCK - state), BF16)
    joined = jnp.concatenate(
        [
            pool_weight,
            gate_weight,
            out_weights,
            read_weight,
            fill,
        ],
        axis=1,
    )
    later_weights = lax.all_gather(joined, SP, axis=0, tiled=True)
    fill = jnp.zeros((key_weight.shape[0], BLOCK - state - heads), BF16)
    first_weights = jnp.concatenate([value_weight, key_weight, step_weight, fill], axis=1)
    mine = sent_to_all(first_weights, ("sp_0", "sp_1"))
    other = lax.ppermute(mine, "sp_2", [(0, 1), (1, 0)])
    size = lax.axis_size(SP)
    before = lax.ppermute(activations[length - HALO :], SP, [(k, k + 1) for k in range(size - 1)])
    gains = jnp.broadcast_to(norm_gain[None, :], (PAY, width))
    sent = jnp.concatenate([before, activations, gains], axis=0)
    pieces = [sent]
    for shift in range(1, count):
        pairs = [(k, (k + shift) % count) for k in range(count)]
        pieces.append(lax.ppermute(sent, "tp", pairs))
    rows = HALO + length
    early = call(
        early_kernel, "early", (pieces[0], pieces[-1]), (far_of((rows, 1), F32),), 10**6
    )[0]
    normed = call(
        norm_kernel,
        "norm",
        (early, *pieces),
        (shape_of((count, rows, width), BF16),),
        10**6,
        far=range(5),
    )[0]
    lanes = mix + BLOCK
    params = jnp.concatenate(
        [
            padded(jnp.concatenate([taps_value, taps_key], axis=1), lanes),
            padded(taps_read, lanes),
            columns_of(step_bias, lanes),
            columns_of(-jnp.exp(decay_log), lanes),
            padded(jnp.repeat(skip_scale, HEAD)[None, :], lanes),
            padded(pool_scale[None, :], lanes),
            padded(state_gain[None, :], lanes),
            jnp.zeros((5, lanes), F32),
        ]
    )
    extra = jnp.pad(jnp.transpose(decay_extra), ((0, 8 - heads), (0, 0)))
    columns = mix + BLOCK
    pay = shape_of((HEAD + PAY, mix), BF16)
    value, key, cum, step, payload = call(
        first_kernel,
        "first",
        (normed, mine, other, params, extra),
        (
            far_of((length, mix), BF16),
            far_of((length, BLOCK), BF16),
            far_of((8, length), F32),
            far_of((8, length), F32),
            pay,
        ),
        2 * rows * D * columns,
        [pltpu.VMEM((mine.shape[0], 2, mine.shape[1], columns), BF16)],
        far=(3, 4),
    )
    row_pieces = lax.all_gather(payload, ("sp_1", "sp_2"))
    before_row, logs_row, payload = call(
        row_kernel,
        "row",
        (row_pieces,),
        (far_of((HEAD, mix), F32), far_of((8, mix), F32), pay),
        10**6,
    )
    plane_pieces = sent_to_all(payload, "sp_0")
    pool_out, gate, reads, inside = call(
        second_kernel,
        "second",
        (normed, later_weights, later_weights, value, key, cum, step, params, pool_mix[0]),
        (
            far_of((length, mix), BF16),
            far_of((length, mix), BF16),
            far_of((length, BLOCK), BF16),
            far_of((length, mix), F32),
        ),
        2 * rows * D * (2 * mix + BLOCK),
        specs={
            1: pl.BlockSpec((D, 2 * mix), lambda *_: (0, 0)),
            2: pl.BlockSpec((D, BLOCK), lambda *_: (0, 4 * mix // BLOCK)),
        },
        far=range(9),
    )
    rows_here = call(
        third_kernel,
        "third",
        (plane_pieces, before_row, logs_row, reads, inside, gate, cum, params, pool_out),
        (shape_of((length + PAY, 2 * mix), BF16),),
        10**7,
        far=range(1, 9),
    )[0]
    all_rows = sent_to_all(rows_here, "tp")
    return call(
        out_kernel,
        "out",
        (all_rows, later_weights),
        (shape_of((length, width), BF16),),
        2 * length * 2 * mix * D,
        specs={1: pl.BlockSpec((D, 2 * mix), lambda *_: (0, 1))},
        far=(1,),
    )[0]


def solution(mesh):
    torus = Mesh(mesh.devices.reshape(8, 8, 2, mesh.shape["tp"]), ("sp_0", "sp_1", "sp_2", "tp"))
    placed = (
        P(SP, "tp"),
        P("tp"),
        P(SP, "tp"),
        P(SP, "tp"),
        P(SP, "tp"),
        P(SP, "tp"),
        P(SP, "tp"),
        P(SP, "tp"),
        P("tp", None, None),
        P("tp"),
        P(None, "tp"),
        P(None, "tp"),
        P(None, "tp"),
        P("tp"),
        P("tp"),
        P(SP, "tp"),
        P("tp"),
        P("tp"),
        P("tp", SP),
        P("tp", SP),
    )
    return jax.shard_map(local, mesh=torus, in_specs=placed, out_specs=P(SP, "tp"), check_vma=False)
```

```python
import jax
import jax.numpy as jnp
from jax import lax
from jax.experimental import pallas as pl
from jax.experimental.pallas import tpu as pltpu
from jax.sharding import Mesh
from jax.sharding import PartitionSpec as P


D = 2048
POOL_GROUPS = 4
HEAD = 64
MIX_W = 1024
HALO = 16
PAY = 16
BLOCK = 128
SP = ("sp_0", "sp_1", "sp_2")
EPSILON = 1e-06
HIGH = lax.Precision.HIGHEST
F32 = jnp.float32
BF16 = jnp.bfloat16


def sent_to_all(array, axis):
    copies = jnp.broadcast_to(array, (lax.axis_size(axis), *array.shape))
    return lax.all_to_all(copies, axis, split_axis=0, concat_axis=0, tiled=True)


def dot(a, b, left=1, right=0, precision=None):
    return lax.dot_general(
        a, b, (((left,), (right,)), ((), ())), precision=precision, preferred_element_type=F32
    )


def silu(x):
    return x * jax.nn.sigmoid(x)


def heads_of_lanes(lanes):
    head = lax.broadcasted_iota(jnp.int32, (8, lanes), 0)
    lane = lax.broadcasted_iota(jnp.int32, (8, lanes), 1)
    return (head == lane // HEAD).astype(F32)


def convolved(raw, taps, length):
    width = taps.shape[0]
    total = jnp.zeros((length, raw.shape[1]), F32)
    for k in range(width):
        at = HALO - width + 1 + k
        total = total + taps[k : k + 1] * raw[at : at + length]
    return silu(total).astype(BF16)


def write_payload(ref, state, log_row):
    rows = state.shape[0]
    high = log_row.astype(BF16).astype(F32)
    middle = (log_row - high).astype(BF16).astype(F32)
    low = log_row - high - middle
    at = lax.broadcasted_iota(jnp.int32, (PAY, log_row.shape[1]), 0)
    tail = jnp.where(at == 0, high, jnp.where(at == 1, middle, jnp.where(at == 2, low, 0.0)))
    ref[:rows] = state.astype(BF16)
    ref[rows:] = tail.astype(BF16)


def read_payload(ref, k):
    rows = ref.shape[1] - PAY
    tail = ref[k, rows:].astype(F32)
    return ref[k, :rows].astype(F32), jnp.sum(tail, axis=0, keepdims=True)


def scan_payloads(ref, place):
    rows, lanes = ref.shape[1] - PAY, ref.shape[2]
    total = before = jnp.zeros((rows, lanes), F32)
    logs = logs_before = jnp.zeros((1, lanes), F32)
    for k in range(ref.shape[0]):
        state, log_row = read_payload(ref, k)
        total = total * jnp.exp(log_row) + state
        logs = logs + log_row
        before = jnp.where(k < place, total, before)
        logs_before = jnp.where(k < place, logs, logs_before)
    return total, logs, before, logs_before


def squares_of(pieces, total_rows):
    squares = jnp.zeros((total_rows, 1), F32)
    for piece in pieces:
        values = piece[:total_rows].astype(F32)
        squares = squares + jnp.sum(values * values, axis=1, keepdims=True)
    return squares


def norm_kernel(x0, x1, x2, x3, normed):
    total_rows = normed.shape[1]
    scale = lax.rsqrt(squares_of((x0, x1, x2, x3), total_rows) / D + EPSILON)
    for k, piece in enumerate((x0, x1, x2, x3)):
        gain = piece[total_rows : total_rows + 1].astype(F32)
        normed[k] = (piece[:total_rows].astype(F32) * scale * gain).astype(BF16)


def first_kernel(
    normed, mine, other, params, extra,
    value_out, key_out, cum_out, step_out, payload, weight,
):
    core = lax.axis_index("sp_2")
    place = lax.axis_index("tp")
    weight[:, pl.ds(core, 1)] = mine[...][:, None]
    weight[:, pl.ds(1 - core, 1)] = other[...][:, None]
    total_rows = normed.shape[1]
    length = total_rows - HALO
    chips, columns = weight.shape[0] // 4, weight.shape[3]
    acc = jnp.zeros((total_rows, columns), F32)
    for k in range(normed.shape[0]):
        block = weight[pl.ds(((place - k) & 3) * chips, chips)]
        acc = acc + dot(normed[k], block.reshape(-1, columns))
    mix = value_out.shape[1]
    done = convolved(acc.astype(BF16).astype(F32), params[:4], length)
    value_out[...] = done[:, :mix]
    key_out[...] = done[:, mix:]
    raw = jnp.transpose(acc[HALO:, mix:])[HEAD : HEAD + 8] + params[8:16, :1]
    step = jnp.maximum(raw, 0.0) + jnp.log1p(jnp.exp(-jnp.abs(raw)))
    decay = params[16:24, :1] * step + extra[...]
    rows = lax.broadcasted_iota(jnp.int32, (BLOCK, BLOCK), 0)
    upper = (rows <= lax.broadcasted_iota(jnp.int32, (BLOCK, BLOCK), 1)).astype(F32)
    carry, cums = jnp.zeros((8, 1), F32), []
    for b in range(length // BLOCK):
        cums.append(dot(decay[:, b * BLOCK : (b + 1) * BLOCK], upper, precision=HIGH) + carry)
        carry = cums[-1][:, BLOCK - 1 :]
    cum = jnp.concatenate(cums, axis=1)
    cum_out[...] = cum
    step_out[...] = step
    lanes = heads_of_lanes(mix)
    spread = dot(jnp.exp(carry - cum) * step, lanes, 0, 0, HIGH)
    state = dot(done[:, mix:].astype(F32), done[:, :mix].astype(F32) * spread, 0, 0, HIGH)
    write_payload(payload, state[:HEAD], jnp.sum(carry * lanes, axis=0, keepdims=True))


def row_kernel(rows, before_out, logs_out, payload):
    total, logs, before, logs_before = scan_payloads(rows, lax.axis_index(("sp_1", "sp_2")))
    before_out[...] = before
    logs_out[...] = jnp.broadcast_to(logs_before, logs_out.shape)
    write_payload(payload, total, logs)


def inner_kernel(value, cum, step, factors, scaled):
    length, span = scaled.shape
    lanes = heads_of_lanes(span)
    scaled[...] = (value[...].astype(F32) * dot(step[...], lanes, 0, 0, HIGH)).astype(BF16)
    columns = jnp.transpose(cum[...])
    lower = lax.broadcasted_iota(jnp.int32, (BLOCK, BLOCK), 0) >= lax.broadcasted_iota(
        jnp.int32, (BLOCK, BLOCK), 1
    )
    at = 0
    for i in range(length // BLOCK):
        for h in range(span // HEAD):
            for j in range(i + 1):
                column = columns[i * BLOCK : (i + 1) * BLOCK, h : h + 1]
                gap = column - cum[h : h + 1, j * BLOCK : (j + 1) * BLOCK]
                if i == j:
                    gap = jnp.where(lower, gap, -jnp.inf)
                factors[at] = jnp.exp(gap)
                at = at + 1


def second_kernel(
    normed, weight, value, key, factors, scaled, params, mix_weight,
    pool_out, gate_out, read_out, local_out,
    rows_here, weight_here, read_here, arrived,
):
    length, span = pool_out.shape
    place = lax.axis_index("tp")
    count, total_rows, width = rows_here.shape
    copies = []
    for k in range(count):
        start = pl.multiple_of(((place - k) & 3) * width, width)
        block = weight.at[pl.ds(start, width)]
        copies.append(
            [
                pltpu.make_async_copy(normed.at[k], rows_here.at[k], arrived.at[k, 0]),
                pltpu.make_async_copy(
                    block.at[:, : 2 * span], weight_here.at[k], arrived.at[k, 1]
                ),
                pltpu.make_async_copy(
                    block.at[:, 4 * span :], read_here.at[k], arrived.at[k, 2]
                ),
            ]
        )
        for copy in copies[k]:
            copy.start()
    acc = jnp.zeros((total_rows, 2 * span), F32)
    acc_read = jnp.zeros((total_rows, BLOCK), F32)
    for k in range(count):
        for copy in copies[k]:
            copy.wait()
        acc = acc + dot(rows_here[k], weight_here[k])
        acc_read = acc_read + dot(rows_here[k], read_here[k])
    gate_out[...] = acc[HALO:, span:].astype(BF16)
    running = acc[:, :span].astype(BF16).astype(F32)
    own = running[HALO:]
    chosen = own
    for level in range(POOL_GROUPS):
        stride = 2**level
        running = running[stride:] + running[:-stride]
        chosen = jnp.where(place == level, running[running.shape[0] - length :], chosen)
    position = lax.axis_index(SP) * length + lax.broadcasted_iota(jnp.int32, (length, 1), 0) + 1
    counts = jnp.minimum(position, 2 << place).astype(F32)
    pooled = (chosen / counts - own).astype(BF16)
    pool_out[...] = (dot(pooled, mix_weight[...]) * params[25:26, :span]).astype(BF16)
    reads = convolved(acc_read.astype(BF16).astype(F32), params[4:8, :BLOCK], length)
    read_out[...] = reads
    at = 0
    for i in range(length // BLOCK):
        here = slice(i * BLOCK, (i + 1) * BLOCK)
        products = [
            dot(reads[here], key[j * BLOCK : (j + 1) * BLOCK], 1, 1) for j in range(i + 1)
        ]
        results = []
        for h in range(span // HEAD):
            parts = []
            for j in range(i + 1):
                parts.append((products[j] * factors[at]).astype(BF16))
                at = at + 1
            left = jnp.concatenate(parts, axis=1)
            results.append(dot(left, scaled[: (i + 1) * BLOCK, h * HEAD : (h + 1) * HEAD]))
        local_out[here] = jnp.concatenate(results, axis=1) + params[24:25, :span] * value[
            here
        ].astype(F32)


def third_kernel(
    planes, before, logs_before, reads, local_in, gate, cum, params, rows_out, squares_out
):
    _, _, earlier, _ = scan_payloads(planes, lax.axis_index("sp_0"))
    incoming = earlier * jnp.exp(logs_before[:1]) + before[...]
    lanes = heads_of_lanes(local_in.shape[1])
    decay = dot(jnp.exp(cum[...]), lanes, 0, 0, HIGH)
    far = dot(reads[:, :HEAD].astype(F32), incoming, precision=HIGH) * decay
    gated = (local_in[...] + far) * silu(gate[...].astype(F32))
    ones = jnp.ones((8, gated.shape[1]), F32)
    squares_out[...] = dot(ones, gated * gated, 1, 1, HIGH)
    rows_out[...] = (gated * params[26:27, : gated.shape[1]]).astype(BF16)


def out_kernel(pool, rows, weight, s0, s1, s2, s3, out):
    span = pool.shape[1]
    mean = (s0[...] + s1[...] + s2[...] + s3[...]) / MIX_W
    scale = jnp.transpose(lax.rsqrt(mean + EPSILON))[:, :1]
    for d in range(out.shape[0]):
        width = out.shape[2]
        block = weight[d * width : (d + 1) * width]
        terms = dot(pool[...], block[:, :span], 1, 1)
        terms = terms + dot(rows[...], block[:, span:], 1, 1) * scale
        out[d] = terms.astype(BF16)


def whole(shape):
    return pl.BlockSpec(shape, lambda *_: (0,) * len(shape))


LIMITS = {"inner": 24, "norm": 16, "first": 16, "row": 6, "second": 24, "third": 10, "out": 16}


def call(kernel, name, args, outs, flops, scratch=(), specs=None, far=()):
    specs = specs or {}
    moved = sum(a.size * a.dtype.itemsize for a in args)
    args = [
        pltpu.with_memory_space_constraint(a, pltpu.HBM) if k in far else a
        for k, a in enumerate(args)
    ]
    return pl.pallas_call(
        kernel,
        grid=(1,),
        in_specs=[specs.get(k, whole(a.shape)) for k, a in enumerate(args)],
        out_specs=[whole(o.shape) for o in outs],
        out_shape=outs,
        scratch_shapes=list(scratch),
        compiler_params=pltpu.CompilerParams(vmem_limit_bytes=LIMITS[name] * 2**20),
        cost_estimate=pl.CostEstimate(flops=flops, transcendentals=0, bytes_accessed=moved),
    )(*args)


def far_of(shape, dtype):
    return pltpu.HBM(shape, dtype)


def shape_of(shape, dtype):
    return jax.ShapeDtypeStruct(shape, dtype)


def columns_of(array, lanes):
    return jnp.broadcast_to(jnp.pad(array, (0, 8 - array.shape[0]))[:, None], (8, lanes))


def padded(array, lanes):
    return jnp.pad(array, ((0, 0), (0, lanes - array.shape[1])))


def local(
    activations,
    norm_gain,
    pool_weight,
    gate_weight,
    value_weight,
    key_weight,
    read_weight,
    step_weight,
    pool_mix,
    pool_scale,
    taps_value,
    taps_key,
    taps_read,
    step_bias,
    decay_log,
    decay_extra,
    skip_scale,
    state_gain,
    out_pool_weight,
    out_state_weight,
):
    length, width = activations.shape
    mix = value_weight.shape[1]
    state = key_weight.shape[1]
    heads = step_weight.shape[1]
    count = lax.axis_size("tp")
    fill = jnp.zeros((read_weight.shape[0], BLOCK - state), BF16)
    joined = jnp.concatenate(
        [
            pool_weight,
            gate_weight,
            jnp.transpose(out_pool_weight),
            jnp.transpose(out_state_weight),
            read_weight,
            fill,
        ],
        axis=1,
    )
    later_weights = lax.all_gather(joined, SP, axis=0, tiled=True)
    fill = jnp.zeros((key_weight.shape[0], BLOCK - state - heads), BF16)
    first_weights = jnp.concatenate([value_weight, key_weight, step_weight, fill], axis=1)
    mine = sent_to_all(first_weights, ("sp_0", "sp_1"))
    other = lax.ppermute(mine, "sp_2", [(0, 1), (1, 0)])
    size = lax.axis_size(SP)
    before = lax.ppermute(activations[length - HALO :], SP, [(k, k + 1) for k in range(size - 1)])
    gains = jnp.broadcast_to(norm_gain[None, :], (PAY, width))
    sent = jnp.concatenate([before, activations, gains], axis=0)
    pieces = [sent]
    for shift in range(1, count):
        pairs = [(k, (k + shift) % count) for k in range(count)]
        pieces.append(lax.ppermute(sent, "tp", pairs))
    rows = HALO + length
    normed = call(
        norm_kernel,
        "norm",
        pieces,
        (shape_of((count, rows, width), BF16),),
        10**6,
        far=range(4),
    )[0]
    lanes = mix + BLOCK
    params = jnp.concatenate(
        [
            padded(jnp.concatenate([taps_value, taps_key], axis=1), lanes),
            padded(taps_read, lanes),
            columns_of(step_bias, lanes),
            columns_of(-jnp.exp(decay_log), lanes),
            padded(jnp.repeat(skip_scale, HEAD)[None, :], lanes),
            padded(pool_scale[None, :], lanes),
            padded(state_gain[None, :], lanes),
            jnp.zeros((5, lanes), F32),
        ]
    )
    extra = jnp.pad(jnp.transpose(decay_extra), ((0, 8 - heads), (0, 0)))
    columns = mix + BLOCK
    pay = shape_of((HEAD + PAY, mix), BF16)
    value, key, cum, step, payload = call(
        first_kernel,
        "first",
        (normed, mine, other, params, extra),
        (
            far_of((length, mix), BF16),
            far_of((length, BLOCK), BF16),
            far_of((8, length), F32),
            far_of((8, length), F32),
            pay,
        ),
        2 * rows * D * columns,
        [pltpu.VMEM((mine.shape[0], 2, mine.shape[1], columns), BF16)],
        far=(3, 4),
    )
    row_pieces = lax.all_gather(payload, ("sp_1", "sp_2"))
    before_row, logs_row, payload = call(
        row_kernel,
        "row",
        (row_pieces,),
        (far_of((HEAD, mix), F32), far_of((8, mix), F32), pay),
        10**6,
    )
    plane_pieces = sent_to_all(payload, "sp_0")
    blocks = length // BLOCK
    factors, scaled = call(
        inner_kernel,
        "inner",
        (value, cum, step),
        (
            far_of((heads * blocks * (blocks + 1) // 2, BLOCK, BLOCK), F32),
            far_of((length, mix), BF16),
        ),
        10**7,
        far=range(3),
    )
    anywhere = pl.BlockSpec(memory_space=pl.ANY)
    pool_out, gate, reads, inside = call(
        second_kernel,
        "second",
        (normed, later_weights, value, key, factors, scaled, params, pool_mix[0]),
        (
            far_of((length, mix), BF16),
            far_of((length, mix), BF16),
            far_of((length, BLOCK), BF16),
            far_of((length, mix), F32),
        ),
        2 * rows * D * (2 * mix + BLOCK),
        [
            pltpu.VMEM((count, rows, width), BF16),
            pltpu.VMEM((count, width, 2 * mix), BF16),
            pltpu.VMEM((count, width, BLOCK), BF16),
            pltpu.SemaphoreType.DMA((count, 3)),
        ],
        specs={0: anywhere, 1: anywhere},
        far=range(8),
    )
    gated, squares = call(
        third_kernel,
        "third",
        (plane_pieces, before_row, logs_row, reads, inside, gate, cum, params),
        (shape_of((length, mix), BF16), shape_of((8, length), F32)),
        10**7,
        far=range(1, 8),
    )
    all_squares = [squares] + [
        lax.ppermute(squares, "tp", [(k, (k + shift) % count) for k in range(count)])
        for shift in range(1, count)
    ]
    terms = call(
        out_kernel,
        "out",
        (pool_out, gated, later_weights, *all_squares),
        (shape_of((count, length, width), BF16),),
        2 * length * 2 * mix * D,
        specs={2: pl.BlockSpec((D, 2 * mix), lambda *_: (0, 1))},
        far=(0, 2),
    )[0]
    arrived = lax.all_to_all(terms, "tp", split_axis=0, concat_axis=0, tiled=True)
    return arrived.astype(F32).sum(axis=0).astype(BF16)


def solution(mesh):
    torus = Mesh(mesh.devices.reshape(8, 8, 2, mesh.shape["tp"]), ("sp_0", "sp_1", "sp_2", "tp"))
    placed = (
        P(SP, "tp"),
        P("tp"),
        P(SP, "tp"),
        P(SP, "tp"),
        P(SP, "tp"),
        P(SP, "tp"),
        P(SP, "tp"),
        P(SP, "tp"),
        P("tp", None, None),
        P("tp"),
        P(None, "tp"),
        P(None, "tp"),
        P(None, "tp"),
        P("tp"),
        P("tp"),
        P(SP, "tp"),
        P("tp"),
        P("tp"),
        P("tp", SP),
        P("tp", SP),
    )
    return jax.shard_map(local, mesh=torus, in_specs=placed, out_specs=P(SP, "tp"), check_vma=False)
```

```python
import jax
import jax.numpy as jnp
from jax import lax
from jax.experimental import pallas as pl
from jax.experimental.pallas import tpu as pltpu
from jax.sharding import Mesh
from jax.sharding import PartitionSpec as P


D = 2048
POOL_GROUPS = 4
HEAD = 64
MIX_W = 1024
HALO = 16
PAY = 16
BLOCK = 128
SP = ("sp_0", "sp_1", "sp_2")
EPSILON = 1e-06
HIGH = lax.Precision.HIGHEST
F32 = jnp.float32
BF16 = jnp.bfloat16


def sent_to_all(array, axis):
    copies = jnp.broadcast_to(array, (lax.axis_size(axis), *array.shape))
    return lax.all_to_all(copies, axis, split_axis=0, concat_axis=0, tiled=True)


def dot(a, b, left=1, right=0, precision=None):
    return lax.dot_general(
        a, b, (((left,), (right,)), ((), ())), precision=precision, preferred_element_type=F32
    )


def silu(x):
    return x * jax.nn.sigmoid(x)


def heads_of_lanes(lanes):
    head = lax.broadcasted_iota(jnp.int32, (8, lanes), 0)
    lane = lax.broadcasted_iota(jnp.int32, (8, lanes), 1)
    return (head == lane // HEAD).astype(F32)


def convolved(raw, taps, length):
    width = taps.shape[0]
    total = jnp.zeros((length, raw.shape[1]), F32)
    for k in range(width):
        at = HALO - width + 1 + k
        total = total + taps[k : k + 1] * raw[at : at + length]
    return silu(total).astype(BF16)


def write_payload(ref, state, log_row):
    rows = state.shape[0]
    high = log_row.astype(BF16).astype(F32)
    middle = (log_row - high).astype(BF16).astype(F32)
    low = log_row - high - middle
    at = lax.broadcasted_iota(jnp.int32, (PAY, log_row.shape[1]), 0)
    tail = jnp.where(at == 0, high, jnp.where(at == 1, middle, jnp.where(at == 2, low, 0.0)))
    ref[:rows] = state.astype(BF16)
    ref[rows:] = tail.astype(BF16)


def read_payload(ref, k):
    rows = ref.shape[1] - PAY
    tail = ref[k, rows:].astype(F32)
    return ref[k, :rows].astype(F32), jnp.sum(tail, axis=0, keepdims=True)


def scan_payloads(ref, place):
    rows, lanes = ref.shape[1] - PAY, ref.shape[2]
    total = before = jnp.zeros((rows, lanes), F32)
    logs = logs_before = jnp.zeros((1, lanes), F32)
    for k in range(ref.shape[0]):
        state, log_row = read_payload(ref, k)
        total = total * jnp.exp(log_row) + state
        logs = logs + log_row
        before = jnp.where(k < place, total, before)
        logs_before = jnp.where(k < place, logs, logs_before)
    return total, logs, before, logs_before


def squares_of(pieces, total_rows):
    squares = jnp.zeros((total_rows, 1), F32)
    for piece in pieces:
        values = piece[:total_rows].astype(F32)
        squares = squares + jnp.sum(values * values, axis=1, keepdims=True)
    return squares


def norm_kernel(x0, x1, x2, x3, normed):
    total_rows = normed.shape[1]
    scale = lax.rsqrt(squares_of((x0, x1, x2, x3), total_rows) / D + EPSILON)
    for k, piece in enumerate((x0, x1, x2, x3)):
        gain = piece[total_rows : total_rows + 1].astype(F32)
        normed[k] = (piece[:total_rows].astype(F32) * scale * gain).astype(BF16)


def first_kernel(
    normed, mine, other, params, extra,
    value_out, key_out, cum_out, step_out, payload, weight,
):
    core = lax.axis_index("sp_2")
    place = lax.axis_index("tp")
    weight[:, pl.ds(core, 1)] = mine[...][:, None]
    weight[:, pl.ds(1 - core, 1)] = other[...][:, None]
    total_rows = normed.shape[1]
    length = total_rows - HALO
    chips, columns = weight.shape[0] // 4, weight.shape[3]
    acc = jnp.zeros((total_rows, columns), F32)
    for k in range(normed.shape[0]):
        block = weight[pl.ds(((place - k) & 3) * chips, chips)]
        acc = acc + dot(normed[k], block.reshape(-1, columns))
    mix = value_out.shape[1]
    done = convolved(acc.astype(BF16).astype(F32), params[:4], length)
    value_out[...] = done[:, :mix]
    key_out[...] = done[:, mix:]
    raw = jnp.transpose(acc[HALO:, mix:])[HEAD : HEAD + 8] + params[8:16, :1]
    step = jnp.maximum(raw, 0.0) + jnp.log1p(jnp.exp(-jnp.abs(raw)))
    decay = params[16:24, :1] * step + extra[...]
    rows = lax.broadcasted_iota(jnp.int32, (BLOCK, BLOCK), 0)
    upper = (rows <= lax.broadcasted_iota(jnp.int32, (BLOCK, BLOCK), 1)).astype(F32)
    carry, cums = jnp.zeros((8, 1), F32), []
    for b in range(length // BLOCK):
        cums.append(dot(decay[:, b * BLOCK : (b + 1) * BLOCK], upper, precision=HIGH) + carry)
        carry = cums[-1][:, BLOCK - 1 :]
    cum = jnp.concatenate(cums, axis=1)
    cum_out[...] = cum
    step_out[...] = step
    lanes = heads_of_lanes(mix)
    spread = dot(jnp.exp(carry - cum) * step, lanes, 0, 0, HIGH)
    state = dot(done[:, mix:].astype(F32), done[:, :mix].astype(F32) * spread, 0, 0, HIGH)
    write_payload(payload, state[:HEAD], jnp.sum(carry * lanes, axis=0, keepdims=True))


def row_kernel(rows, before_out, logs_out, payload):
    total, logs, before, logs_before = scan_payloads(rows, lax.axis_index(("sp_1", "sp_2")))
    before_out[...] = before
    logs_out[...] = jnp.broadcast_to(logs_before, logs_out.shape)
    write_payload(payload, total, logs)


def inner_kernel(value, cum, step, factors, scaled):
    length, span = scaled.shape
    lanes = heads_of_lanes(span)
    scaled[...] = (value[...].astype(F32) * dot(step[...], lanes, 0, 0, HIGH)).astype(BF16)
    columns = jnp.transpose(cum[...])
    lower = lax.broadcasted_iota(jnp.int32, (BLOCK, BLOCK), 0) >= lax.broadcasted_iota(
        jnp.int32, (BLOCK, BLOCK), 1
    )
    at = 0
    for i in range(length // BLOCK):
        for h in range(span // HEAD):
            for j in range(i + 1):
                column = columns[i * BLOCK : (i + 1) * BLOCK, h : h + 1]
                gap = column - cum[h : h + 1, j * BLOCK : (j + 1) * BLOCK]
                if i == j:
                    gap = jnp.where(lower, gap, -jnp.inf)
                factors[at] = jnp.exp(gap)
                at = at + 1


def block_products(normed, weight, rows_here, weight_here, arrived, lanes):
    place = lax.axis_index("tp")
    count, total_rows, width = rows_here.shape
    copies = []
    for k in range(count):
        start = pl.multiple_of(((place - k) & 3) * width, width)
        block = weight.at[pl.ds(start, width)]
        copies.append([pltpu.make_async_copy(normed.at[k], rows_here.at[k], arrived.at[k, 0])])
        for n, (first, size) in enumerate(lanes):
            copies[k].append(
                pltpu.make_async_copy(
                    block.at[:, first : first + size], weight_here[n].at[k], arrived.at[k, n + 1]
                )
            )
        for copy in copies[k]:
            copy.start()
    sums = [jnp.zeros((total_rows, size), F32) for _, size in lanes]
    for k in range(count):
        for copy in copies[k]:
            copy.wait()
        for n in range(len(lanes)):
            sums[n] = sums[n] + dot(rows_here[k], weight_here[n][k])
    return sums


def pool_kernel(normed, weight, params, mix_weight, pool_out, rows_here, weight_here, arrived):
    length, span = pool_out.shape
    place = lax.axis_index("tp")
    acc = block_products(normed, weight, rows_here, [weight_here], arrived, [(0, span)])[0]
    running = acc.astype(BF16).astype(F32)
    own = running[HALO:]
    chosen = own
    for level in range(POOL_GROUPS):
        stride = 2**level
        running = running[stride:] + running[:-stride]
        chosen = jnp.where(place == level, running[running.shape[0] - length :], chosen)
    position = lax.axis_index(SP) * length + lax.broadcasted_iota(jnp.int32, (length, 1), 0) + 1
    counts = jnp.minimum(position, 2 << place).astype(F32)
    pooled = (chosen / counts - own).astype(BF16)
    pool_out[...] = (dot(pooled, mix_weight[...]) * params[25:26, :span]).astype(BF16)


def second_kernel(
    normed, weight, value, key, factors_far, scaled, params,
    gate_out, read_out, local_out,
    rows_here, gate_here, read_here, factors, arrived, factors_arrived,
):
    length, span = gate_out.shape
    fetch = pltpu.make_async_copy(factors_far, factors, factors_arrived)
    fetch.start()
    lanes = [(span, span), (4 * span, BLOCK)]
    acc, acc_read = block_products(
        normed, weight, rows_here, [gate_here, read_here], arrived, lanes
    )
    gate_out[...] = acc[HALO:].astype(BF16)
    reads = convolved(acc_read.astype(BF16).astype(F32), params[4:8, :BLOCK], length)
    read_out[...] = reads
    fetch.wait()
    at = 0
    for i in range(length // BLOCK):
        here = slice(i * BLOCK, (i + 1) * BLOCK)
        products = [
            dot(reads[here], key[j * BLOCK : (j + 1) * BLOCK], 1, 1) for j in range(i + 1)
        ]
        results = []
        for h in range(span // HEAD):
            parts = []
            for j in range(i + 1):
                parts.append((products[j] * factors[at]).astype(BF16))
                at = at + 1
            left = jnp.concatenate(parts, axis=1)
            results.append(dot(left, scaled[: (i + 1) * BLOCK, h * HEAD : (h + 1) * HEAD]))
        local_out[here] = jnp.concatenate(results, axis=1) + params[24:25, :span] * value[
            here
        ].astype(F32)


def third_kernel(
    planes, before, logs_before, reads, local_in, gate, cum, params, rows_out, squares_out
):
    _, _, earlier, _ = scan_payloads(planes, lax.axis_index("sp_0"))
    incoming = earlier * jnp.exp(logs_before[:1]) + before[...]
    lanes = heads_of_lanes(local_in.shape[1])
    decay = dot(jnp.exp(cum[...]), lanes, 0, 0, HIGH)
    far = dot(reads[:, :HEAD].astype(F32), incoming, precision=HIGH) * decay
    gated = (local_in[...] + far) * silu(gate[...].astype(F32))
    ones = jnp.ones((8, gated.shape[1]), F32)
    squares_out[...] = dot(ones, gated * gated, 1, 1, HIGH)[:1]
    rows_out[...] = (gated * params[26:27, : gated.shape[1]]).astype(BF16)


def out_kernel(pool, rows, weight, squares, out):
    span = pool.shape[1]
    scale = lax.rsqrt(jnp.sum(squares[...], axis=0) / MIX_W + EPSILON)
    scale = jnp.transpose(jnp.broadcast_to(scale, (8, scale.shape[1])))[:, :1]
    for d in range(out.shape[0]):
        width = out.shape[2]
        block = weight[d * width : (d + 1) * width]
        terms = dot(pool[...], block[:, :span], 1, 1)
        terms = terms + dot(rows[...], block[:, span:], 1, 1) * scale
        out[d] = terms.astype(BF16)


def whole(shape):
    return pl.BlockSpec(shape, lambda *_: (0,) * len(shape))


LIMITS = {"pool": 16, "inner": 24, "norm": 16, "first": 16, "row": 6, "second": 24, "third": 10, "out": 16}


def call(kernel, name, args, outs, flops, scratch=(), specs=None, far=()):
    specs = specs or {}
    moved = sum(a.size * a.dtype.itemsize for a in args)
    args = [
        pltpu.with_memory_space_constraint(a, pltpu.HBM) if k in far else a
        for k, a in enumerate(args)
    ]
    return pl.pallas_call(
        kernel,
        grid=(1,),
        in_specs=[specs.get(k, whole(a.shape)) for k, a in enumerate(args)],
        out_specs=[whole(o.shape) for o in outs],
        out_shape=outs,
        scratch_shapes=list(scratch),
        compiler_params=pltpu.CompilerParams(vmem_limit_bytes=LIMITS[name] * 2**20),
        cost_estimate=pl.CostEstimate(flops=flops, transcendentals=0, bytes_accessed=moved),
    )(*args)


def far_of(shape, dtype):
    return pltpu.HBM(shape, dtype)


def shape_of(shape, dtype):
    return jax.ShapeDtypeStruct(shape, dtype)


def columns_of(array, lanes):
    return jnp.broadcast_to(jnp.pad(array, (0, 8 - array.shape[0]))[:, None], (8, lanes))


def padded(array, lanes):
    return jnp.pad(array, ((0, 0), (0, lanes - array.shape[1])))


def local(
    activations,
    norm_gain,
    pool_weight,
    gate_weight,
    value_weight,
    key_weight,
    read_weight,
    step_weight,
    pool_mix,
    pool_scale,
    taps_value,
    taps_key,
    taps_read,
    step_bias,
    decay_log,
    decay_extra,
    skip_scale,
    state_gain,
    out_pool_weight,
    out_state_weight,
):
    length, width = activations.shape
    mix = value_weight.shape[1]
    state = key_weight.shape[1]
    heads = step_weight.shape[1]
    count = lax.axis_size("tp")
    fill = jnp.zeros((read_weight.shape[0], BLOCK - state), BF16)
    joined = jnp.concatenate(
        [
            pool_weight,
            gate_weight,
            jnp.transpose(out_pool_weight),
            jnp.transpose(out_state_weight),
            read_weight,
            fill,
        ],
        axis=1,
    )
    later_weights = lax.all_gather(joined, SP, axis=0, tiled=True)
    fill = jnp.zeros((key_weight.shape[0], BLOCK - state - heads), BF16)
    first_weights = jnp.concatenate([value_weight, key_weight, step_weight, fill], axis=1)
    mine = sent_to_all(first_weights, ("sp_0", "sp_1"))
    other = lax.ppermute(mine, "sp_2", [(0, 1), (1, 0)])
    size = lax.axis_size(SP)
    before = lax.ppermute(activations[length - HALO :], SP, [(k, k + 1) for k in range(size - 1)])
    gains = jnp.broadcast_to(norm_gain[None, :], (PAY, width))
    sent = jnp.concatenate([before, activations, gains], axis=0)
    pieces = [sent]
    for shift in range(1, count):
        pairs = [(k, (k + shift) % count) for k in range(count)]
        pieces.append(lax.ppermute(sent, "tp", pairs))
    rows = HALO + length
    normed = call(
        norm_kernel,
        "norm",
        pieces,
        (shape_of((count, rows, width), BF16),),
        10**6,
        far=range(4),
    )[0]
    lanes = mix + BLOCK
    params = jnp.concatenate(
        [
            padded(jnp.concatenate([taps_value, taps_key], axis=1), lanes),
            padded(taps_read, lanes),
            columns_of(step_bias, lanes),
            columns_of(-jnp.exp(decay_log), lanes),
            padded(jnp.repeat(skip_scale, HEAD)[None, :], lanes),
            padded(pool_scale[None, :], lanes),
            padded(state_gain[None, :], lanes),
            jnp.zeros((5, lanes), F32),
        ]
    )
    extra = jnp.pad(jnp.transpose(decay_extra), ((0, 8 - heads), (0, 0)))
    columns = mix + BLOCK
    pay = shape_of((HEAD + PAY, mix), BF16)
    value, key, cum, step, payload = call(
        first_kernel,
        "first",
        (normed, mine, other, params, extra),
        (
            far_of((length, mix), BF16),
            far_of((length, BLOCK), BF16),
            far_of((8, length), F32),
            far_of((8, length), F32),
            pay,
        ),
        2 * rows * D * columns,
        [pltpu.VMEM((mine.shape[0], 2, mine.shape[1], columns), BF16)],
        far=(3, 4),
    )
    row_pieces = lax.all_gather(payload, ("sp_1", "sp_2"))
    before_row, logs_row, payload = call(
        row_kernel,
        "row",
        (row_pieces,),
        (far_of((HEAD, mix), F32), far_of((8, mix), F32), pay),
        10**6,
    )
    plane_pieces = sent_to_all(payload, "sp_0")
    blocks = length // BLOCK
    factors, scaled = call(
        inner_kernel,
        "inner",
        (value, cum, step),
        (
            far_of((heads * blocks * (blocks + 1) // 2, BLOCK, BLOCK), F32),
            far_of((length, mix), BF16),
        ),
        10**7,
        far=range(3),
    )
    anywhere = pl.BlockSpec(memory_space=pl.ANY)
    gate, reads, inside = call(
        second_kernel,
        "second",
        (normed, later_weights, value, key, factors, scaled, params),
        (
            far_of((length, mix), BF16),
            far_of((length, BLOCK), BF16),
            far_of((length, mix), F32),
        ),
        2 * rows * D * (mix + BLOCK),
        [
            pltpu.VMEM((count, rows, width), BF16),
            pltpu.VMEM((count, width, mix), BF16),
            pltpu.VMEM((count, width, BLOCK), BF16),
            pltpu.VMEM(factors.shape, F32),
            pltpu.SemaphoreType.DMA((count, 3)),
            pltpu.SemaphoreType.DMA,
        ],
        specs={0: anywhere, 1: anywhere, 4: anywhere},
        far=range(7),
    )
    pool_out = call(
        pool_kernel,
        "pool",
        (normed, later_weights, params, pool_mix[0]),
        (far_of((length, mix), BF16),),
        2 * rows * D * mix,
        [
            pltpu.VMEM((count, rows, width), BF16),
            pltpu.VMEM((count, width, mix), BF16),
            pltpu.SemaphoreType.DMA((count, 2)),
        ],
        specs={0: anywhere, 1: anywhere},
        far=range(4),
    )[0]
    gated, squares = call(
        third_kernel,
        "third",
        (plane_pieces, before_row, logs_row, reads, inside, gate, cum, params),
        (shape_of((length, mix), BF16), shape_of((1, length), F32)),
        10**7,
        far=range(1, 8),
    )
    all_squares = sent_to_all(squares, "tp")
    terms = call(
        out_kernel,
        "out",
        (pool_out, gated, later_weights, all_squares),
        (shape_of((count, length, width), BF16),),
        2 * length * 2 * mix * D,
        specs={2: pl.BlockSpec((D, 2 * mix), lambda *_: (0, 1))},
        far=(0, 2),
    )[0]
    arrived = lax.all_to_all(terms, "tp", split_axis=0, concat_axis=0, tiled=True)
    return arrived.astype(F32).sum(axis=0).astype(BF16)


def solution(mesh):
    torus = Mesh(mesh.devices.reshape(8, 8, 2, mesh.shape["tp"]), ("sp_0", "sp_1", "sp_2", "tp"))
    placed = (
        P(SP, "tp"),
        P("tp"),
        P(SP, "tp"),
        P(SP, "tp"),
        P(SP, "tp"),
        P(SP, "tp"),
        P(SP, "tp"),
        P(SP, "tp"),
        P("tp", None, None),
        P("tp"),
        P(None, "tp"),
        P(None, "tp"),
        P(None, "tp"),
        P("tp"),
        P("tp"),
        P(SP, "tp"),
        P("tp"),
        P("tp"),
        P("tp", SP),
        P("tp", SP),
    )
    return jax.shard_map(local, mesh=torus, in_specs=placed, out_specs=P(SP, "tp"), check_vma=False)
```

```python
import jax
import jax.numpy as jnp
from jax import lax
from jax.experimental import pallas as pl
from jax.experimental.pallas import tpu as pltpu
from jax.sharding import Mesh
from jax.sharding import PartitionSpec as P


D = 2048
POOL_GROUPS = 4
HEAD = 64
MIX_W = 1024
HALO = 16
PAY = 16
BLOCK = 128
SP = ("sp_0", "sp_1", "sp_2")
EPSILON = 1e-06
HIGH = lax.Precision.HIGHEST
F32 = jnp.float32
BF16 = jnp.bfloat16


def sent_to_all(array, axis):
    copies = jnp.broadcast_to(array, (lax.axis_size(axis), *array.shape))
    return lax.all_to_all(copies, axis, split_axis=0, concat_axis=0, tiled=True)


def dot(a, b, left=1, right=0, precision=None):
    return lax.dot_general(
        a, b, (((left,), (right,)), ((), ())), precision=precision, preferred_element_type=F32
    )


def silu(x):
    return x * jax.nn.sigmoid(x)


def heads_of_lanes(lanes):
    head = lax.broadcasted_iota(jnp.int32, (8, lanes), 0)
    lane = lax.broadcasted_iota(jnp.int32, (8, lanes), 1)
    return (head == lane // HEAD).astype(F32)


def convolved(raw, taps, length):
    width = taps.shape[0]
    total = jnp.zeros((length, raw.shape[1]), F32)
    for k in range(width):
        at = HALO - width + 1 + k
        total = total + taps[k : k + 1] * raw[at : at + length]
    return silu(total).astype(BF16)


def write_payload(ref, state, log_row):
    rows = state.shape[0]
    high = log_row.astype(BF16).astype(F32)
    middle = (log_row - high).astype(BF16).astype(F32)
    low = log_row - high - middle
    at = lax.broadcasted_iota(jnp.int32, (PAY, log_row.shape[1]), 0)
    tail = jnp.where(at == 0, high, jnp.where(at == 1, middle, jnp.where(at == 2, low, 0.0)))
    ref[:rows] = state.astype(BF16)
    ref[rows:] = tail.astype(BF16)


def read_payload(ref, k):
    rows = ref.shape[1] - PAY
    tail = ref[k, rows:].astype(F32)
    return ref[k, :rows].astype(F32), jnp.sum(tail, axis=0, keepdims=True)


def scan_payloads(ref, place):
    rows, lanes = ref.shape[1] - PAY, ref.shape[2]
    total = before = jnp.zeros((rows, lanes), F32)
    logs = logs_before = jnp.zeros((1, lanes), F32)
    for k in range(ref.shape[0]):
        state, log_row = read_payload(ref, k)
        total = total * jnp.exp(log_row) + state
        logs = logs + log_row
        before = jnp.where(k < place, total, before)
        logs_before = jnp.where(k < place, logs, logs_before)
    return total, logs, before, logs_before


def squares_of(pieces, total_rows):
    squares = jnp.zeros((total_rows, 1), F32)
    for piece in pieces:
        values = piece[:total_rows].astype(F32)
        squares = squares + jnp.sum(values * values, axis=1, keepdims=True)
    return squares


def norm_kernel(x0, x1, x2, x3, normed):
    total_rows = normed.shape[1]
    scale = lax.rsqrt(squares_of((x0, x1, x2, x3), total_rows) / D + EPSILON)
    for k, piece in enumerate((x0, x1, x2, x3)):
        gain = piece[total_rows : total_rows + 1].astype(F32)
        normed[k] = (piece[:total_rows].astype(F32) * scale * gain).astype(BF16)


def first_kernel(
    normed, mine, other, params, extra,
    value_out, key_out, cum_out, step_out, payload, weight,
):
    core = lax.axis_index("sp_2")
    place = lax.axis_index("tp")
    weight[:, pl.ds(core, 1)] = mine[...][:, None]
    weight[:, pl.ds(1 - core, 1)] = other[...][:, None]
    total_rows = normed.shape[1]
    length = total_rows - HALO
    chips, columns = weight.shape[0] // 4, weight.shape[3]
    acc = jnp.zeros((total_rows, columns), F32)
    for k in range(normed.shape[0]):
        block = weight[pl.ds(((place - k) & 3) * chips, chips)]
        acc = acc + dot(normed[k], block.reshape(-1, columns))
    mix = value_out.shape[1]
    done = convolved(acc.astype(BF16).astype(F32), params[:4], length)
    value_out[...] = done[:, :mix]
    key_out[...] = done[:, mix:]
    raw = jnp.transpose(acc[HALO:, mix:])[HEAD : HEAD + 8] + params[8:16, :1]
    step = jnp.maximum(raw, 0.0) + jnp.log1p(jnp.exp(-jnp.abs(raw)))
    decay = params[16:24, :1] * step + extra[...]
    rows = lax.broadcasted_iota(jnp.int32, (BLOCK, BLOCK), 0)
    upper = (rows <= lax.broadcasted_iota(jnp.int32, (BLOCK, BLOCK), 1)).astype(F32)
    carry, cums = jnp.zeros((8, 1), F32), []
    for b in range(length // BLOCK):
        cums.append(dot(decay[:, b * BLOCK : (b + 1) * BLOCK], upper, precision=HIGH) + carry)
        carry = cums[-1][:, BLOCK - 1 :]
    cum = jnp.concatenate(cums, axis=1)
    cum_out[...] = cum
    step_out[...] = step
    lanes = heads_of_lanes(mix)
    spread = dot(jnp.exp(carry - cum) * step, lanes, 0, 0, HIGH)
    state = dot(done[:, mix:].astype(F32), done[:, :mix].astype(F32) * spread, 0, 0, HIGH)
    write_payload(payload, state[:HEAD], jnp.sum(carry * lanes, axis=0, keepdims=True))


def row_kernel(rows, before_out, logs_out, payload):
    total, logs, before, logs_before = scan_payloads(rows, lax.axis_index(("sp_1", "sp_2")))
    before_out[...] = before
    logs_out[...] = jnp.broadcast_to(logs_before, logs_out.shape)
    write_payload(payload, total, logs)


def inner_kernel(value, cum, step, factors, scaled):
    length, span = scaled.shape
    lanes = heads_of_lanes(span)
    scaled[...] = (value[...].astype(F32) * dot(step[...], lanes, 0, 0, HIGH)).astype(BF16)
    columns = jnp.transpose(cum[...])
    lower = lax.broadcasted_iota(jnp.int32, (BLOCK, BLOCK), 0) >= lax.broadcasted_iota(
        jnp.int32, (BLOCK, BLOCK), 1
    )
    at = 0
    for i in range(length // BLOCK):
        for h in range(span // HEAD):
            for j in range(i + 1):
                column = columns[i * BLOCK : (i + 1) * BLOCK, h : h + 1]
                gap = column - cum[h : h + 1, j * BLOCK : (j + 1) * BLOCK]
                if i == j:
                    gap = jnp.where(lower, gap, -jnp.inf)
                factors[at] = jnp.exp(gap)
                at = at + 1


def block_products(normed, weight, rows_here, weight_here, arrived, lanes):
    place = lax.axis_index("tp")
    count, total_rows, width = rows_here.shape
    copies = []
    for k in range(count):
        start = pl.multiple_of(((place - k) & 3) * width, width)
        block = weight.at[pl.ds(start, width)]
        copies.append([pltpu.make_async_copy(normed.at[k], rows_here.at[k], arrived.at[k, 0])])
        for n, (first, size) in enumerate(lanes):
            copies[k].append(
                pltpu.make_async_copy(
                    block.at[:, first : first + size], weight_here[n].at[k], arrived.at[k, n + 1]
                )
            )
        for copy in copies[k]:
            copy.start()
    sums = [jnp.zeros((total_rows, size), F32) for _, size in lanes]
    for k in range(count):
        for copy in copies[k]:
            copy.wait()
        for n in range(len(lanes)):
            sums[n] = sums[n] + dot(rows_here[k], weight_here[n][k])
    return sums


def pool_kernel(normed, weight, params, mix_weight, pool_out, rows_here, weight_here, arrived):
    length, span = pool_out.shape
    place = lax.axis_index("tp")
    acc = block_products(normed, weight, rows_here, [weight_here], arrived, [(0, span)])[0]
    running = acc.astype(BF16).astype(F32)
    own = running[HALO:]
    chosen = own
    for level in range(POOL_GROUPS):
        stride = 2**level
        running = running[stride:] + running[:-stride]
        chosen = jnp.where(place == level, running[running.shape[0] - length :], chosen)
    position = lax.axis_index(SP) * length + lax.broadcasted_iota(jnp.int32, (length, 1), 0) + 1
    counts = jnp.minimum(position, 2 << place).astype(F32)
    pooled = (chosen / counts - own).astype(BF16)
    pool_out[...] = (dot(pooled, mix_weight[...]) * params[25:26, :span]).astype(BF16)


def second_kernel(
    normed, weight, value, key, factors_far, scaled, params, planes, before, logs_before, cum,
    rows_out, squares_out,
    rows_here, gate_here, read_here, factors, arrived, factors_arrived,
):
    length, span = rows_out.shape
    fetch = pltpu.make_async_copy(factors_far, factors, factors_arrived)
    fetch.start()
    lanes = [(span, span), (4 * span, BLOCK)]
    acc, acc_read = block_products(
        normed, weight, rows_here, [gate_here, read_here], arrived, lanes
    )
    gate = silu(acc[HALO:].astype(BF16).astype(F32))
    reads = convolved(acc_read.astype(BF16).astype(F32), params[4:8, :BLOCK], length)
    _, _, earlier, _ = scan_payloads(planes, lax.axis_index("sp_0"))
    incoming = earlier * jnp.exp(logs_before[:1]) + before[...]
    decay = dot(jnp.exp(cum[...]), heads_of_lanes(span), 0, 0, HIGH)
    far = dot(reads[:, :HEAD].astype(F32), incoming, precision=HIGH) * decay
    ones = jnp.ones((8, span), F32)
    fetch.wait()
    at = 0
    for i in range(length // BLOCK):
        here = slice(i * BLOCK, (i + 1) * BLOCK)
        products = [
            dot(reads[here], key[j * BLOCK : (j + 1) * BLOCK], 1, 1) for j in range(i + 1)
        ]
        results = []
        for h in range(span // HEAD):
            parts = []
            for j in range(i + 1):
                parts.append((products[j] * factors[at]).astype(BF16))
                at = at + 1
            left = jnp.concatenate(parts, axis=1)
            results.append(dot(left, scaled[: (i + 1) * BLOCK, h * HEAD : (h + 1) * HEAD]))
        near = jnp.concatenate(results, axis=1) + params[24:25, :span] * value[here].astype(F32)
        gated = (near + far[here]) * gate[here]
        squares_out[:, here] = dot(ones, gated * gated, 1, 1, HIGH)[:1]
        rows_out[here] = (gated * params[26:27, :span]).astype(BF16)


def out_kernel(pool, rows, weight, squares, out, weight_here, arrived):
    span = pool.shape[1]
    count, _, width = out.shape
    copies = [
        pltpu.make_async_copy(
            weight.at[pl.ds(d * width, width), pl.ds(2 * span, 2 * span)],
            weight_here.at[d],
            arrived.at[d],
        )
        for d in range(count)
    ]
    for copy in copies:
        copy.start()
    scale = lax.rsqrt(jnp.sum(squares[...], axis=0) / MIX_W + EPSILON)
    scale = jnp.transpose(jnp.broadcast_to(scale, (8, scale.shape[1])))[:, :1]
    for d in range(count):
        copies[d].wait()
        terms = dot(pool[...], weight_here[d, :, :span], 1, 1)
        terms = terms + dot(rows[...], weight_here[d, :, span:], 1, 1) * scale
        out[d] = terms.astype(BF16)


def whole(shape):
    return pl.BlockSpec(shape, lambda *_: (0,) * len(shape))


LIMITS = {"pool": 16, "inner": 24, "norm": 16, "first": 16, "row": 6, "second": 28, "out": 16}


def call(kernel, name, args, outs, flops, scratch=(), specs=None, far=()):
    specs = specs or {}
    moved = sum(a.size * a.dtype.itemsize for a in args)
    args = [
        pltpu.with_memory_space_constraint(a, pltpu.HBM) if k in far else a
        for k, a in enumerate(args)
    ]
    return pl.pallas_call(
        kernel,
        grid=(1,),
        in_specs=[specs.get(k, whole(a.shape)) for k, a in enumerate(args)],
        out_specs=[whole(o.shape) for o in outs],
        out_shape=outs,
        scratch_shapes=list(scratch),
        compiler_params=pltpu.CompilerParams(vmem_limit_bytes=LIMITS[name] * 2**20),
        cost_estimate=pl.CostEstimate(flops=flops, transcendentals=0, bytes_accessed=moved),
    )(*args)


def far_of(shape, dtype):
    return pltpu.HBM(shape, dtype)


def shape_of(shape, dtype):
    return jax.ShapeDtypeStruct(shape, dtype)


def columns_of(array, lanes):
    return jnp.broadcast_to(jnp.pad(array, (0, 8 - array.shape[0]))[:, None], (8, lanes))


def padded(array, lanes):
    return jnp.pad(array, ((0, 0), (0, lanes - array.shape[1])))


def local(
    activations,
    norm_gain,
    pool_weight,
    gate_weight,
    value_weight,
    key_weight,
    read_weight,
    step_weight,
    pool_mix,
    pool_scale,
    taps_value,
    taps_key,
    taps_read,
    step_bias,
    decay_log,
    decay_extra,
    skip_scale,
    state_gain,
    out_pool_weight,
    out_state_weight,
):
    length, width = activations.shape
    mix = value_weight.shape[1]
    state = key_weight.shape[1]
    heads = step_weight.shape[1]
    count = lax.axis_size("tp")
    fill = jnp.zeros((read_weight.shape[0], BLOCK - state), BF16)
    joined = jnp.concatenate(
        [
            pool_weight,
            gate_weight,
            jnp.transpose(out_pool_weight),
            jnp.transpose(out_state_weight),
            read_weight,
            fill,
        ],
        axis=1,
    )
    later_weights = lax.all_gather(joined, SP, axis=0, tiled=True)
    fill = jnp.zeros((key_weight.shape[0], BLOCK - state - heads), BF16)
    first_weights = jnp.concatenate([value_weight, key_weight, step_weight, fill], axis=1)
    mine = sent_to_all(first_weights, ("sp_0", "sp_1"))
    other = lax.ppermute(mine, "sp_2", [(0, 1), (1, 0)])
    size = lax.axis_size(SP)
    before = lax.ppermute(activations[length - HALO :], SP, [(k, k + 1) for k in range(size - 1)])
    gains = jnp.broadcast_to(norm_gain[None, :], (PAY, width))
    sent = jnp.concatenate([before, activations, gains], axis=0)
    pieces = [sent]
    for shift in range(1, count):
        pairs = [(k, (k + shift) % count) for k in range(count)]
        pieces.append(lax.ppermute(sent, "tp", pairs))
    rows = HALO + length
    normed = call(
        norm_kernel,
        "norm",
        pieces,
        (shape_of((count, rows, width), BF16),),
        10**6,
        far=range(4),
    )[0]
    lanes = mix + BLOCK
    params = jnp.concatenate(
        [
            padded(jnp.concatenate([taps_value, taps_key], axis=1), lanes),
            padded(taps_read, lanes),
            columns_of(step_bias, lanes),
            columns_of(-jnp.exp(decay_log), lanes),
            padded(jnp.repeat(skip_scale, HEAD)[None, :], lanes),
            padded(pool_scale[None, :], lanes),
            padded(state_gain[None, :], lanes),
            jnp.zeros((5, lanes), F32),
        ]
    )
    extra = jnp.pad(jnp.transpose(decay_extra), ((0, 8 - heads), (0, 0)))
    columns = mix + BLOCK
    pay = shape_of((HEAD + PAY, mix), BF16)
    value, key, cum, step, payload = call(
        first_kernel,
        "first",
        (normed, mine, other, params, extra),
        (
            far_of((length, mix), BF16),
            far_of((length, BLOCK), BF16),
            far_of((8, length), F32),
            far_of((8, length), F32),
            pay,
        ),
        2 * rows * D * columns,
        [pltpu.VMEM((mine.shape[0], 2, mine.shape[1], columns), BF16)],
        far=(3, 4),
    )
    row_pieces = lax.all_gather(payload, ("sp_1", "sp_2"))
    before_row, logs_row, payload = call(
        row_kernel,
        "row",
        (row_pieces,),
        (far_of((HEAD, mix), F32), far_of((8, mix), F32), pay),
        10**6,
    )
    plane_pieces = sent_to_all(payload, "sp_0")
    blocks = length // BLOCK
    factors, scaled = call(
        inner_kernel,
        "inner",
        (value, cum, step),
        (
            far_of((heads * blocks * (blocks + 1) // 2, BLOCK, BLOCK), F32),
            far_of((length, mix), BF16),
        ),
        10**7,
        far=range(3),
    )
    anywhere = pl.BlockSpec(memory_space=pl.ANY)
    gated, squares = call(
        second_kernel,
        "second",
        (
            normed, later_weights, value, key, factors, scaled, params,
            plane_pieces, before_row, logs_row, cum,
        ),
        (shape_of((length, mix), BF16), shape_of((1, length), F32)),
        2 * rows * D * (mix + BLOCK),
        [
            pltpu.VMEM((count, rows, width), BF16),
            pltpu.VMEM((count, width, mix), BF16),
            pltpu.VMEM((count, width, BLOCK), BF16),
            pltpu.VMEM(factors.shape, F32),
            pltpu.SemaphoreType.DMA((count, 3)),
            pltpu.SemaphoreType.DMA,
        ],
        specs={0: anywhere, 1: anywhere, 4: anywhere},
        far=(0, 1, 2, 3, 4, 5, 6, 8, 9, 10),
    )
    pool_out = call(
        pool_kernel,
        "pool",
        (normed, later_weights, params, pool_mix[0]),
        (far_of((length, mix), BF16),),
        2 * rows * D * mix,
        [
            pltpu.VMEM((count, rows, width), BF16),
            pltpu.VMEM((count, width, mix), BF16),
            pltpu.SemaphoreType.DMA((count, 2)),
        ],
        specs={0: anywhere, 1: anywhere},
        far=range(4),
    )[0]
    all_squares = sent_to_all(squares, "tp")
    terms = call(
        out_kernel,
        "out",
        (pool_out, gated, later_weights, all_squares),
        (shape_of((count, length, width), BF16),),
        2 * length * 2 * mix * D,
        [
            pltpu.VMEM((count, width, 2 * mix), BF16),
            pltpu.SemaphoreType.DMA((count,)),
        ],
        specs={2: anywhere},
        far=(0, 2),
    )[0]
    arrived = lax.all_to_all(terms, "tp", split_axis=0, concat_axis=0, tiled=True)
    return arrived.astype(F32).sum(axis=0).astype(BF16)


def solution(mesh):
    torus = Mesh(mesh.devices.reshape(8, 8, 2, mesh.shape["tp"]), ("sp_0", "sp_1", "sp_2", "tp"))
    placed = (
        P(SP, "tp"),
        P("tp"),
        P(SP, "tp"),
        P(SP, "tp"),
        P(SP, "tp"),
        P(SP, "tp"),
        P(SP, "tp"),
        P(SP, "tp"),
        P("tp", None, None),
        P("tp"),
        P(None, "tp"),
        P(None, "tp"),
        P(None, "tp"),
        P("tp"),
        P("tp"),
        P(SP, "tp"),
        P("tp"),
        P("tp"),
        P("tp", SP),
        P("tp", SP),
    )
    return jax.shard_map(local, mesh=torus, in_specs=placed, out_specs=P(SP, "tp"), check_vma=False)
```

```python
import jax
import jax.numpy as jnp
from jax import lax
from jax.experimental import pallas as pl
from jax.experimental.pallas import tpu as pltpu
from jax.sharding import Mesh
from jax.sharding import PartitionSpec as P


D = 2048
POOL_GROUPS = 4
HEAD = 64
MIX_W = 1024
HALO = 16
PAY = 16
BLOCK = 128
SP = ("sp_0", "sp_1", "sp_2")
EPSILON = 1e-06
HIGH = lax.Precision.HIGHEST
F32 = jnp.float32
BF16 = jnp.bfloat16


def sent_to_all(array, axis):
    copies = jnp.broadcast_to(array, (lax.axis_size(axis), *array.shape))
    return lax.all_to_all(copies, axis, split_axis=0, concat_axis=0, tiled=True)


def dot(a, b, left=1, right=0, precision=None):
    return lax.dot_general(
        a, b, (((left,), (right,)), ((), ())), precision=precision, preferred_element_type=F32
    )


def silu(x):
    return x * jax.nn.sigmoid(x)


def heads_of_lanes(lanes):
    head = lax.broadcasted_iota(jnp.int32, (8, lanes), 0)
    lane = lax.broadcasted_iota(jnp.int32, (8, lanes), 1)
    return (head == lane // HEAD).astype(F32)


def convolved(raw, taps, length):
    width = taps.shape[0]
    total = jnp.zeros((length, raw.shape[1]), F32)
    for k in range(width):
        at = HALO - width + 1 + k
        total = total + taps[k : k + 1] * raw[at : at + length]
    return silu(total).astype(BF16)


def write_payload(ref, state, log_row):
    rows = state.shape[0]
    high = log_row.astype(BF16).astype(F32)
    middle = (log_row - high).astype(BF16).astype(F32)
    low = log_row - high - middle
    at = lax.broadcasted_iota(jnp.int32, (PAY, log_row.shape[1]), 0)
    tail = jnp.where(at == 0, high, jnp.where(at == 1, middle, jnp.where(at == 2, low, 0.0)))
    ref[:rows] = state.astype(BF16)
    ref[rows:] = tail.astype(BF16)


def read_payload(ref, k):
    rows = ref.shape[1] - PAY
    tail = ref[k, rows:].astype(F32)
    return ref[k, :rows].astype(F32), jnp.sum(tail, axis=0, keepdims=True)


def scan_payloads(ref, place):
    rows, lanes = ref.shape[1] - PAY, ref.shape[2]
    total = before = jnp.zeros((rows, lanes), F32)
    logs = logs_before = jnp.zeros((1, lanes), F32)
    for k in range(ref.shape[0]):
        state, log_row = read_payload(ref, k)
        total = total * jnp.exp(log_row) + state
        logs = logs + log_row
        before = jnp.where(k < place, total, before)
        logs_before = jnp.where(k < place, logs, logs_before)
    return total, logs, before, logs_before


def squares_of(pieces, total_rows):
    squares = jnp.zeros((total_rows, 1), F32)
    for piece in pieces:
        values = piece[:total_rows].astype(F32)
        squares = squares + jnp.sum(values * values, axis=1, keepdims=True)
    return squares


def norm_kernel(x0, x1, x2, x3, normed):
    total_rows = normed.shape[1]
    scale = lax.rsqrt(squares_of((x0, x1, x2, x3), total_rows) / D + EPSILON)
    for k, piece in enumerate((x0, x1, x2, x3)):
        gain = piece[total_rows : total_rows + 1].astype(F32)
        normed[k] = (piece[:total_rows].astype(F32) * scale * gain).astype(BF16)


def first_kernel(
    normed, mine, other, params, extra,
    value_out, key_out, cum_out, step_out, payload, weight,
):
    core = lax.axis_index("sp_2")
    place = lax.axis_index("tp")
    weight[:, pl.ds(core, 1)] = mine[...][:, None]
    weight[:, pl.ds(1 - core, 1)] = other[...][:, None]
    total_rows = normed.shape[1]
    length = total_rows - HALO
    chips, columns = weight.shape[0] // 4, weight.shape[3]
    acc = jnp.zeros((total_rows, columns), F32)
    for k in range(normed.shape[0]):
        block = weight[pl.ds(((place - k) & 3) * chips, chips)]
        acc = acc + dot(normed[k], block.reshape(-1, columns))
    mix = value_out.shape[1]
    done = convolved(acc.astype(BF16).astype(F32), params[:4], length)
    value_out[...] = done[:, :mix]
    key_out[...] = done[:, mix:]
    raw = jnp.transpose(acc[HALO:, mix:])[HEAD : HEAD + 8] + params[8:16, :1]
    step = jnp.maximum(raw, 0.0) + jnp.log1p(jnp.exp(-jnp.abs(raw)))
    decay = params[16:24, :1] * step + extra[...]
    rows = lax.broadcasted_iota(jnp.int32, (BLOCK, BLOCK), 0)
    upper = (rows <= lax.broadcasted_iota(jnp.int32, (BLOCK, BLOCK), 1)).astype(F32)
    carry, cums = jnp.zeros((8, 1), F32), []
    for b in range(length // BLOCK):
        cums.append(dot(decay[:, b * BLOCK : (b + 1) * BLOCK], upper, precision=HIGH) + carry)
        carry = cums[-1][:, BLOCK - 1 :]
    cum = jnp.concatenate(cums, axis=1)
    cum_out[...] = cum
    step_out[...] = step
    lanes = heads_of_lanes(mix)
    spread = dot(jnp.exp(carry - cum) * step, lanes, 0, 0, HIGH)
    state = dot(done[:, mix:].astype(F32), done[:, :mix].astype(F32) * spread, 0, 0, HIGH)
    write_payload(payload, state[:HEAD], jnp.sum(carry * lanes, axis=0, keepdims=True))


def row_kernel(rows, before_out, logs_out, payload):
    total, logs, before, logs_before = scan_payloads(rows, lax.axis_index(("sp_1", "sp_2")))
    before_out[...] = before
    logs_out[...] = jnp.broadcast_to(logs_before, logs_out.shape)
    write_payload(payload, total, logs)


def inner_kernel(value, cum, step, factors, scaled):
    length, span = scaled.shape
    lanes = heads_of_lanes(span)
    scaled[...] = (value[...].astype(F32) * dot(step[...], lanes, 0, 0, HIGH)).astype(BF16)
    columns = jnp.transpose(cum[...])
    lower = lax.broadcasted_iota(jnp.int32, (BLOCK, BLOCK), 0) >= lax.broadcasted_iota(
        jnp.int32, (BLOCK, BLOCK), 1
    )
    at = 0
    for i in range(length // BLOCK):
        for h in range(span // HEAD):
            for j in range(i + 1):
                column = columns[i * BLOCK : (i + 1) * BLOCK, h : h + 1]
                gap = column - cum[h : h + 1, j * BLOCK : (j + 1) * BLOCK]
                if i == j:
                    gap = jnp.where(lower, gap, -jnp.inf)
                factors[at] = jnp.exp(gap)
                at = at + 1


def block_products(normed, weight, rows_here, weight_here, arrived, lanes, later=()):
    place = lax.axis_index("tp")
    count, total_rows, width = rows_here.shape
    copies = []
    for k in range(count):
        start = pl.multiple_of(((place - k) & 3) * width, width)
        block = weight.at[pl.ds(start, width)]
        copies.append([pltpu.make_async_copy(normed.at[k], rows_here.at[k], arrived.at[k, 0])])
        for n, (first, size) in enumerate(lanes):
            copies[k].append(
                pltpu.make_async_copy(
                    block.at[:, first : first + size], weight_here[n].at[k], arrived.at[k, n + 1]
                )
            )
        for copy in copies[k]:
            copy.start()
    for copy in later:
        copy.start()
    sums = [jnp.zeros((total_rows, size), F32) for _, size in lanes]
    for k in range(count):
        for copy in copies[k]:
            copy.wait()
        for n in range(len(lanes)):
            sums[n] = sums[n] + dot(rows_here[k], weight_here[n][k])
    return sums


def pool_kernel(normed, weight, params, mix_weight, pool_out, rows_here, weight_here, arrived):
    length, span = pool_out.shape
    place = lax.axis_index("tp")
    acc = block_products(normed, weight, rows_here, [weight_here], arrived, [(0, span)])[0]
    running = acc.astype(BF16).astype(F32)
    own = running[HALO:]
    chosen = own
    for level in range(POOL_GROUPS):
        stride = 2**level
        running = running[stride:] + running[:-stride]
        chosen = jnp.where(place == level, running[running.shape[0] - length :], chosen)
    position = lax.axis_index(SP) * length + lax.broadcasted_iota(jnp.int32, (length, 1), 0) + 1
    counts = jnp.minimum(position, 2 << place).astype(F32)
    pooled = (chosen / counts - own).astype(BF16)
    pool_out[...] = (dot(pooled, mix_weight[...]) * params[25:26, :span]).astype(BF16)


def second_kernel(
    normed, weight, value, key, factors_far, scaled, params, planes, before, logs_before, cum,
    rows_out, squares_out,
    rows_here, gate_here, read_here, factors, arrived, factors_arrived,
):
    length, span = rows_out.shape
    fetch = pltpu.make_async_copy(factors_far, factors, factors_arrived)
    lanes = [(span, span), (4 * span, BLOCK)]
    acc, acc_read = block_products(
        normed, weight, rows_here, [gate_here, read_here], arrived, lanes, [fetch]
    )
    gate = silu(acc[HALO:].astype(BF16).astype(F32))
    reads = convolved(acc_read.astype(BF16).astype(F32), params[4:8, :BLOCK], length)
    _, _, earlier, _ = scan_payloads(planes, lax.axis_index("sp_0"))
    incoming = earlier * jnp.exp(logs_before[:1]) + before[...]
    decay = dot(jnp.exp(cum[...]), heads_of_lanes(span), 0, 0, HIGH)
    far = dot(reads[:, :HEAD].astype(F32), incoming, precision=HIGH) * decay
    ones = jnp.ones((8, span), F32)
    fetch.wait()
    at = 0
    for i in range(length // BLOCK):
        here = slice(i * BLOCK, (i + 1) * BLOCK)
        products = [
            dot(reads[here], key[j * BLOCK : (j + 1) * BLOCK], 1, 1) for j in range(i + 1)
        ]
        results = []
        for h in range(span // HEAD):
            parts = []
            for j in range(i + 1):
                parts.append((products[j] * factors[at]).astype(BF16))
                at = at + 1
            left = jnp.concatenate(parts, axis=1)
            results.append(dot(left, scaled[: (i + 1) * BLOCK, h * HEAD : (h + 1) * HEAD]))
        near = jnp.concatenate(results, axis=1) + params[24:25, :span] * value[here].astype(F32)
        gated = (near + far[here]) * gate[here]
        squares_out[:, here] = dot(ones, gated * gated, 1, 1, HIGH)[:1]
        rows_out[here] = (gated * params[26:27, :span]).astype(BF16)


def out_kernel(pool, rows, weight, squares, out):
    span = pool.shape[1]
    scale = lax.rsqrt(jnp.sum(squares[...], axis=0) / MIX_W + EPSILON)
    scale = jnp.transpose(jnp.broadcast_to(scale, (8, scale.shape[1])))[:, :1]
    for d in range(out.shape[0]):
        width = out.shape[2]
        block = weight[d * width : (d + 1) * width]
        terms = dot(pool[...], block[:, :span], 1, 1)
        terms = terms + dot(rows[...], block[:, span:], 1, 1) * scale
        out[d] = terms.astype(BF16)


def whole(shape):
    return pl.BlockSpec(shape, lambda *_: (0,) * len(shape))


LIMITS = {"pool": 16, "inner": 24, "norm": 16, "first": 16, "row": 6, "second": 28, "out": 16}


def call(kernel, name, args, outs, flops, scratch=(), specs=None, far=()):
    specs = specs or {}
    moved = sum(a.size * a.dtype.itemsize for a in args)
    args = [
        pltpu.with_memory_space_constraint(a, pltpu.HBM) if k in far else a
        for k, a in enumerate(args)
    ]
    return pl.pallas_call(
        kernel,
        grid=(1,),
        in_specs=[specs.get(k, whole(a.shape)) for k, a in enumerate(args)],
        out_specs=[whole(o.shape) for o in outs],
        out_shape=outs,
        scratch_shapes=list(scratch),
        compiler_params=pltpu.CompilerParams(vmem_limit_bytes=LIMITS[name] * 2**20),
        cost_estimate=pl.CostEstimate(flops=flops, transcendentals=0, bytes_accessed=moved),
    )(*args)


def far_of(shape, dtype):
    return pltpu.HBM(shape, dtype)


def shape_of(shape, dtype):
    return jax.ShapeDtypeStruct(shape, dtype)


def columns_of(array, lanes):
    return jnp.broadcast_to(jnp.pad(array, (0, 8 - array.shape[0]))[:, None], (8, lanes))


def padded(array, lanes):
    return jnp.pad(array, ((0, 0), (0, lanes - array.shape[1])))


def local(
    activations,
    norm_gain,
    pool_weight,
    gate_weight,
    value_weight,
    key_weight,
    read_weight,
    step_weight,
    pool_mix,
    pool_scale,
    taps_value,
    taps_key,
    taps_read,
    step_bias,
    decay_log,
    decay_extra,
    skip_scale,
    state_gain,
    out_pool_weight,
    out_state_weight,
):
    length, width = activations.shape
    mix = value_weight.shape[1]
    state = key_weight.shape[1]
    heads = step_weight.shape[1]
    count = lax.axis_size("tp")
    fill = jnp.zeros((read_weight.shape[0], BLOCK - state), BF16)
    joined = jnp.concatenate(
        [
            pool_weight,
            gate_weight,
            jnp.transpose(out_pool_weight),
            jnp.transpose(out_state_weight),
            read_weight,
            fill,
        ],
        axis=1,
    )
    later_weights = lax.all_gather(joined, SP, axis=0, tiled=True)
    fill = jnp.zeros((key_weight.shape[0], BLOCK - state - heads), BF16)
    first_weights = jnp.concatenate([value_weight, key_weight, step_weight, fill], axis=1)
    mine = sent_to_all(first_weights, ("sp_0", "sp_1"))
    other = lax.ppermute(mine, "sp_2", [(0, 1), (1, 0)])
    size = lax.axis_size(SP)
    before = lax.ppermute(activations[length - HALO :], SP, [(k, k + 1) for k in range(size - 1)])
    gains = jnp.broadcast_to(norm_gain[None, :], (PAY, width))
    sent = jnp.concatenate([before, activations, gains], axis=0)
    pieces = [sent]
    for shift in range(1, count):
        pairs = [(k, (k + shift) % count) for k in range(count)]
        pieces.append(lax.ppermute(sent, "tp", pairs))
    rows = HALO + length
    normed = call(
        norm_kernel,
        "norm",
        pieces,
        (shape_of((count, rows, width), BF16),),
        10**6,
        far=range(4),
    )[0]
    lanes = mix + BLOCK
    params = jnp.concatenate(
        [
            padded(jnp.concatenate([taps_value, taps_key], axis=1), lanes),
            padded(taps_read, lanes),
            columns_of(step_bias, lanes),
            columns_of(-jnp.exp(decay_log), lanes),
            padded(jnp.repeat(skip_scale, HEAD)[None, :], lanes),
            padded(pool_scale[None, :], lanes),
            padded(state_gain[None, :], lanes),
            jnp.zeros((5, lanes), F32),
        ]
    )
    extra = jnp.pad(jnp.transpose(decay_extra), ((0, 8 - heads), (0, 0)))
    columns = mix + BLOCK
    pay = shape_of((HEAD + PAY, mix), BF16)
    value, key, cum, step, payload = call(
        first_kernel,
        "first",
        (normed, mine, other, params, extra),
        (
            far_of((length, mix), BF16),
            far_of((length, BLOCK), BF16),
            far_of((8, length), F32),
            far_of((8, length), F32),
            pay,
        ),
        2 * rows * D * columns,
        [pltpu.VMEM((mine.shape[0], 2, mine.shape[1], columns), BF16)],
        far=(3, 4),
    )
    row_pieces = lax.all_gather(payload, ("sp_1", "sp_2"))
    before_row, logs_row, payload = call(
        row_kernel,
        "row",
        (row_pieces,),
        (far_of((HEAD, mix), F32), far_of((8, mix), F32), pay),
        10**6,
    )
    plane_pieces = sent_to_all(payload, "sp_0")
    blocks = length // BLOCK
    factors, scaled = call(
        inner_kernel,
        "inner",
        (value, cum, step),
        (
            far_of((heads * blocks * (blocks + 1) // 2, BLOCK, BLOCK), F32),
            far_of((length, mix), BF16),
        ),
        10**7,
        far=range(3),
    )
    anywhere = pl.BlockSpec(memory_space=pl.ANY)
    gated, squares = call(
        second_kernel,
        "second",
        (
            normed, later_weights, value, key, factors, scaled, params,
            plane_pieces, before_row, logs_row, cum,
        ),
        (shape_of((length, mix), BF16), shape_of((1, length), F32)),
        2 * rows * D * (mix + BLOCK),
        [
            pltpu.VMEM((count, rows, width), BF16),
            pltpu.VMEM((count, width, mix), BF16),
            pltpu.VMEM((count, width, BLOCK), BF16),
            pltpu.VMEM(factors.shape, F32),
            pltpu.SemaphoreType.DMA((count, 3)),
            pltpu.SemaphoreType.DMA,
        ],
        specs={0: anywhere, 1: anywhere, 4: anywhere},
        far=(0, 1, 2, 3, 4, 5, 6, 8, 9, 10),
    )
    pool_out = call(
        pool_kernel,
        "pool",
        (normed, later_weights, params, pool_mix[0]),
        (far_of((length, mix), BF16),),
        2 * rows * D * mix,
        [
            pltpu.VMEM((count, rows, width), BF16),
            pltpu.VMEM((count, width, mix), BF16),
            pltpu.SemaphoreType.DMA((count, 2)),
        ],
        specs={0: anywhere, 1: anywhere},
        far=range(4),
    )[0]
    all_squares = sent_to_all(squares, "tp")
    terms = call(
        out_kernel,
        "out",
        (pool_out, gated, later_weights, all_squares),
        (shape_of((count, length, width), BF16),),
        2 * length * 2 * mix * D,
        specs={2: pl.BlockSpec((D, 2 * mix), lambda *_: (0, 1))},
        far=(0, 2),
    )[0]
    arrived = lax.all_to_all(terms, "tp", split_axis=0, concat_axis=0, tiled=True)
    return arrived.astype(F32).sum(axis=0).astype(BF16)


def solution(mesh):
    torus = Mesh(mesh.devices.reshape(8, 8, 2, mesh.shape["tp"]), ("sp_0", "sp_1", "sp_2", "tp"))
    placed = (
        P(SP, "tp"),
        P("tp"),
        P(SP, "tp"),
        P(SP, "tp"),
        P(SP, "tp"),
        P(SP, "tp"),
        P(SP, "tp"),
        P(SP, "tp"),
        P("tp", None, None),
        P("tp"),
        P(None, "tp"),
        P(None, "tp"),
        P(None, "tp"),
        P("tp"),
        P("tp"),
        P(SP, "tp"),
        P("tp"),
        P("tp"),
        P("tp", SP),
        P("tp", SP),
    )
    return jax.shard_map(local, mesh=torus, in_specs=placed, out_specs=P(SP, "tp"), check_vma=False)
```

```python
import jax
import jax.numpy as jnp
from jax import lax
from jax.experimental import pallas as pl
from jax.experimental.pallas import tpu as pltpu
from jax.sharding import Mesh
from jax.sharding import PartitionSpec as P


D = 2048
HEAD = 64
MIX_W = 1024
HALO = 16
PAY = 16
BLOCK = 128
SP = ("sp_0", "sp_1", "sp_2")
EPSILON = 1e-06
HIGH = lax.Precision.HIGHEST
F32 = jnp.float32
BF16 = jnp.bfloat16


def sent_to_all(array, axis):
    copies = jnp.broadcast_to(array, (lax.axis_size(axis), *array.shape))
    return lax.all_to_all(copies, axis, split_axis=0, concat_axis=0, tiled=True)


def dot(a, b, left=1, right=0, precision=None):
    return lax.dot_general(
        a, b, (((left,), (right,)), ((), ())), precision=precision, preferred_element_type=F32
    )


def silu(x):
    return x * jax.nn.sigmoid(x)


def heads_of_lanes(lanes):
    head = lax.broadcasted_iota(jnp.int32, (8, lanes), 0)
    lane = lax.broadcasted_iota(jnp.int32, (8, lanes), 1)
    return (head == lane // HEAD).astype(F32)


def convolved(raw, taps, length):
    width = taps.shape[0]
    total = jnp.zeros((length, raw.shape[1]), F32)
    for k in range(width):
        at = HALO - width + 1 + k
        total = total + taps[k : k + 1] * raw[at : at + length]
    return silu(total).astype(BF16)


def write_payload(ref, state, log_row):
    rows = state.shape[0]
    high = log_row.astype(BF16).astype(F32)
    middle = (log_row - high).astype(BF16).astype(F32)
    low = log_row - high - middle
    at = lax.broadcasted_iota(jnp.int32, (PAY, log_row.shape[1]), 0)
    tail = jnp.where(at == 0, high, jnp.where(at == 1, middle, jnp.where(at == 2, low, 0.0)))
    ref[:rows] = state.astype(BF16)
    ref[rows:] = tail.astype(BF16)


def read_payload(ref, k):
    rows = ref.shape[1] - PAY
    tail = ref[k, rows:].astype(F32)
    return ref[k, :rows].astype(F32), jnp.sum(tail, axis=0, keepdims=True)


def scan_payloads(ref, place):
    rows, lanes = ref.shape[1] - PAY, ref.shape[2]
    total = before = jnp.zeros((rows, lanes), F32)
    logs = logs_before = jnp.zeros((1, lanes), F32)
    for k in range(ref.shape[0]):
        state, log_row = read_payload(ref, k)
        total = total * jnp.exp(log_row) + state
        logs = logs + log_row
        before = jnp.where(k < place, total, before)
        logs_before = jnp.where(k < place, logs, logs_before)
    return total, logs, before, logs_before


def squares_of(pieces, total_rows):
    squares = jnp.zeros((total_rows, 1), F32)
    for piece in pieces:
        values = piece[:total_rows].astype(F32)
        squares = squares + jnp.sum(values * values, axis=1, keepdims=True)
    return squares


def norm_kernel(x0, x1, x2, x3, normed):
    total_rows = normed.shape[1]
    scale = lax.rsqrt(squares_of((x0, x1, x2, x3), total_rows) / D + EPSILON)
    for k, piece in enumerate((x0, x1, x2, x3)):
        gain = piece[total_rows : total_rows + 1].astype(F32)
        normed[k] = (piece[:total_rows].astype(F32) * scale * gain).astype(BF16)


def first_kernel(
    normed, mine, other, params, extra,
    value_out, key_out, cum_out, step_out, payload, weight,
):
    core = lax.axis_index("sp_2")
    place = lax.axis_index("tp")
    weight[:, pl.ds(core, 1)] = mine[...][:, None]
    weight[:, pl.ds(1 - core, 1)] = other[...][:, None]
    total_rows = normed.shape[1]
    length = total_rows - HALO
    chips, columns = weight.shape[0] // 4, weight.shape[3]
    acc = jnp.zeros((total_rows, columns), F32)
    for k in range(normed.shape[0]):
        block = weight[pl.ds(((place - k) & 3) * chips, chips)]
        acc = acc + dot(normed[k], block.reshape(-1, columns))
    mix = value_out.shape[1]
    done = convolved(acc.astype(BF16).astype(F32), params[:4], length)
    value_out[...] = done[:, :mix]
    key_out[...] = done[:, mix:]
    raw = jnp.transpose(acc[HALO:, mix:])[HEAD : HEAD + 8] + params[8:16, :1]
    step = jnp.maximum(raw, 0.0) + jnp.log1p(jnp.exp(-jnp.abs(raw)))
    decay = params[16:24, :1] * step + extra[...]
    rows = lax.broadcasted_iota(jnp.int32, (BLOCK, BLOCK), 0)
    upper = (rows <= lax.broadcasted_iota(jnp.int32, (BLOCK, BLOCK), 1)).astype(F32)
    carry, cums = jnp.zeros((8, 1), F32), []
    for b in range(length // BLOCK):
        cums.append(dot(decay[:, b * BLOCK : (b + 1) * BLOCK], upper, precision=HIGH) + carry)
        carry = cums[-1][:, BLOCK - 1 :]
    cum = jnp.concatenate(cums, axis=1)
    cum_out[...] = cum
    step_out[...] = step
    lanes = heads_of_lanes(mix)
    spread = dot(jnp.exp(carry - cum) * step, lanes, 0, 0, HIGH)
    state = dot(done[:, mix:].astype(F32), done[:, :mix].astype(F32) * spread, 0, 0, HIGH)
    write_payload(payload, state[:HEAD], jnp.sum(carry * lanes, axis=0, keepdims=True))


def row_kernel(rows, before_out, logs_out, payload):
    total, logs, before, logs_before = scan_payloads(rows, lax.axis_index(("sp_1", "sp_2")))
    before_out[...] = before
    logs_out[...] = jnp.broadcast_to(logs_before, logs_out.shape)
    write_payload(payload, total, logs)


def inner_kernel(value, cum, step, factors, scaled):
    length, span = scaled.shape
    lanes = heads_of_lanes(span)
    scaled[...] = (value[...].astype(F32) * dot(step[...], lanes, 0, 0, HIGH)).astype(BF16)
    columns = jnp.transpose(cum[...])
    lower = lax.broadcasted_iota(jnp.int32, (BLOCK, BLOCK), 0) >= lax.broadcasted_iota(
        jnp.int32, (BLOCK, BLOCK), 1
    )
    at = 0
    for i in range(length // BLOCK):
        for h in range(span // HEAD):
            for j in range(i + 1):
                column = columns[i * BLOCK : (i + 1) * BLOCK, h : h + 1]
                gap = column - cum[h : h + 1, j * BLOCK : (j + 1) * BLOCK]
                if i == j:
                    gap = jnp.where(lower, gap, -jnp.inf)
                factors[at] = jnp.exp(gap)
                at = at + 1


def block_products(normed, weight, rows_here, weight_here, arrived, lanes, later=()):
    place = lax.axis_index("tp")
    count, total_rows, width = rows_here.shape
    copies = []
    for k in range(count):
        start = pl.multiple_of(((place - k) & 3) * width, width)
        block = weight.at[pl.ds(start, width)]
        copies.append([pltpu.make_async_copy(normed.at[k], rows_here.at[k], arrived.at[k, 0])])
        for n, (first, size) in enumerate(lanes):
            copies[k].append(
                pltpu.make_async_copy(
                    block.at[:, first : first + size], weight_here[n].at[k], arrived.at[k, n + 1]
                )
            )
        for copy in copies[k]:
            copy.start()
    for copy in later:
        copy.start()
    sums = [jnp.zeros((total_rows, size), F32) for _, size in lanes]
    for k in range(count):
        for copy in copies[k]:
            copy.wait()
        for n in range(len(lanes)):
            sums[n] = sums[n] + dot(rows_here[k], weight_here[n][k])
    return sums


def pool_kernel(normed, weight, params, mix_weight, pool_out, rows_here, weight_here, arrived):
    length, span = pool_out.shape
    place = lax.axis_index("tp")
    acc = block_products(normed, weight, rows_here, [weight_here], arrived, [(0, span)])[0]
    values = acc.astype(BF16)
    own = values[HALO:].astype(F32)
    shape = (length, values.shape[0])
    back = HALO + lax.broadcasted_iota(jnp.int32, shape, 0) - lax.broadcasted_iota(jnp.int32, shape, 1)
    band = jnp.where((back >= 0) & (back < (2 << place)), 1.0, 0.0).astype(BF16)
    chosen = dot(band, values)
    position = lax.axis_index(SP) * length + lax.broadcasted_iota(jnp.int32, (length, 1), 0) + 1
    counts = jnp.minimum(position, 2 << place).astype(F32)
    pooled = (chosen / counts - own).astype(BF16)
    pool_out[...] = (dot(pooled, mix_weight[...]) * params[25:26, :span]).astype(BF16)


def second_kernel(
    normed, weight, value, key, factors_far, scaled, params, planes, before, logs_before, cum,
    rows_out, squares_out,
    rows_here, gate_here, read_here, factors, arrived, factors_arrived,
):
    length, span = rows_out.shape
    fetch = pltpu.make_async_copy(factors_far, factors, factors_arrived)
    lanes = [(span, span), (4 * span, BLOCK)]
    acc, acc_read = block_products(
        normed, weight, rows_here, [gate_here, read_here], arrived, lanes, [fetch]
    )
    gate = silu(acc[HALO:].astype(BF16).astype(F32))
    reads = convolved(acc_read.astype(BF16).astype(F32), params[4:8, :BLOCK], length)
    _, _, earlier, _ = scan_payloads(planes, lax.axis_index("sp_0"))
    incoming = earlier * jnp.exp(logs_before[:1]) + before[...]
    decay = dot(jnp.exp(cum[...]), heads_of_lanes(span), 0, 0, HIGH)
    far = dot(reads[:, :HEAD].astype(F32), incoming, precision=HIGH) * decay
    ones = jnp.ones((8, span), F32)
    fetch.wait()
    at = 0
    for i in range(length // BLOCK):
        here = slice(i * BLOCK, (i + 1) * BLOCK)
        products = [
            dot(reads[here], key[j * BLOCK : (j + 1) * BLOCK], 1, 1) for j in range(i + 1)
        ]
        results = []
        for h in range(span // HEAD):
            parts = []
            for j in range(i + 1):
                parts.append((products[j] * factors[at]).astype(BF16))
                at = at + 1
            left = jnp.concatenate(parts, axis=1)
            results.append(dot(left, scaled[: (i + 1) * BLOCK, h * HEAD : (h + 1) * HEAD]))
        near = jnp.concatenate(results, axis=1) + params[24:25, :span] * value[here].astype(F32)
        gated = (near + far[here]) * gate[here]
        squares_out[:, here] = dot(ones, gated * gated, 1, 1, HIGH)[:1]
        rows_out[here] = (gated * params[26:27, :span]).astype(BF16)


def out_kernel(pool, rows, weight, squares, out):
    span = pool.shape[1]
    scale = lax.rsqrt(jnp.sum(squares[...], axis=0) / MIX_W + EPSILON)
    scale = jnp.transpose(jnp.broadcast_to(scale, (8, scale.shape[1])))[:, :1]
    for d in range(out.shape[0]):
        width = out.shape[2]
        block = weight[d * width : (d + 1) * width]
        terms = dot(pool[...], block[:, :span], 1, 1)
        terms = terms + dot(rows[...], block[:, span:], 1, 1) * scale
        out[d] = terms.astype(BF16)


def whole(shape):
    return pl.BlockSpec(shape, lambda *_: (0,) * len(shape))


LIMITS = {"pool": 16, "inner": 24, "norm": 16, "first": 16, "row": 6, "second": 28, "out": 16}


def call(kernel, name, args, outs, flops, scratch=(), specs=None, far=()):
    specs = specs or {}
    moved = sum(a.size * a.dtype.itemsize for a in args)
    args = [
        pltpu.with_memory_space_constraint(a, pltpu.HBM) if k in far else a
        for k, a in enumerate(args)
    ]
    return pl.pallas_call(
        kernel,
        grid=(1,),
        in_specs=[specs.get(k, whole(a.shape)) for k, a in enumerate(args)],
        out_specs=[whole(o.shape) for o in outs],
        out_shape=outs,
        scratch_shapes=list(scratch),
        compiler_params=pltpu.CompilerParams(vmem_limit_bytes=LIMITS[name] * 2**20),
        cost_estimate=pl.CostEstimate(flops=flops, transcendentals=0, bytes_accessed=moved),
    )(*args)


def far_of(shape, dtype):
    return pltpu.HBM(shape, dtype)


def shape_of(shape, dtype):
    return jax.ShapeDtypeStruct(shape, dtype)


def columns_of(array, lanes):
    return jnp.broadcast_to(jnp.pad(array, (0, 8 - array.shape[0]))[:, None], (8, lanes))


def padded(array, lanes):
    return jnp.pad(array, ((0, 0), (0, lanes - array.shape[1])))


def local(
    activations,
    norm_gain,
    pool_weight,
    gate_weight,
    value_weight,
    key_weight,
    read_weight,
    step_weight,
    pool_mix,
    pool_scale,
    taps_value,
    taps_key,
    taps_read,
    step_bias,
    decay_log,
    decay_extra,
    skip_scale,
    state_gain,
    out_pool_weight,
    out_state_weight,
):
    length, width = activations.shape
    mix = value_weight.shape[1]
    state = key_weight.shape[1]
    heads = step_weight.shape[1]
    count = lax.axis_size("tp")
    fill = jnp.zeros((read_weight.shape[0], BLOCK - state), BF16)
    joined = jnp.concatenate(
        [
            pool_weight,
            gate_weight,
            jnp.transpose(out_pool_weight),
            jnp.transpose(out_state_weight),
            read_weight,
            fill,
        ],
        axis=1,
    )
    later_weights = lax.all_gather(joined, SP, axis=0, tiled=True)
    fill = jnp.zeros((key_weight.shape[0], BLOCK - state - heads), BF16)
    first_weights = jnp.concatenate([value_weight, key_weight, step_weight, fill], axis=1)
    mine = sent_to_all(first_weights, ("sp_0", "sp_1"))
    other = lax.ppermute(mine, "sp_2", [(0, 1), (1, 0)])
    size = lax.axis_size(SP)
    before = lax.ppermute(activations[length - HALO :], SP, [(k, k + 1) for k in range(size - 1)])
    gains = jnp.broadcast_to(norm_gain[None, :], (PAY, width))
    sent = jnp.concatenate([before, activations, gains], axis=0)
    pieces = [sent]
    for shift in range(1, count):
        pairs = [(k, (k + shift) % count) for k in range(count)]
        pieces.append(lax.ppermute(sent, "tp", pairs))
    rows = HALO + length
    normed = call(
        norm_kernel,
        "norm",
        pieces,
        (shape_of((count, rows, width), BF16),),
        10**6,
        far=range(4),
    )[0]
    lanes = mix + BLOCK
    params = jnp.concatenate(
        [
            padded(jnp.concatenate([taps_value, taps_key], axis=1), lanes),
            padded(taps_read, lanes),
            columns_of(step_bias, lanes),
            columns_of(-jnp.exp(decay_log), lanes),
            padded(jnp.repeat(skip_scale, HEAD)[None, :], lanes),
            padded(pool_scale[None, :], lanes),
            padded(state_gain[None, :], lanes),
            jnp.zeros((5, lanes), F32),
        ]
    )
    extra = jnp.pad(jnp.transpose(decay_extra), ((0, 8 - heads), (0, 0)))
    columns = mix + BLOCK
    pay = shape_of((HEAD + PAY, mix), BF16)
    value, key, cum, step, payload = call(
        first_kernel,
        "first",
        (normed, mine, other, params, extra),
        (
            far_of((length, mix), BF16),
            far_of((length, BLOCK), BF16),
            far_of((8, length), F32),
            far_of((8, length), F32),
            pay,
        ),
        2 * rows * D * columns,
        [pltpu.VMEM((mine.shape[0], 2, mine.shape[1], columns), BF16)],
        far=(3, 4),
    )
    row_pieces = lax.all_gather(payload, ("sp_1", "sp_2"))
    before_row, logs_row, payload = call(
        row_kernel,
        "row",
        (row_pieces,),
        (far_of((HEAD, mix), F32), far_of((8, mix), F32), pay),
        10**6,
    )
    plane_pieces = sent_to_all(payload, "sp_0")
    blocks = length // BLOCK
    factors, scaled = call(
        inner_kernel,
        "inner",
        (value, cum, step),
        (
            far_of((heads * blocks * (blocks + 1) // 2, BLOCK, BLOCK), F32),
            far_of((length, mix), BF16),
        ),
        10**7,
        far=range(3),
    )
    anywhere = pl.BlockSpec(memory_space=pl.ANY)
    gated, squares = call(
        second_kernel,
        "second",
        (
            normed, later_weights, value, key, factors, scaled, params,
            plane_pieces, before_row, logs_row, cum,
        ),
        (shape_of((length, mix), BF16), shape_of((1, length), F32)),
        2 * rows * D * (mix + BLOCK),
        [
            pltpu.VMEM((count, rows, width), BF16),
            pltpu.VMEM((count, width, mix), BF16),
            pltpu.VMEM((count, width, BLOCK), BF16),
            pltpu.VMEM(factors.shape, F32),
            pltpu.SemaphoreType.DMA((count, 3)),
            pltpu.SemaphoreType.DMA,
        ],
        specs={0: anywhere, 1: anywhere, 4: anywhere},
        far=(0, 1, 2, 3, 4, 5, 6, 8, 9, 10),
    )
    pool_out = call(
        pool_kernel,
        "pool",
        (normed, later_weights, params, pool_mix[0]),
        (far_of((length, mix), BF16),),
        2 * rows * D * mix,
        [
            pltpu.VMEM((count, rows, width), BF16),
            pltpu.VMEM((count, width, mix), BF16),
            pltpu.SemaphoreType.DMA((count, 2)),
        ],
        specs={0: anywhere, 1: anywhere},
        far=range(4),
    )[0]
    all_squares = sent_to_all(squares, "tp")
    terms = call(
        out_kernel,
        "out",
        (pool_out, gated, later_weights, all_squares),
        (shape_of((count, length, width), BF16),),
        2 * length * 2 * mix * D,
        specs={2: pl.BlockSpec((D, 2 * mix), lambda *_: (0, 1))},
        far=(0, 2),
    )[0]
    arrived = lax.all_to_all(terms, "tp", split_axis=0, concat_axis=0, tiled=True)
    return arrived.astype(F32).sum(axis=0).astype(BF16)


def solution(mesh):
    torus = Mesh(mesh.devices.reshape(8, 8, 2, mesh.shape["tp"]), ("sp_0", "sp_1", "sp_2", "tp"))
    placed = (
        P(SP, "tp"),
        P("tp"),
        P(SP, "tp"),
        P(SP, "tp"),
        P(SP, "tp"),
        P(SP, "tp"),
        P(SP, "tp"),
        P(SP, "tp"),
        P("tp", None, None),
        P("tp"),
        P(None, "tp"),
        P(None, "tp"),
        P(None, "tp"),
        P("tp"),
        P("tp"),
        P(SP, "tp"),
        P("tp"),
        P("tp"),
        P("tp", SP),
        P("tp", SP),
    )
    return jax.shard_map(local, mesh=torus, in_specs=placed, out_specs=P(SP, "tp"), check_vma=False)
```

```python
import jax
import jax.numpy as jnp
from jax import lax
from jax.experimental import pallas as pl
from jax.experimental.pallas import tpu as pltpu
from jax.sharding import Mesh
from jax.sharding import PartitionSpec as P


D = 2048
HEAD = 64
MIX_W = 1024
HALO = 16
PAY = 16
BLOCK = 128
SP = ("sp_0", "sp_1", "sp_2")
EPSILON = 1e-06
HIGH = lax.Precision.HIGHEST
F32 = jnp.float32
BF16 = jnp.bfloat16


def sent_to_all(array, axis):
    copies = jnp.broadcast_to(array, (lax.axis_size(axis), *array.shape))
    return lax.all_to_all(copies, axis, split_axis=0, concat_axis=0, tiled=True)


def dot(a, b, left=1, right=0, precision=None):
    return lax.dot_general(
        a, b, (((left,), (right,)), ((), ())), precision=precision, preferred_element_type=F32
    )


def silu(x):
    return x * jax.nn.sigmoid(x)


def heads_of_lanes(lanes):
    head = lax.broadcasted_iota(jnp.int32, (8, lanes), 0)
    lane = lax.broadcasted_iota(jnp.int32, (8, lanes), 1)
    return (head == lane // HEAD).astype(F32)


def convolved(raw, taps, length):
    width = taps.shape[0]
    total = jnp.zeros((length, raw.shape[1]), F32)
    for k in range(width):
        at = HALO - width + 1 + k
        total = total + taps[k : k + 1] * raw[at : at + length]
    return silu(total).astype(BF16)


def write_payload(ref, state, log_row):
    rows = state.shape[0]
    high = log_row.astype(BF16).astype(F32)
    middle = (log_row - high).astype(BF16).astype(F32)
    low = log_row - high - middle
    at = lax.broadcasted_iota(jnp.int32, (PAY, log_row.shape[1]), 0)
    tail = jnp.where(at == 0, high, jnp.where(at == 1, middle, jnp.where(at == 2, low, 0.0)))
    ref[:rows] = state.astype(BF16)
    ref[rows:] = tail.astype(BF16)


def read_payload(ref, k):
    rows = ref.shape[1] - PAY
    tail = ref[k, rows:].astype(F32)
    return ref[k, :rows].astype(F32), jnp.sum(tail, axis=0, keepdims=True)


def scan_payloads(ref, place):
    rows, lanes = ref.shape[1] - PAY, ref.shape[2]
    total = before = jnp.zeros((rows, lanes), F32)
    logs = logs_before = jnp.zeros((1, lanes), F32)
    for k in range(ref.shape[0]):
        state, log_row = read_payload(ref, k)
        total = total * jnp.exp(log_row) + state
        logs = logs + log_row
        before = jnp.where(k < place, total, before)
        logs_before = jnp.where(k < place, logs, logs_before)
    return total, logs, before, logs_before


def squares_of(pieces, total_rows):
    squares = jnp.zeros((total_rows, 1), F32)
    for piece in pieces:
        values = piece[:total_rows].astype(F32)
        squares = squares + jnp.sum(values * values, axis=1, keepdims=True)
    return squares


def norm_kernel(x0, x1, x2, x3, normed):
    total_rows = normed.shape[1]
    scale = lax.rsqrt(squares_of((x0, x1, x2, x3), total_rows) / D + EPSILON)
    for k, piece in enumerate((x0, x1, x2, x3)):
        gain = piece[total_rows : total_rows + 1].astype(F32)
        normed[k] = (piece[:total_rows].astype(F32) * scale * gain).astype(BF16)


def first_kernel(
    normed, mine, other, params, extra,
    value_out, key_out, cum_out, step_out, payload, weight,
):
    core = lax.axis_index("sp_2")
    place = lax.axis_index("tp")
    weight[:, pl.ds(core, 1)] = mine[...][:, None]
    weight[:, pl.ds(1 - core, 1)] = other[...][:, None]
    total_rows = normed.shape[1]
    length = total_rows - HALO
    chips, columns = weight.shape[0] // 4, weight.shape[3]
    acc = jnp.zeros((total_rows, columns), F32)
    for k in range(normed.shape[0]):
        block = weight[pl.ds(((place - k) & 3) * chips, chips)]
        acc = acc + dot(normed[k], block.reshape(-1, columns))
    mix = value_out.shape[1]
    done = convolved(acc.astype(BF16).astype(F32), params[:4], length)
    value_out[...] = done[:, :mix]
    key_out[...] = done[:, mix:]
    raw = jnp.transpose(acc[HALO:, mix:])[HEAD : HEAD + 8] + params[8:16, :1]
    step = jnp.maximum(raw, 0.0) + jnp.log1p(jnp.exp(-jnp.abs(raw)))
    decay = params[16:24, :1] * step + extra[...]
    rows = lax.broadcasted_iota(jnp.int32, (BLOCK, BLOCK), 0)
    upper = (rows <= lax.broadcasted_iota(jnp.int32, (BLOCK, BLOCK), 1)).astype(F32)
    carry, cums = jnp.zeros((8, 1), F32), []
    for b in range(length // BLOCK):
        cums.append(dot(decay[:, b * BLOCK : (b + 1) * BLOCK], upper, precision=HIGH) + carry)
        carry = cums[-1][:, BLOCK - 1 :]
    cum = jnp.concatenate(cums, axis=1)
    cum_out[...] = cum
    step_out[...] = step
    lanes = heads_of_lanes(mix)
    spread = dot(jnp.exp(carry - cum) * step, lanes, 0, 0, HIGH)
    state = dot(done[:, mix:].astype(F32), done[:, :mix].astype(F32) * spread, 0, 0, HIGH)
    write_payload(payload, state[:HEAD], jnp.sum(carry * lanes, axis=0, keepdims=True))


def row_kernel(rows, before_out, logs_out, payload):
    total, logs, before, logs_before = scan_payloads(rows, lax.axis_index(("sp_1", "sp_2")))
    before_out[...] = before
    logs_out[...] = jnp.broadcast_to(logs_before, logs_out.shape)
    write_payload(payload, total, logs)


def inner_kernel(value, cum, step, factors, scaled):
    length, span = scaled.shape
    lanes = heads_of_lanes(span)
    scaled[...] = (value[...].astype(F32) * dot(step[...], lanes, 0, 0, HIGH)).astype(BF16)
    columns = jnp.transpose(cum[...])
    lower = lax.broadcasted_iota(jnp.int32, (BLOCK, BLOCK), 0) >= lax.broadcasted_iota(
        jnp.int32, (BLOCK, BLOCK), 1
    )
    at = 0
    for i in range(length // BLOCK):
        for h in range(span // HEAD):
            for j in range(i + 1):
                column = columns[i * BLOCK : (i + 1) * BLOCK, h : h + 1]
                gap = column - cum[h : h + 1, j * BLOCK : (j + 1) * BLOCK]
                if i == j:
                    gap = jnp.where(lower, gap, -jnp.inf)
                factors[at] = jnp.exp(gap).astype(BF16)
                at = at + 1


def block_products(normed, weight, rows_here, weight_here, arrived, lanes, later=()):
    place = lax.axis_index("tp")
    count, total_rows, width = rows_here.shape
    copies = []
    for k in range(count):
        start = pl.multiple_of(((place - k) & 3) * width, width)
        block = weight.at[pl.ds(start, width)]
        copies.append([pltpu.make_async_copy(normed.at[k], rows_here.at[k], arrived.at[k, 0])])
        for n, (first, size) in enumerate(lanes):
            copies[k].append(
                pltpu.make_async_copy(
                    block.at[:, first : first + size], weight_here[n].at[k], arrived.at[k, n + 1]
                )
            )
        for copy in copies[k]:
            copy.start()
    for copy in later:
        copy.start()
    sums = [jnp.zeros((total_rows, size), F32) for _, size in lanes]
    for k in range(count):
        for copy in copies[k]:
            copy.wait()
        for n in range(len(lanes)):
            sums[n] = sums[n] + dot(rows_here[k], weight_here[n][k])
    return sums


def pool_kernel(normed, weight, params, mix_weight, pool_out, rows_here, weight_here, arrived):
    length, span = pool_out.shape
    place = lax.axis_index("tp")
    acc = block_products(normed, weight, rows_here, [weight_here], arrived, [(0, span)])[0]
    values = acc.astype(BF16)
    own = values[HALO:].astype(F32)
    shape = (length, values.shape[0])
    back = HALO + lax.broadcasted_iota(jnp.int32, shape, 0) - lax.broadcasted_iota(jnp.int32, shape, 1)
    band = jnp.where((back >= 0) & (back < (2 << place)), 1.0, 0.0).astype(BF16)
    chosen = dot(band, values)
    position = lax.axis_index(SP) * length + lax.broadcasted_iota(jnp.int32, (length, 1), 0) + 1
    counts = jnp.minimum(position, 2 << place).astype(F32)
    pooled = (chosen / counts - own).astype(BF16)
    pool_out[...] = (dot(pooled, mix_weight[...]) * params[25:26, :span]).astype(BF16)


def second_kernel(
    normed, weight, value, key, factors_far, scaled, params, planes, before, logs_before, cum,
    rows_out, squares_out,
    rows_here, gate_here, read_here, factors, arrived, factors_arrived,
):
    length, span = rows_out.shape
    fetch = pltpu.make_async_copy(factors_far, factors, factors_arrived)
    lanes = [(span, span), (4 * span, BLOCK)]
    acc, acc_read = block_products(
        normed, weight, rows_here, [gate_here, read_here], arrived, lanes, [fetch]
    )
    gate = silu(acc[HALO:].astype(BF16).astype(F32))
    reads = convolved(acc_read.astype(BF16).astype(F32), params[4:8, :BLOCK], length)
    _, _, earlier, _ = scan_payloads(planes, lax.axis_index("sp_0"))
    incoming = earlier * jnp.exp(logs_before[:1]) + before[...]
    decay = dot(jnp.exp(cum[...]), heads_of_lanes(span), 0, 0, HIGH)
    far = dot(reads[:, :HEAD].astype(F32), incoming, precision=HIGH) * decay
    ones = jnp.ones((8, span), F32)
    fetch.wait()
    at = 0
    for i in range(length // BLOCK):
        here = slice(i * BLOCK, (i + 1) * BLOCK)
        products = [
            dot(reads[here], key[j * BLOCK : (j + 1) * BLOCK], 1, 1) for j in range(i + 1)
        ]
        results = []
        for h in range(span // HEAD):
            parts = []
            for j in range(i + 1):
                parts.append((products[j] * factors[at].astype(F32)).astype(BF16))
                at = at + 1
            left = jnp.concatenate(parts, axis=1)
            results.append(dot(left, scaled[: (i + 1) * BLOCK, h * HEAD : (h + 1) * HEAD]))
        near = jnp.concatenate(results, axis=1) + params[24:25, :span] * value[here].astype(F32)
        gated = (near + far[here]) * gate[here]
        squares_out[:, here] = dot(ones, gated * gated, 1, 1, HIGH)[:1]
        rows_out[here] = (gated * params[26:27, :span]).astype(BF16)


def out_kernel(pool, rows, weight, squares, out):
    span = pool.shape[1]
    scale = lax.rsqrt(jnp.sum(squares[...], axis=0) / MIX_W + EPSILON)
    scale = jnp.transpose(jnp.broadcast_to(scale, (8, scale.shape[1])))[:, :1]
    for d in range(out.shape[0]):
        width = out.shape[2]
        block = weight[d * width : (d + 1) * width]
        terms = dot(pool[...], block[:, :span], 1, 1)
        terms = terms + dot(rows[...], block[:, span:], 1, 1) * scale
        out[d] = terms.astype(BF16)


def whole(shape):
    return pl.BlockSpec(shape, lambda *_: (0,) * len(shape))


LIMITS = {"pool": 16, "inner": 24, "norm": 16, "first": 16, "row": 6, "second": 28, "out": 16}


def call(kernel, name, args, outs, flops, scratch=(), specs=None, far=()):
    specs = specs or {}
    moved = sum(a.size * a.dtype.itemsize for a in args)
    args = [
        pltpu.with_memory_space_constraint(a, pltpu.HBM) if k in far else a
        for k, a in enumerate(args)
    ]
    return pl.pallas_call(
        kernel,
        grid=(1,),
        in_specs=[specs.get(k, whole(a.shape)) for k, a in enumerate(args)],
        out_specs=[whole(o.shape) for o in outs],
        out_shape=outs,
        scratch_shapes=list(scratch),
        compiler_params=pltpu.CompilerParams(vmem_limit_bytes=LIMITS[name] * 2**20),
        cost_estimate=pl.CostEstimate(flops=flops, transcendentals=0, bytes_accessed=moved),
    )(*args)


def far_of(shape, dtype):
    return pltpu.HBM(shape, dtype)


def shape_of(shape, dtype):
    return jax.ShapeDtypeStruct(shape, dtype)


def columns_of(array, lanes):
    return jnp.broadcast_to(jnp.pad(array, (0, 8 - array.shape[0]))[:, None], (8, lanes))


def padded(array, lanes):
    return jnp.pad(array, ((0, 0), (0, lanes - array.shape[1])))


def local(
    activations,
    norm_gain,
    pool_weight,
    gate_weight,
    value_weight,
    key_weight,
    read_weight,
    step_weight,
    pool_mix,
    pool_scale,
    taps_value,
    taps_key,
    taps_read,
    step_bias,
    decay_log,
    decay_extra,
    skip_scale,
    state_gain,
    out_pool_weight,
    out_state_weight,
):
    length, width = activations.shape
    mix = value_weight.shape[1]
    state = key_weight.shape[1]
    heads = step_weight.shape[1]
    count = lax.axis_size("tp")
    fill = jnp.zeros((read_weight.shape[0], BLOCK - state), BF16)
    joined = jnp.concatenate(
        [
            pool_weight,
            gate_weight,
            jnp.transpose(out_pool_weight),
            jnp.transpose(out_state_weight),
            read_weight,
            fill,
        ],
        axis=1,
    )
    later_weights = lax.all_gather(joined, SP, axis=0, tiled=True)
    fill = jnp.zeros((key_weight.shape[0], BLOCK - state - heads), BF16)
    first_weights = jnp.concatenate([value_weight, key_weight, step_weight, fill], axis=1)
    mine = sent_to_all(first_weights, ("sp_0", "sp_1"))
    other = lax.ppermute(mine, "sp_2", [(0, 1), (1, 0)])
    size = lax.axis_size(SP)
    before = lax.ppermute(activations[length - HALO :], SP, [(k, k + 1) for k in range(size - 1)])
    gains = jnp.broadcast_to(norm_gain[None, :], (PAY, width))
    sent = jnp.concatenate([before, activations, gains], axis=0)
    pieces = [sent]
    for shift in range(1, count):
        pairs = [(k, (k + shift) % count) for k in range(count)]
        pieces.append(lax.ppermute(sent, "tp", pairs))
    rows = HALO + length
    normed = call(
        norm_kernel,
        "norm",
        pieces,
        (shape_of((count, rows, width), BF16),),
        10**6,
        far=range(4),
    )[0]
    lanes = mix + BLOCK
    params = jnp.concatenate(
        [
            padded(jnp.concatenate([taps_value, taps_key], axis=1), lanes),
            padded(taps_read, lanes),
            columns_of(step_bias, lanes),
            columns_of(-jnp.exp(decay_log), lanes),
            padded(jnp.repeat(skip_scale, HEAD)[None, :], lanes),
            padded(pool_scale[None, :], lanes),
            padded(state_gain[None, :], lanes),
            jnp.zeros((5, lanes), F32),
        ]
    )
    extra = jnp.pad(jnp.transpose(decay_extra), ((0, 8 - heads), (0, 0)))
    columns = mix + BLOCK
    pay = shape_of((HEAD + PAY, mix), BF16)
    value, key, cum, step, payload = call(
        first_kernel,
        "first",
        (normed, mine, other, params, extra),
        (
            far_of((length, mix), BF16),
            far_of((length, BLOCK), BF16),
            far_of((8, length), F32),
            far_of((8, length), F32),
            pay,
        ),
        2 * rows * D * columns,
        [pltpu.VMEM((mine.shape[0], 2, mine.shape[1], columns), BF16)],
        far=(3, 4),
    )
    row_pieces = lax.all_gather(payload, ("sp_1", "sp_2"))
    before_row, logs_row, payload = call(
        row_kernel,
        "row",
        (row_pieces,),
        (far_of((HEAD, mix), F32), far_of((8, mix), F32), pay),
        10**6,
    )
    plane_pieces = sent_to_all(payload, "sp_0")
    blocks = length // BLOCK
    factors, scaled = call(
        inner_kernel,
        "inner",
        (value, cum, step),
        (
            far_of((heads * blocks * (blocks + 1) // 2, BLOCK, BLOCK), BF16),
            far_of((length, mix), BF16),
        ),
        10**7,
        far=range(3),
    )
    anywhere = pl.BlockSpec(memory_space=pl.ANY)
    gated, squares = call(
        second_kernel,
        "second",
        (
            normed, later_weights, value, key, factors, scaled, params,
            plane_pieces, before_row, logs_row, cum,
        ),
        (shape_of((length, mix), BF16), shape_of((1, length), F32)),
        2 * rows * D * (mix + BLOCK),
        [
            pltpu.VMEM((count, rows, width), BF16),
            pltpu.VMEM((count, width, mix), BF16),
            pltpu.VMEM((count, width, BLOCK), BF16),
            pltpu.VMEM(factors.shape, BF16),
            pltpu.SemaphoreType.DMA((count, 3)),
            pltpu.SemaphoreType.DMA,
        ],
        specs={0: anywhere, 1: anywhere, 4: anywhere},
        far=(0, 1, 2, 3, 4, 5, 6, 8, 9, 10),
    )
    pool_out = call(
        pool_kernel,
        "pool",
        (normed, later_weights, params, pool_mix[0]),
        (far_of((length, mix), BF16),),
        2 * rows * D * mix,
        [
            pltpu.VMEM((count, rows, width), BF16),
            pltpu.VMEM((count, width, mix), BF16),
            pltpu.SemaphoreType.DMA((count, 2)),
        ],
        specs={0: anywhere, 1: anywhere},
        far=range(4),
    )[0]
    all_squares = sent_to_all(squares, "tp")
    terms = call(
        out_kernel,
        "out",
        (pool_out, gated, later_weights, all_squares),
        (shape_of((count, length, width), BF16),),
        2 * length * 2 * mix * D,
        specs={2: pl.BlockSpec((D, 2 * mix), lambda *_: (0, 1))},
        far=(0, 2),
    )[0]
    arrived = lax.all_to_all(terms, "tp", split_axis=0, concat_axis=0, tiled=True)
    return arrived.astype(F32).sum(axis=0).astype(BF16)


def solution(mesh):
    torus = Mesh(mesh.devices.reshape(8, 8, 2, mesh.shape["tp"]), ("sp_0", "sp_1", "sp_2", "tp"))
    placed = (
        P(SP, "tp"),
        P("tp"),
        P(SP, "tp"),
        P(SP, "tp"),
        P(SP, "tp"),
        P(SP, "tp"),
        P(SP, "tp"),
        P(SP, "tp"),
        P("tp", None, None),
        P("tp"),
        P(None, "tp"),
        P(None, "tp"),
        P(None, "tp"),
        P("tp"),
        P("tp"),
        P(SP, "tp"),
        P("tp"),
        P("tp"),
        P("tp", SP),
        P("tp", SP),
    )
    return jax.shard_map(local, mesh=torus, in_specs=placed, out_specs=P(SP, "tp"), check_vma=False)
```
